256 devices in a mesh: sp: 64 (over z, x, core), tp: 4 (over y).
Axes of the slice: x: 4, y: 4, z: 8, core: 2. Of those that a mesh axis runs over, the one named last changes fastest.
Arguments:
- residual: bfloat16 [32768, 2048], P(('sp', 'tp')), may hold values from -6 to 6
- conv_value: bfloat16 [32768, 1024], P('sp', 'tp'), may hold values from -6 to 6
- conv_gate: bfloat16 [32768, 1024], P('sp', 'tp'), may hold values from -9 to 9
- segments: int32 [32768], P('sp'), may hold values from 0 to 31, never falling along the last dimension, each value on 1 to 2048 neighbouring positions
- conv_weight: float32 [31, 1024], P(None, 'tp'), may hold values from -1 to 1
- norm_gain: float32 [1024], P('tp'), may hold values from 0.1 to 1.9
- norm_shift: float32 [1024], P('tp'), may hold values from -3 to 3
- out_weight: bfloat16 [1024, 2048], replicated, may hold values from -0.1875 to 0.1875
- ffn_gain: float32 [2048], replicated, may hold values from 0.1 to 1.9
- routes: int32 [32768, 2], P('sp'), may hold values from 0 to 63, all different within a row; in each aligned block of 128 rows (0 to 127, 128 to 255, ...) at most 8 rows name the same one
- route_weights: float32 [32768, 2], P('sp'), may hold values from 0.2 to 1
- w_gate: bfloat16 [64, 2048, 1024], P('sp', None, 'tp'), may hold values from -0.125 to 0.125
- w_up: bfloat16 [64, 2048, 1024], P('sp', None, 'tp'), may hold values from -0.125 to 0.125
- w_down: bfloat16 [64, 1024, 2048], P('sp', 'tp'), may hold values from -0.1875 to 0.1875
Outputs:
- layer_out: bfloat16 [32768, 2048], P(('sp', 'tp'))
The draws below stay inside these ranges and needn't reach their ends.
Inputs may be any that keep to these rules, and one draw needn't show every extreme that they name: `routes`: within the rows of one device (aligned blocks of 512 / 4 rows), no expert is named more than 8 times; the two experts of a row differ. `segments`: document numbers never fall along the sequence.
All inputs are finite; a program needn't handle non-finite values.
Results may differ from the reference program's by a relative error of at most 0.007.
Values may be sent and summed in bfloat16 or wider, within the bound.
No kernel may reach another device: no remote copies, remote signals or barrier semaphores. Data moves between devices by JAX's collectives and lax.ppermute only.
A program may use at most 128 MiB of HBM per device.

```python
import math
import jax
import jax.numpy as jnp
import numpy as np
from jax import lax

D = 2048
DC = 1024
FF = 1024
CONV_WIDTH = 31
CONV_GROUPS = 8
TOPK = 2
TOK_DEV = 512
TOKENS = 32768
EXPERTS = 64
CAP = 8
N_SP = 64
N_TP = 4


def steps_of(stream_key, shape, cuts, low, largest):
    level = 1.0
    for dim, shards_of in cuts:
        heights = jax.random.uniform(jax.random.fold_in(jax.random.fold_in(stream_key, 6), dim), (shards_of,), jnp.float32, low / len(cuts), largest / len(cuts))
        level = level * jnp.repeat(jnp.exp(heights), shape[dim] // shards_of).reshape((-1,) + (1,) * (len(shape) - 1 - dim))
    return level


def profile(amount, total, bound, slope):
    weights = [(1 << 20) // math.isqrt(grade ** slope) + 1 for grade in range(2, amount + 1)]
    spare, given = total - bound - (amount - 1), [1] * (amount - 1)
    while spare > 0:
        candidates = [i for i in range(amount - 1) if given[i] < bound]
        pool, left = sum([weights[i] for i in candidates]), spare
        for i in candidates:
            more = min(bound - given[i], max(1, left * weights[i] // pool), spare)
            given[i] = given[i] + more
            spare = spare - more
    return np.array([bound] + given)


def uneven(key, number_of, total, most, lean):
    if number_of == 2:
        one = jax.random.randint(key, (), max(1, total - most), min(most, total - 1) + 1)
        return jnp.stack([one, total - one])
    sizes = jnp.asarray(profile(number_of, total, most, lean), jnp.int32)
    couples = (number_of - 1) // 2
    donor, sink = sizes[1:1 + 2 * couples:2], sizes[2:2 + 2 * couples:2]
    margin = jnp.minimum(donor - 1, most - sink)
    shifted = jax.random.randint(jax.random.fold_in(key, 1), (couples,), 0, 1 << 20) % (margin + 1)
    sizes = sizes.at[1:1 + 2 * couples:2].set(donor - shifted).at[2:2 + 2 * couples:2].set(sink + shifted)
    return sizes[jax.random.permutation(jax.random.fold_in(key, 2), number_of)]


def assign_block(key, own, number, rows, count, top, most, lean):
    sequence = jax.random.permutation(key, count)
    crowded, usual = portions_of(count, rows * top, most, lean, True), portions_of(count, rows * top, most, lean, False)
    places = jnp.arange(count)

    def named(tallies, turn):
        used = int((tallies > 0).sum())
        fixed = max(1, used // 4)
        passed = fixed + (places - fixed + turn * (used - fixed)) % max(1, count - fixed)
        return jnp.zeros((count,), jnp.int32).at[sequence[jnp.where(places < fixed, places, passed)]].set(jnp.asarray(tallies, jnp.int32))

    tallies = jnp.where(number % 4 == 0, named(crowded, number // 4), named(usual, number - number // 4 - 1))
    mixed = jax.random.permutation(jax.random.fold_in(own, 3), count)
    donor, taker = mixed[0:count // 2 * 2:2], mixed[1:count // 2 * 2:2]
    slack = jnp.minimum(tallies[donor] - 1, most - tallies[taker]) // 2
    slack = jnp.where((donor == sequence[0]) | (taker == sequence[0]) | (tallies[taker] == 0), 0, jnp.maximum(slack, 0))
    passed = jax.random.randint(jax.random.fold_in(own, 4), (count // 2,), 0, 1 << 20) % (slack + 1)
    tallies = tallies.at[donor].add(-passed).at[taker].add(passed)
    items = jnp.searchsorted(jnp.cumsum(tallies), jnp.arange(rows * top), side="right").astype(jnp.int32)
    table = items.reshape(top, rows).T
    table = table[jax.random.permutation(jax.random.fold_in(own, 1), rows)]
    turn = jax.random.randint(jax.random.fold_in(own, 2), (rows, 1), 0, top)
    return jnp.take_along_axis(table, (jnp.arange(top)[None, :] + turn) % top, axis=1)


def portions_of(count, total, limit, slope, full):
    loads = [(1 << 20) // math.isqrt(standing ** slope) + 1 for standing in range(1, count + 1)]
    largest = limit if full else min(limit, max(-(-total // count), total * loads[0] // sum(loads)))
    least = 1 if total - largest >= count - 1 else 0
    holding, rest = [largest] + [least] * (count - 1), total - largest - least * (count - 1)
    while rest > 0:
        movable = [i for i in range(1, count) if holding[i] < largest] or [i for i in range(1, count) if holding[i] < limit]
        pool, budget = sum([loads[i] for i in movable]), rest
        for i in movable:
            addition = min(limit - holding[i], max(1, budget * loads[i] // pool), rest)
            holding[i] = holding[i] + addition
            rest = rest - addition
    return np.array(holding)


def gaussian(stream_key, extent, scale, most, cuts=(), kind=jnp.bfloat16):
    result = scale * jax.random.normal(stream_key, extent, jnp.float32)
    if cuts:
        result = result * steps_of(stream_key, extent, cuts, -0.22, 0.18)
    return jnp.clip(result, -most, most).astype(kind)


def setup_inputs(seed: int = 0) -> dict:
    arg_keys = jax.random.split(jax.random.key(seed), 15)
    residual = gaussian(arg_keys[0], (TOKENS, D), 1.0, 6.0, ((0, 256),))
    conv_value = gaussian(arg_keys[1], (TOKENS, DC), 1.0, 6.0, ((0, 64), (1, 4)))
    conv_gate = gaussian(arg_keys[2], (TOKENS, DC), 1.5, 9.0, ((0, 64), (1, 4)))
    segments = jnp.searchsorted(jnp.cumsum(uneven(arg_keys[3], N_SP // 2, TOKENS, 4 * TOK_DEV, 0)), jnp.arange(TOKENS), side="right").astype(jnp.int32)
    conv_weight = gaussian(arg_keys[4], (CONV_WIDTH, DC), CONV_WIDTH ** -0.5, 1.0, ((1, 4),), jnp.float32)
    norm_gain = jnp.clip(1.0 + 0.18 * jax.random.normal(arg_keys[5], (DC,), jnp.float32), 0.1, 1.9)
    norm_shift = gaussian(arg_keys[6], (DC,), 0.5, 3.0, ((0, 4),), jnp.float32)
    out_weight = gaussian(arg_keys[7], (DC, D), DC ** -0.5, 0.1875)
    ffn_gain = jnp.clip(1.0 + 0.18 * jax.random.normal(arg_keys[8], (D,), jnp.float32), 0.1, 1.9)
    routes_keys = jax.random.split(jax.random.fold_in(arg_keys[9], 1), TOKENS // (TOK_DEV // N_TP))
    routes_turns = jax.random.permutation(jax.random.fold_in(arg_keys[9], 3), TOKENS // (TOK_DEV // N_TP))
    routes = jax.vmap(lambda own, number: assign_block(jax.random.fold_in(arg_keys[9], 2), own, number, TOK_DEV // N_TP, EXPERTS, TOPK, CAP, 2))(routes_keys, routes_turns).reshape((TOKENS, TOPK))
    route_weights = jnp.clip(0.2 + 0.8 * jax.random.uniform(arg_keys[10], (TOKENS, TOPK), jnp.float32) ** steps_of(arg_keys[10], (TOKENS, TOPK), ((0, 64),), -0.2, 0.2), 0.2, 1.0)
    w_gate = gaussian(arg_keys[11], (EXPERTS, D, FF), D ** -0.5, 0.125, ((0, 64), (2, 4)))
    w_up = gaussian(arg_keys[12], (EXPERTS, D, FF), D ** -0.5, 0.125, ((0, 64), (2, 4)))
    w_down = gaussian(arg_keys[13], (EXPERTS, FF, D), FF ** -0.5, 0.1875, ((0, 64), (1, 4)))
    return dict(residual=residual, conv_value=conv_value, conv_gate=conv_gate, segments=segments, conv_weight=conv_weight, norm_gain=norm_gain, norm_shift=norm_shift, out_weight=out_weight, ffn_gain=ffn_gain, routes=routes, route_weights=route_weights, w_gate=w_gate, w_up=w_up, w_down=w_down)


def reference(residual, conv_value, conv_gate, segments, conv_weight, norm_gain, norm_shift, out_weight, ffn_gain, routes, route_weights, w_gate, w_up, w_down):
    gated = (conv_value.astype(jnp.float32) * jax.nn.sigmoid(conv_gate.astype(jnp.float32))).astype(jnp.bfloat16)
    reach = CONV_WIDTH - 1
    padded = jnp.concatenate([jnp.zeros((reach, DC), jnp.bfloat16), gated], 0).astype(jnp.float32)
    seg_padded = jnp.concatenate([jnp.full((reach,), -1, jnp.int32), segments.astype(jnp.int32)], 0)
    convolved = jnp.zeros((TOKENS, DC), jnp.float32)
    for offset in range(CONV_WIDTH):
        same_doc = (seg_padded[offset:offset + TOKENS] == segments)[:, None]
        convolved = convolved + jnp.where(same_doc, padded[offset:offset + TOKENS] * conv_weight[offset], 0.0)
    grouped = convolved.reshape(TOKENS, CONV_GROUPS, DC // CONV_GROUPS)
    group_mean = lax.optimization_barrier(jnp.mean(grouped, axis=-1, keepdims=True))
    group_var = lax.optimization_barrier(jnp.mean(jnp.square(grouped - group_mean), axis=-1, keepdims=True))
    scaled = ((grouped - group_mean) * lax.rsqrt(group_var + 1e-05)).reshape(TOKENS, DC) * norm_gain + norm_shift
    conv_out = jax.nn.silu(scaled).astype(jnp.bfloat16)
    mixed = jnp.dot(conv_out, out_weight, preferred_element_type=jnp.float32).astype(jnp.bfloat16)
    stream = residual.astype(jnp.float32) + lax.optimization_barrier(mixed).astype(jnp.float32)
    normed = (stream * lax.rsqrt(lax.optimization_barrier(jnp.mean(stream * stream, axis=-1, keepdims=True)) + 1e-06) * ffn_gain).astype(jnp.bfloat16)
    rows_dev = TOK_DEV // N_TP
    blocks = TOKENS // rows_dev
    route_pairs = routes.reshape(blocks, rows_dev * TOPK)
    onehot = (route_pairs[..., None] == jnp.arange(EXPERTS, dtype=jnp.int32)).astype(jnp.int32)
    slot_rank = lax.optimization_barrier(jnp.sum((jnp.cumsum(onehot, axis=1) - onehot) * onehot, axis=2)).reshape(TOKENS, TOPK)
    token_id = jnp.broadcast_to(jnp.arange(TOKENS, dtype=jnp.int32)[:, None], (TOKENS, TOPK))
    block_id = token_id // rows_dev
    owners = jnp.full((EXPERTS, blocks, CAP), TOKENS, jnp.int32).at[routes, block_id, slot_rank].set(token_id)
    weight_table = jnp.zeros((EXPERTS, blocks, CAP), jnp.float32).at[routes, block_id, slot_rank].set(route_weights)
    rows_pad = jnp.concatenate([normed, jnp.zeros((1, D), jnp.bfloat16)], 0)

    def one_expert(totals, inputs):
        gate_w, up_w, down_w, expert_owners, expert_weights = inputs
        row_index = expert_owners.reshape(-1)
        picked = rows_pad[row_index]
        gate_act = jnp.dot(picked, gate_w, preferred_element_type=jnp.float32)
        up_act = jnp.dot(picked, up_w, preferred_element_type=jnp.float32)
        hidden = (jax.nn.silu(gate_act) * up_act).astype(jnp.bfloat16)
        summed = jnp.dot(hidden, down_w, preferred_element_type=jnp.float32)
        expert_out = lax.optimization_barrier(summed.astype(jnp.bfloat16)).astype(jnp.float32)
        totals = totals.at[row_index].add(expert_weights.reshape(-1)[:, None] * expert_out)
        return (totals, None)
    totals, _ = lax.scan(one_expert, jnp.zeros((TOKENS + 1, D), jnp.float32), (w_gate, w_up, w_down, owners, weight_table))
    return (stream + totals[:TOKENS]).astype(jnp.bfloat16)
```

```python
import jax
import jax.numpy as jnp
from jax import lax
from jax.experimental import pallas as pl
from jax.experimental.pallas import tpu as pltpu
from jax.sharding import PartitionSpec as P

TAPS = 31
RIM = 32
LANES = 128
BLOCK = 64


def passed_along(value, axis, steps):
    count = lax.axis_size(axis)
    initial, last = (max(0, -steps), min(count, count - steps))
    return lax.ppermute(value, axis, [(source, source + steps) for source in range(initial, last)])


def ring(value, axis, steps):
    count = lax.axis_size(axis)
    return lax.ppermute(value, axis, [(i, (i + steps) % count) for i in range(count)])


def slot_numbers(block_routes, capacity, experts_n):
    route_pairs = block_routes.reshape(block_routes.shape[:-2] + (-1,))
    onehot = (route_pairs[..., None] == jnp.arange(experts_n, dtype=jnp.int32)).astype(jnp.int32)
    slot_rank = jnp.sum((jnp.cumsum(onehot, axis=-2) - onehot) * onehot, axis=-1)
    return (route_pairs * capacity + slot_rank).reshape(block_routes.shape)


def dispatch_matrix(slot_ids, slot_total):
    numbers = jnp.arange(slot_total, dtype=jnp.int32)[:, None, None]
    matches = jnp.any(numbers == slot_ids[..., None, :, :], axis=-1)
    return matches.astype(jnp.bfloat16)


def conv_body(value_ref, gate_ref, rim_ref, seen_ref, taps_ref, gain_ref, shift_ref, out_ref, rows_ref):
    tok = value_ref.shape[0]
    gated = value_ref[...].astype(jnp.float32) * jax.nn.sigmoid(gate_ref[...].astype(jnp.float32))
    rows_ref[0, :RIM] = rim_ref[...].astype(jnp.float32)
    rows_ref[0, RIM:] = gated.astype(jnp.bfloat16).astype(jnp.float32)
    for r in range(1, 8):
        rows_ref[r, 8:] = rows_ref[0, 8 - r : RIM + tok - r]

    def block(i, carry):
        at = pl.multiple_of(i * BLOCK, BLOCK)
        seen = seen_ref[pl.ds(at, BLOCK), :]
        for lane in range(0, value_ref.shape[1], LANES):
            cols = slice(lane, lane + LANES)
            total = rows_ref[0, pl.ds(at + RIM, BLOCK), cols] * taps_ref[TAPS - 1 : TAPS, cols]
            for back in range(1, TAPS):
                tap = TAPS - 1 - back
                rows = rows_ref[back % 8, pl.ds(at + RIM - back // 8 * 8, BLOCK), cols]
                total = total + jnp.where(seen >= back, rows * taps_ref[tap : tap + 1, cols], 0.0)
            dev = total - jnp.mean(total, axis=1, keepdims=True)
            var = jnp.mean(dev * dev, axis=1, keepdims=True)
            v = dev * lax.rsqrt(var + 1e-05) * gain_ref[:, cols] + shift_ref[:, cols]
            out_ref[pl.ds(at, BLOCK), cols] = (v / (1.0 + jnp.exp(-v))).astype(jnp.bfloat16)
        return carry

    lax.fori_loop(0, tok // BLOCK, block, 0)


def conv_module(value, gate, rim, seen, taps, gain, shift):
    tok, width = value.shape
    return pl.pallas_call(
        conv_body,
        out_shape=jax.ShapeDtypeStruct((tok, width), jnp.bfloat16),
        scratch_shapes=[pltpu.VMEM((8, RIM + tok, width), jnp.float32)],
        name="conv_module",
    )(value, gate, rim, seen, taps, gain[None], shift[None])


def gathered(shard):
    half = shard.shape[0] // 2
    left, right, far = [], [], []
    for part in range(2):
        piece = shard[part * half : (part + 1) * half]
        left.append(ring(piece, "tp", 1))
        right.append(ring(piece, "tp", -1))
    far.append(ring(left[0], "tp", 1))
    far.append(ring(right[1], "tp", -1))
    return left, right, far


def dot(a, b):
    return jnp.dot(a, b, preferred_element_type=jnp.float32)


def shards(
    residual,
    conv_value,
    conv_gate,
    segments,
    conv_weight,
    norm_gain,
    norm_shift,
    out_weight,
    ffn_gain,
    routes,
    route_weights,
    w_gate,
    w_up,
    w_down,
):
    tok_dev, local_channels = conv_value.shape
    reach = conv_weight.shape[0] - 1
    gates = gathered(w_gate[0])
    ups = gathered(w_up[0])
    downs = gathered(w_down[0])
    tail = slice(tok_dev - reach, tok_dev)
    rim = (
        conv_value[tail].astype(jnp.float32) * jax.nn.sigmoid(conv_gate[tail].astype(jnp.float32))
    ).astype(jnp.bfloat16)
    named = jnp.pad(segments[tail].astype(jnp.bfloat16)[None], ((0, 1), (0, local_channels - reach)))
    rim = passed_along(jnp.concatenate([named, rim], 0), "sp", 1)
    seg_ext = jnp.concatenate([rim[0, :reach].astype(jnp.int32), segments], 0)
    seen = jnp.zeros((tok_dev,), jnp.int32)
    for offset in range(reach):
        seen = seen + (seg_ext[offset : offset + tok_dev] == segments).astype(jnp.int32)
    seen = jnp.broadcast_to(seen[:, None], (tok_dev, LANES))
    conv_out = conv_module(
        conv_value, conv_gate, rim, seen, conv_weight, norm_gain, norm_shift
    )
    columns = lax.axis_size("tp")
    column = lax.axis_index("tp")
    rows_own = tok_dev // columns
    regrouped = lax.all_to_all(conv_out, "tp", split_axis=0, concat_axis=1, tiled=True)
    mixed = dot(regrouped, out_weight)
    stream = residual.astype(jnp.float32) + lax.optimization_barrier(
        mixed.astype(jnp.bfloat16)
    ).astype(jnp.float32)
    normed = (
        stream * lax.rsqrt(jnp.mean(stream * stream, axis=-1, keepdims=True) + 1e-06) * ffn_gain
    ).astype(jnp.bfloat16)
    experts_n = lax.axis_size("sp")
    top_count = routes.shape[1]
    model_width = normed.shape[1]
    capacity = max(2, 2 * tok_dev * top_count // (columns * experts_n))
    slot_total = experts_n * capacity
    own_routes = lax.dynamic_slice_in_dim(routes, column * rows_own, rows_own, 0)
    own_weights = lax.dynamic_slice_in_dim(route_weights, column * rows_own, rows_own, 0)
    own_slots = slot_numbers(own_routes, capacity, experts_n)
    routing_table = dispatch_matrix(own_slots, slot_total)
    outgoing = dot(routing_table, normed).astype(jnp.bfloat16)
    outgoing = outgoing.reshape(experts_n, capacity, model_width)
    arrived = lax.all_to_all(outgoing, "sp", split_axis=0, concat_axis=1, tiled=True)
    arrived = arrived.reshape(slot_total, model_width)

    def quarter(gate, up, down):
        def rows(x, parts):
            half = x.shape[1] // 2
            return dot(x[:, :half], parts[0]) + dot(x[:, half:], parts[1])

        hidden = (jax.nn.silu(rows(arrived, gate)) * rows(arrived, up)).astype(jnp.bfloat16)
        return rows(hidden, down)

    hidden = (jax.nn.silu(dot(arrived, w_gate[0])) * dot(arrived, w_up[0])).astype(jnp.bfloat16)
    summed = dot(hidden, w_down[0])
    for side in range(3):
        summed = summed + quarter(gates[side], ups[side], downs[side])
    expert_out = summed.astype(jnp.bfloat16).reshape(experts_n, capacity, model_width)
    returned = lax.all_to_all(expert_out, "sp", split_axis=0, concat_axis=0, tiled=True)
    returned = returned.reshape(slot_total, model_width)
    combined = stream
    for member in range(top_count):
        chosen = jnp.take(returned, own_slots[:, member], axis=0).astype(jnp.float32)
        combined = combined + own_weights[:, member : member + 1] * chosen
    return combined.astype(jnp.bfloat16)


def solution(mesh):
    return jax.shard_map(
        shards,
        mesh=mesh,
        in_specs=(
            P(("sp", "tp"), None),
            P("sp", "tp"),
            P("sp", "tp"),
            P("sp"),
            P(None, "tp"),
            P("tp"),
            P("tp"),
            P(),
            P(),
            P("sp", None),
            P("sp", None),
            P("sp", None, "tp"),
            P("sp", None, "tp"),
            P("sp", "tp", None),
        ),
        out_specs=P(("sp", "tp"), None),
        check_vma=False,
    )
```

```python
import functools

import jax
import jax.numpy as jnp
from jax import lax
from jax.experimental import pallas as pl
from jax.experimental.pallas import tpu as pltpu
from jax.sharding import PartitionSpec as P

TAPS = 31
RIM = 32
LANES = 128
BLOCK = 64


def passed_along(value, axis, steps):
    count = lax.axis_size(axis)
    initial, last = (max(0, -steps), min(count, count - steps))
    return lax.ppermute(value, axis, [(source, source + steps) for source in range(initial, last)])


def ring(value, axis, steps):
    count = lax.axis_size(axis)
    return lax.ppermute(value, axis, [(i, (i + steps) % count) for i in range(count)])


def slot_numbers(block_routes, capacity, experts_n):
    route_pairs = block_routes.reshape(block_routes.shape[:-2] + (-1,))
    onehot = (route_pairs[..., None] == jnp.arange(experts_n, dtype=jnp.int32)).astype(jnp.int32)
    slot_rank = jnp.sum((jnp.cumsum(onehot, axis=-2) - onehot) * onehot, axis=-1)
    return (route_pairs * capacity + slot_rank).reshape(block_routes.shape)


def conv_body(value_ref, gate_ref, rim_ref, seen_ref, taps_ref, gain_ref, shift_ref, out_ref, rows_ref):
    tok = value_ref.shape[0]
    gated = value_ref[...].astype(jnp.float32) * jax.nn.sigmoid(gate_ref[...].astype(jnp.float32))
    rows_ref[0, :RIM] = rim_ref[...].astype(jnp.float32)
    rows_ref[0, RIM:] = gated.astype(jnp.bfloat16).astype(jnp.float32)
    for r in range(1, 8):
        rows_ref[r, 8:] = rows_ref[0, 8 - r : RIM + tok - r]

    def block(i, carry):
        at = pl.multiple_of(i * BLOCK, BLOCK)
        seen = seen_ref[pl.ds(at, BLOCK), :]
        for lane in range(0, value_ref.shape[1], LANES):
            cols = slice(lane, lane + LANES)
            total = rows_ref[0, pl.ds(at + RIM, BLOCK), cols] * taps_ref[TAPS - 1 : TAPS, cols]
            for back in range(1, TAPS):
                tap = TAPS - 1 - back
                rows = rows_ref[back % 8, pl.ds(at + RIM - back // 8 * 8, BLOCK), cols]
                total = total + jnp.where(seen >= back, rows * taps_ref[tap : tap + 1, cols], 0.0)
            dev = total - jnp.mean(total, axis=1, keepdims=True)
            var = jnp.mean(dev * dev, axis=1, keepdims=True)
            v = dev * lax.rsqrt(var + 1e-05) * gain_ref[:, cols] + shift_ref[:, cols]
            out_ref[pl.ds(at, BLOCK), cols] = (v / (1.0 + jnp.exp(-v))).astype(jnp.bfloat16)
        return carry

    lax.fori_loop(0, tok // BLOCK, block, 0)


def conv_module(value, gate, rim, seen, taps, gain, shift):
    tok, width = value.shape
    return pl.pallas_call(
        conv_body,
        out_shape=jax.ShapeDtypeStruct((tok, width), jnp.bfloat16),
        scratch_shapes=[pltpu.VMEM((8, RIM + tok, width), jnp.float32)],
        name="conv_module",
    )(value, gate, rim, seen, taps, gain[None], shift[None])


def dot(a, b):
    return jnp.dot(a, b, preferred_element_type=jnp.float32)


def places(slots, total):
    numbers = lax.broadcasted_iota(jnp.int32, (slots.shape[0], total), 1)
    return [numbers == slots[:, m : m + 1] for m in range(slots.shape[1])]


def route_body(parts_ref, out_weight_ref, residual_ref, gain_ref, slots_ref, stream_ref, *sent_refs):
    width = parts_ref.shape[2]
    mixed = dot(parts_ref[0], out_weight_ref[:width])
    for j in range(1, parts_ref.shape[0]):
        mixed = mixed + dot(parts_ref[j], out_weight_ref[j * width : (j + 1) * width])
    stream = residual_ref[...].astype(jnp.float32) + mixed.astype(jnp.bfloat16).astype(jnp.float32)
    stream_ref[...] = stream
    scale = lax.rsqrt(jnp.mean(stream * stream, axis=1, keepdims=True) + 1e-06)
    normed = (stream * scale * gain_ref[...]).astype(jnp.bfloat16)
    table = functools.reduce(jnp.logical_or, places(slots_ref[...], sent_refs[0].shape[0]))
    table = jnp.where(table, 1.0, 0.0).astype(jnp.bfloat16)
    at = 0
    for sent in sent_refs:
        cols = normed[:, at : at + sent.shape[1]]
        sent[...] = lax.dot_general(
            table, cols, (((0,), (0,)), ((), ())), preferred_element_type=jnp.float32
        ).astype(jnp.bfloat16)
        at += sent.shape[1]


def combine_body(stream_ref, slots_ref, weights_ref, *refs):
    *back_refs, out_ref = refs
    hits = places(slots_ref[...], back_refs[0].shape[0])
    table = sum(
        jnp.where(hit, weights_ref[:, m : m + 1], 0.0) for m, hit in enumerate(hits)
    )
    high = table.astype(jnp.bfloat16)
    low = (table - high.astype(jnp.float32)).astype(jnp.bfloat16)
    at = 0
    for back in back_refs:
        cols = slice(at, at + back.shape[1])
        rows = back[...]
        out_ref[:, cols] = (stream_ref[:, cols] + (dot(high, rows) + dot(low, rows))).astype(
            jnp.bfloat16
        )
        at += back.shape[1]


def fetch(copies, sems):
    started = [pltpu.make_async_copy(src, dst, sems.at[i]) for i, (src, dst) in enumerate(copies)]
    for c in started:
        c.start()
    return started


def hidden_of(rows, weights):
    act = dot(rows, weights)
    half = act.shape[1] // 2
    gate = act[:, :half]
    return (gate / (1.0 + jnp.exp(-gate)) * act[:, half:]).astype(jnp.bfloat16)


def near_body(n_rows, *refs):
    rows_in, quarters, (out_ref, rows_ref, w_ref, sems) = refs[:n_rows], refs[n_rows:-4], refs[-4:]
    width = quarters[0].shape[1]
    copies, at = [], 0
    for src in rows_in:
        copies.append((src, rows_ref.at[:, at : at + src.shape[1]]))
        at += src.shape[1]
    ends, i = [], 0
    for q in range(3):
        for kind in range(2):
            top = 0
            while top < w_ref.shape[1]:
                src = quarters[i]
                copies.append(
                    (src, w_ref.at[q, top : top + src.shape[0], kind * width : (kind + 1) * width])
                )
                top += src.shape[0]
                i += 1
        ends.append(len(copies))
    copies = fetch(copies, sems)
    done = 0
    for q in range(3):
        for c in copies[done : ends[q]]:
            c.wait()
        done = ends[q]
        out_ref[:, q * width : (q + 1) * width] = hidden_of(rows_ref[...], w_ref[q])


def near_hidden(rows, quarters):
    n, width = rows[0].shape[0], quarters[0].shape[1]
    d = sum(r.shape[1] for r in rows)
    n_copies = len(rows) + len(quarters)
    return pl.pallas_call(
        functools.partial(near_body, len(rows)),
        out_shape=jax.ShapeDtypeStruct((n, 3 * width), jnp.bfloat16),
        in_specs=[pl.BlockSpec(memory_space=pl.ANY)] * n_copies,
        out_specs=pl.BlockSpec(memory_space=pltpu.VMEM),
        scratch_shapes=[
            pltpu.VMEM((n, d), jnp.bfloat16),
            pltpu.VMEM((3, d, 2 * width), jnp.bfloat16),
            pltpu.SemaphoreType.DMA((n_copies,)),
        ],
        name="near_hidden",
    )(*rows, *quarters)


def far_body(n_rows, n_far, *refs):
    rows_in, far_in = refs[:n_rows], refs[n_rows : n_rows + n_far]
    near_ref, *downs = refs[n_rows + n_far : -6]
    out_ref, rows_ref, w_ref, hidden_ref, down_ref, sems = refs[-6:]
    width = far_in[0].shape[1]
    copies, at = [], 0
    for src in rows_in:
        copies.append((src, rows_ref.at[:, at : at + src.shape[1]]))
        at += src.shape[1]
    i = 0
    for kind in range(2):
        top = 0
        while top < w_ref.shape[0]:
            src = far_in[i]
            copies.append((src, w_ref.at[top : top + src.shape[0], kind * width : (kind + 1) * width]))
            top += src.shape[0]
            i += 1
    first = len(copies)
    copies.append((near_ref, hidden_ref.at[:, : 3 * width]))
    top = 0
    for src in downs:
        copies.append((src, down_ref.at[top : top + src.shape[0]]))
        top += src.shape[0]
    copies = fetch(copies, sems)
    for c in copies[:first]:
        c.wait()
    hidden_ref[:, 3 * width :] = hidden_of(rows_ref[...], w_ref[...])
    for c in copies[first:]:
        c.wait()
    out_ref[...] = dot(hidden_ref[...], down_ref[...]).astype(jnp.bfloat16)


def expert_rows(rows, far, near, downs):
    n, width, cols = rows[0].shape[0], far[0].shape[1], downs[0].shape[1]
    d = sum(r.shape[1] for r in rows)
    n_copies = len(rows) + len(far) + 1 + len(downs)
    return pl.pallas_call(
        functools.partial(far_body, len(rows), len(far)),
        out_shape=jax.ShapeDtypeStruct((n, cols), jnp.bfloat16),
        in_specs=[pl.BlockSpec(memory_space=pl.ANY)] * n_copies,
        out_specs=pl.BlockSpec(memory_space=pltpu.VMEM),
        scratch_shapes=[
            pltpu.VMEM((n, d), jnp.bfloat16),
            pltpu.VMEM((d, 2 * width), jnp.bfloat16),
            pltpu.VMEM((n, 4 * width), jnp.bfloat16),
            pltpu.VMEM((4 * width, cols), jnp.bfloat16),
            pltpu.SemaphoreType.DMA((n_copies,)),
        ],
        name="expert_rows",
    )(*rows, *far, near, *downs)


def gathered(shard):
    left, right = ring(shard, "tp", 1), ring(shard, "tp", -1)
    half = shard.shape[0] // 2
    far = ring(left[:half], "tp", 1), ring(right[half:], "tp", -1)
    return left, right, far


def shards(
    residual,
    conv_value,
    conv_gate,
    segments,
    conv_weight,
    norm_gain,
    norm_shift,
    out_weight,
    ffn_gain,
    routes,
    route_weights,
    w_gate,
    w_up,
    w_down,
):
    tok_dev, local_channels = conv_value.shape
    reach = conv_weight.shape[0] - 1
    gates = gathered(w_gate[0])
    ups = gathered(w_up[0])
    downs = gathered(w_down[0])
    tail = slice(tok_dev - reach, tok_dev)
    rim = (
        conv_value[tail].astype(jnp.float32) * jax.nn.sigmoid(conv_gate[tail].astype(jnp.float32))
    ).astype(jnp.bfloat16)
    named = jnp.pad(segments[tail].astype(jnp.bfloat16)[None], ((0, 1), (0, local_channels - reach)))
    rim = passed_along(jnp.concatenate([named, rim], 0), "sp", 1)
    seg_ext = jnp.concatenate([rim[0, :reach].astype(jnp.int32), segments], 0)
    seen = jnp.zeros((tok_dev,), jnp.int32)
    for offset in range(reach):
        seen = seen + (seg_ext[offset : offset + tok_dev] == segments).astype(jnp.int32)
    seen = jnp.broadcast_to(seen[:, None], (tok_dev, LANES))
    conv_out = conv_module(
        conv_value, conv_gate, rim, seen, conv_weight, norm_gain, norm_shift
    )
    columns = lax.axis_size("tp")
    column = lax.axis_index("tp")
    rows_own = tok_dev // columns
    regrouped = lax.all_to_all(
        conv_out.reshape(columns, rows_own, local_channels), "tp", 0, 0, tiled=True
    )
    experts_n = lax.axis_size("sp")
    top_count = routes.shape[1]
    model_width = residual.shape[1]
    capacity = max(2, 2 * tok_dev * top_count // (columns * experts_n))
    slot_total = experts_n * capacity
    own_routes = lax.dynamic_slice_in_dim(routes, column * rows_own, rows_own, 0)
    own_weights = lax.dynamic_slice_in_dim(route_weights, column * rows_own, rows_own, 0)
    own_slots = slot_numbers(own_routes, capacity, experts_n)
    stream, outgoing = pl.pallas_call(
        route_body,
        out_shape=(
            jax.ShapeDtypeStruct((rows_own, model_width), jnp.float32),
            jax.ShapeDtypeStruct((slot_total, model_width), jnp.bfloat16),
        ),
        name="project",
    )(regrouped, out_weight, residual, ffn_gain[None], own_slots)
    arrived = lax.all_to_all(
        outgoing.reshape(experts_n, capacity, model_width), "sp", 0, 0, tiled=True
    ).reshape(slot_total, model_width)
    near = near_hidden(
        [arrived], [w_gate[0], w_up[0], gates[0], ups[0], gates[1], ups[1]]
    )
    out = expert_rows(
        [arrived], [*gates[2], *ups[2]], near, [w_down[0], downs[0], downs[1], *downs[2]]
    )
    back = lax.all_to_all(
        out.reshape(experts_n, capacity, model_width), "sp", 0, 0, tiled=True
    ).reshape(slot_total, model_width)
    return pl.pallas_call(
        combine_body,
        out_shape=jax.ShapeDtypeStruct((rows_own, model_width), jnp.bfloat16),
        name="combine",
    )(stream, own_slots, own_weights, back)


def solution(mesh):
    return jax.shard_map(
        shards,
        mesh=mesh,
        in_specs=(
            P(("sp", "tp"), None),
            P("sp", "tp"),
            P("sp", "tp"),
            P("sp"),
            P(None, "tp"),
            P("tp"),
            P("tp"),
            P(),
            P(),
            P("sp", None),
            P("sp", None),
            P("sp", None, "tp"),
            P("sp", None, "tp"),
            P("sp", "tp", None),
        ),
        out_specs=P(("sp", "tp"), None),
        check_vma=False,
    )
```

```python
import functools

import jax
import jax.numpy as jnp
from jax import lax
from jax.experimental import pallas as pl
from jax.experimental.pallas import tpu as pltpu
from jax.sharding import PartitionSpec as P

TAPS = 31
RIM = 32
FIRST = 3
LANES = 128
BLOCK = 64


def passed_along(value, axis, steps):
    count = lax.axis_size(axis)
    initial, last = (max(0, -steps), min(count, count - steps))
    return lax.ppermute(value, axis, [(source, source + steps) for source in range(initial, last)])


def ring(value, axis, steps):
    count = lax.axis_size(axis)
    return lax.ppermute(value, axis, [(i, (i + steps) % count) for i in range(count)])


def slot_numbers(block_routes, capacity, experts_n):
    route_pairs = block_routes.reshape(block_routes.shape[:-2] + (-1,))
    onehot = (route_pairs[..., None] == jnp.arange(experts_n, dtype=jnp.int32)).astype(jnp.int32)
    slot_rank = jnp.sum((jnp.cumsum(onehot, axis=-2) - onehot) * onehot, axis=-1)
    return (route_pairs * capacity + slot_rank).reshape(block_routes.shape)


def kernel(body, out, args, scratch=(), limit=16, far_in=(), far_out=()):
    whole, far = pl.BlockSpec(memory_space=pltpu.VMEM), pl.BlockSpec(memory_space=pltpu.HBM)
    args = [
        pltpu.with_memory_space_constraint(a, pltpu.HBM if i in far_in else pltpu.VMEM)
        for i, a in enumerate(args)
    ]
    outs = out if isinstance(out, list) else [out]
    got = pl.pallas_call(
        body,
        out_shape=[
            pltpu.HBM(*o) if i in far_out else jax.ShapeDtypeStruct(*o) for i, o in enumerate(outs)
        ],
        in_specs=[far if i in far_in else whole for i in range(len(args))],
        out_specs=[far if i in far_out else whole for i in range(len(outs))],
        scratch_shapes=scratch,
        compiler_params=pltpu.CompilerParams(vmem_limit_bytes=limit << 20),
    )(*args)
    return got if isinstance(out, list) else got[0]


def fetch(copies, sems, first=0):
    started = [
        pltpu.make_async_copy(src, dst, sems.at[first + i]) for i, (src, dst) in enumerate(copies)
    ]
    for c in started:
        c.start()
    return started


def gated_rows(value, gate):
    return (value.astype(jnp.float32) * jax.nn.sigmoid(gate.astype(jnp.float32))).astype(jnp.bfloat16)


def rim_body(value_ref, gate_ref, segments_ref, out_ref):
    width = value_ref.shape[1]
    gated = gated_rows(value_ref[...], gate_ref[...]).astype(jnp.float32)
    last = segments_ref[segments_ref.shape[0] - 1 :, :].astype(jnp.float32)
    named = jnp.concatenate([last] + [jnp.zeros_like(last)] * (width // LANES - 1), axis=1)
    row = lax.broadcasted_iota(jnp.int32, gated.shape, 0)
    out_ref[...] = jnp.where(row == 0, named, gated).astype(jnp.bfloat16)


def rim_rows(value, gate, segments):
    tok, width = value.shape
    last = pl.BlockSpec((RIM, width), lambda i: (tok // RIM - 1, 0))
    return pl.pallas_call(
        rim_body,
        grid=(1,),
        in_specs=[last, last, pl.BlockSpec(segments.shape, lambda i: (0, 0))],
        out_specs=pl.BlockSpec((RIM, width), lambda i: (0, 0)),
        out_shape=jax.ShapeDtypeStruct((RIM, width), jnp.bfloat16),
        name="rim_rows",
    )(value, gate, segments)


def conv_body(value_ref, gate_ref, rim_ref, segments_ref, seen_ref, taps_ref, gain_ref, shift_ref, out_ref, rows_ref):
    tok = value_ref.shape[0]
    rows_ref[0, :RIM] = rim_ref[...].astype(jnp.float32)
    rows_ref[0, RIM:] = gated_rows(value_ref[...], gate_ref[...]).astype(jnp.float32)
    for r in range(1, 8):
        rows_ref[r, 8:] = rows_ref[0, 8 - r : RIM + tok - r]
    lane = lax.broadcasted_iota(jnp.int32, (1, LANES), 1)
    same = rim_ref[0:1, :LANES].astype(jnp.float32) == segments_ref[0:1, 0:1].astype(jnp.float32)
    same = jnp.where(same & (lane >= LANES - (TAPS - 1)), 1.0, 0.0)
    before = jnp.sum(same, axis=1, keepdims=True).astype(jnp.int32)

    def block(i, carry):
        at = pl.multiple_of(i * BLOCK, BLOCK)
        seen = seen_ref[pl.ds(at, BLOCK), :]
        row = at + lax.broadcasted_iota(jnp.int32, (BLOCK, LANES), 0)
        seen = jnp.where(seen == row, seen + before, seen)
        for lane in range(0, value_ref.shape[1], LANES):
            cols = slice(lane, lane + LANES)
            total = rows_ref[0, pl.ds(at + RIM, BLOCK), cols] * taps_ref[TAPS - 1 : TAPS, cols]
            for back in range(1, TAPS):
                tap = TAPS - 1 - back
                rows = rows_ref[back % 8, pl.ds(at + RIM - back // 8 * 8, BLOCK), cols]
                total = total + jnp.where(seen >= back, rows * taps_ref[tap : tap + 1, cols], 0.0)
            dev = total - jnp.mean(total, axis=1, keepdims=True)
            var = jnp.mean(dev * dev, axis=1, keepdims=True)
            v = dev * lax.rsqrt(var + 1e-05) * gain_ref[:, cols] + shift_ref[:, cols]
            out_ref[pl.ds(at, BLOCK), cols] = (v / (1.0 + jnp.exp(-v))).astype(jnp.bfloat16)
        return carry

    lax.fori_loop(0, tok // BLOCK, block, 0)


def conv_module(value, gate, rim, segments, seen, taps, gain, shift):
    tok, width = value.shape
    return kernel(
        conv_body,
        ((tok, width), jnp.bfloat16),
        (value, gate, rim, segments, seen, taps, gain[None], shift[None]),
        scratch=[pltpu.VMEM((8, RIM + tok, width), jnp.float32)],
    )


def dot(a, b):
    return jnp.dot(a, b, preferred_element_type=jnp.float32)


def places(slots, total):
    numbers = lax.broadcasted_iota(jnp.int32, (slots.shape[0], total), 1)
    return [numbers == slots[:, m : m + 1] for m in range(slots.shape[1])]


def route_body(
    parts_ref, residual_ref, gain_ref, slots_ref, weight_ref, stream_out, sent_out, w_ref, stream_ref, sent_ref, sems
):
    parts_n, _, width = parts_ref.shape
    spans = [slice(j * width, (j + 1) * width) for j in range(parts_n)]
    loads = fetch([(weight_ref.at[rows], w_ref.at[rows]) for rows in spans], sems)
    table = functools.reduce(jnp.logical_or, places(slots_ref[...], sent_ref.shape[0]))
    table = jnp.where(table, 1.0, 0.0).astype(jnp.bfloat16)
    for j, rows in enumerate(spans):
        loads[j].wait()
        part = dot(parts_ref[j], w_ref[rows])
        stream_ref[...] = part if j == 0 else stream_ref[...] + part
    mixed = stream_ref[...].astype(jnp.bfloat16).astype(jnp.float32)
    stream = residual_ref[...].astype(jnp.float32) + mixed
    stream_ref[...] = stream
    stores = fetch([(stream_ref, stream_out)], sems, parts_n)
    scale = lax.rsqrt(jnp.mean(stream * stream, axis=1, keepdims=True) + 1e-06)
    normed = (stream * scale * gain_ref[...]).astype(jnp.bfloat16)
    step = normed.shape[1] // 4
    for j in range(4):
        cols = slice(j * step, (j + 1) * step)
        sent_ref[:, cols] = lax.dot_general(
            table, normed[:, cols], (((0,), (0,)), ((), ())), preferred_element_type=jnp.float32
        ).astype(jnp.bfloat16)
        stores += fetch([(sent_ref.at[:, cols], sent_out.at[:, cols])], sems, parts_n + 1 + j)
    for c in stores:
        c.wait()


def combine_body(stream_in, slots_ref, weights_ref, *refs):
    *back_refs, out, stream_ref, out_ref, sems = refs
    (load,) = fetch([(stream_in, stream_ref)], sems)
    hits = places(slots_ref[...], back_refs[0].shape[0])
    table = sum(jnp.where(hit, weights_ref[:, m : m + 1], 0.0) for m, hit in enumerate(hits))
    high = table.astype(jnp.bfloat16)
    low = (table - high.astype(jnp.float32)).astype(jnp.bfloat16)
    load.wait()
    at, stores = 0, []
    for i, back in enumerate(back_refs):
        cols = slice(at, at + back.shape[1])
        rows = back[...]
        mixed = dot(high, rows) + dot(low, rows)
        out_ref[:, cols] = (stream_ref[:, cols] + mixed).astype(jnp.bfloat16)
        stores += fetch([(out_ref.at[:, cols], out.at[:, cols])], sems, 1 + i)
        at += back.shape[1]
    for c in stores:
        c.wait()


def hidden_body(counts, *refs):
    rows_in, *pieces, out_ref, rows_ref, w_ref, sems = refs
    width = pieces[0].shape[1]
    (load,) = fetch([(rows_in, rows_ref)], sems, len(pieces))
    loads = []
    for q, kinds in enumerate(counts):
        copies = []
        for kind, n in enumerate(kinds):
            top = 0
            for piece in pieces[:n]:
                end = top + piece.shape[0]
                copies.append((piece, w_ref.at[q, top:end, kind * width : (kind + 1) * width]))
                top = end
            pieces = pieces[n:]
        loads.append(fetch(copies, sems, sum(len(c) for c in loads)))
    load.wait()
    for q, copies in enumerate(loads):
        for c in copies:
            c.wait()
        act = dot(rows_ref[...], w_ref[q])
        gate = act[:, :width]
        hidden = gate / (1.0 + jnp.exp(-gate)) * act[:, width:]
        out_ref[:, q * width : (q + 1) * width] = hidden.astype(jnp.bfloat16)


def hidden_units(rows, quarters):
    counts = tuple((len(gates), len(ups)) for gates, ups in quarters)
    pieces = [p for gates, ups in quarters for p in (*gates, *ups)]
    (n, d), width = rows.shape, pieces[0].shape[1]
    return kernel(
        functools.partial(hidden_body, counts),
        ((n, width * len(counts)), jnp.bfloat16),
        (rows, *pieces),
        scratch=[
            pltpu.VMEM((n, d), jnp.bfloat16),
            pltpu.VMEM((len(counts), d, 2 * width), jnp.bfloat16),
            pltpu.SemaphoreType.DMA((len(pieces) + 1,)),
        ],
        limit=20,
        far_in=range(1 + len(pieces)),
    )


def down_body(cols, hidden_ref, own_ref, *refs):
    *pieces, out, down_ref, out_ref, sems = refs
    at = own_ref.shape[0]
    down_ref[:at] = own_ref[:, cols]
    for piece in pieces:
        down_ref[at : at + piece.shape[0]] = piece[...]
        at += piece.shape[0]
    half = out_ref.shape[1] // 2
    stores = []
    for i in range(2):
        span = slice(i * half, (i + 1) * half)
        out_ref[:, span] = dot(hidden_ref[...], down_ref[:, span]).astype(jnp.bfloat16)
        stores += fetch([(out_ref.at[:, span], out.at[:, span])], sems, i)
    for c in stores:
        c.wait()


def down_rows(hidden, own, pieces, cols):
    n, width = hidden.shape[0], cols.stop - cols.start
    return kernel(
        functools.partial(down_body, cols),
        ((n, width), jnp.bfloat16),
        (hidden, own, *pieces),
        scratch=[
            pltpu.VMEM((hidden.shape[1], width), jnp.bfloat16),
            pltpu.VMEM((n, width), jnp.bfloat16),
            pltpu.SemaphoreType.DMA((2,)),
        ],
        limit=16,
        far_out=(0,),
    )


def gathered(shard, parts):
    half = shard.shape[0] // 2
    pieces = [shard] if parts == 1 else [shard[:half], shard[half:]]
    left, right = [], []
    for piece in pieces:
        left.append(ring(piece, "tp", 1))
        right.append(ring(piece, "tp", -1))
    far = [ring(left[0][:half], "tp", 1), ring(right[-1][-half:], "tp", -1)]
    return left, right, far


def shards(
    residual,
    conv_value,
    conv_gate,
    segments,
    conv_weight,
    norm_gain,
    norm_shift,
    out_weight,
    ffn_gain,
    routes,
    route_weights,
    w_gate,
    w_up,
    w_down,
):
    tok_dev, local_channels = conv_value.shape
    reach = conv_weight.shape[0] - 1
    model_width = w_down.shape[2]
    gates = gathered(w_gate[0], 2)
    ups = gathered(w_up[0], 1)
    cut = model_width * FIRST // 8
    groups = slice(0, cut), slice(cut, model_width)
    downs = [gathered(w_down[0][:, cols], 1) for cols in groups]
    lines = segments.reshape(tok_dev // LANES, LANES)
    rim = passed_along(rim_rows(conv_value, conv_gate, lines), "sp", 1)
    padded = jnp.pad(segments, (reach, 0), constant_values=-1)
    seen = jnp.zeros((tok_dev,), jnp.int32)
    for offset in range(reach):
        seen = seen + (padded[offset : offset + tok_dev] == segments).astype(jnp.int32)
    seen = jnp.broadcast_to(seen[:, None], (tok_dev, LANES))
    conv_out = conv_module(
        conv_value, conv_gate, rim, lines, seen, conv_weight, norm_gain, norm_shift
    )
    columns = lax.axis_size("tp")
    column = lax.axis_index("tp")
    rows_own = tok_dev // columns
    regrouped = lax.all_to_all(
        conv_out.reshape(columns, rows_own, local_channels), "tp", 0, 0, tiled=True
    )
    experts_n = lax.axis_size("sp")
    top_count = routes.shape[1]
    capacity = max(2, 2 * tok_dev * top_count // (columns * experts_n))
    slot_total = experts_n * capacity
    own_routes = lax.dynamic_slice_in_dim(routes, column * rows_own, rows_own, 0)
    own_weights = lax.dynamic_slice_in_dim(route_weights, column * rows_own, rows_own, 0)
    own_slots = slot_numbers(own_routes, capacity, experts_n)
    stream, outgoing = kernel(
        route_body,
        [((rows_own, model_width), jnp.float32), ((slot_total, model_width), jnp.bfloat16)],
        (regrouped, residual, ffn_gain[None], own_slots, out_weight),
        scratch=[
            pltpu.VMEM(out_weight.shape, jnp.bfloat16),
            pltpu.VMEM((rows_own, model_width), jnp.float32),
            pltpu.VMEM((slot_total, model_width), jnp.bfloat16),
            pltpu.SemaphoreType.DMA((columns + 5,)),
        ],
        limit=24,
        far_in=(4,),
        far_out=(0, 1),
    )
    arrived = lax.all_to_all(
        outgoing.reshape(experts_n, capacity, model_width), "sp", 0, 0, tiled=True
    ).reshape(slot_total, model_width)
    hidden = hidden_units(
        arrived,
        [([w_gate[0]], [w_up[0]])] + [(gates[side], ups[side]) for side in range(3)],
    )
    back = []
    for cols, (left, right, far) in zip(groups, downs):
        out = down_rows(hidden, w_down[0], [*left, *right, *far], cols)
        back.append(
            lax.all_to_all(
                out.reshape(experts_n, capacity, -1), "sp", 0, 0, tiled=True
            ).reshape(slot_total, -1)
        )
    return kernel(
        combine_body,
        ((rows_own, model_width), jnp.bfloat16),
        (stream, own_slots, own_weights, *back),
        scratch=[
            pltpu.VMEM((rows_own, model_width), jnp.float32),
            pltpu.VMEM((rows_own, model_width), jnp.bfloat16),
            pltpu.SemaphoreType.DMA((1 + len(back),)),
        ],
        limit=24,
        far_in=(0,),
        far_out=(0,),
    )


def solution(mesh):
    return jax.shard_map(
        shards,
        mesh=mesh,
        in_specs=(
            P(("sp", "tp"), None),
            P("sp", "tp"),
            P("sp", "tp"),
            P("sp"),
            P(None, "tp"),
            P("tp"),
            P("tp"),
            P(),
            P(),
            P("sp", None),
            P("sp", None),
            P("sp", None, "tp"),
            P("sp", None, "tp"),
            P("sp", "tp", None),
        ),
        out_specs=P(("sp", "tp"), None),
        check_vma=False,
    )
```

```python
import functools

import jax
import jax.numpy as jnp
from jax import lax
from jax.experimental import pallas as pl
from jax.experimental.pallas import tpu as pltpu
from jax.sharding import PartitionSpec as P

TAPS = 31
RIM = 32
FIRST = 2
LANES = 128
BLOCK = 64


def passed_along(value, axis, steps):
    count = lax.axis_size(axis)
    initial, last = (max(0, -steps), min(count, count - steps))
    return lax.ppermute(value, axis, [(source, source + steps) for source in range(initial, last)])


def ring(value, axis, steps):
    count = lax.axis_size(axis)
    return lax.ppermute(value, axis, [(i, (i + steps) % count) for i in range(count)])


def kernel(body, out, args, scratch=(), limit=16, far_in=(), far_out=()):
    whole, far = pl.BlockSpec(memory_space=pltpu.VMEM), pl.BlockSpec(memory_space=pltpu.HBM)
    args = [
        pltpu.with_memory_space_constraint(a, pltpu.HBM if i in far_in else pltpu.VMEM)
        for i, a in enumerate(args)
    ]
    outs = out if isinstance(out, list) else [out]
    got = pl.pallas_call(
        body,
        out_shape=[
            pltpu.HBM(*o) if i in far_out else jax.ShapeDtypeStruct(*o) for i, o in enumerate(outs)
        ],
        in_specs=[far if i in far_in else whole for i in range(len(args))],
        out_specs=[far if i in far_out else whole for i in range(len(outs))],
        scratch_shapes=scratch,
        compiler_params=pltpu.CompilerParams(vmem_limit_bytes=limit << 20),
    )(*args)
    return got if isinstance(out, list) else got[0]


def fetch(copies, sems, first=0):
    started = [
        pltpu.make_async_copy(src, dst, sems.at[first + i]) for i, (src, dst) in enumerate(copies)
    ]
    for c in started:
        c.start()
    return started


def gated_rows(value, gate):
    return (value.astype(jnp.float32) * jax.nn.sigmoid(gate.astype(jnp.float32))).astype(jnp.bfloat16)


def rim_body(value_ref, gate_ref, segments_ref, out_ref):
    width = value_ref.shape[1]
    gated = gated_rows(value_ref[...], gate_ref[...]).astype(jnp.float32)
    last = segments_ref[segments_ref.shape[0] - 1 :, :].astype(jnp.float32)
    named = jnp.concatenate([last] + [jnp.zeros_like(last)] * (width // LANES - 1), axis=1)
    row = lax.broadcasted_iota(jnp.int32, gated.shape, 0)
    out_ref[...] = jnp.where(row == 0, named, gated).astype(jnp.bfloat16)


def rim_rows(value, gate, segments):
    tok, width = value.shape
    last = pl.BlockSpec((RIM, width), lambda i: (tok // RIM - 1, 0))
    return pl.pallas_call(
        rim_body,
        grid=(1,),
        in_specs=[last, last, pl.BlockSpec(segments.shape, lambda i: (0, 0))],
        out_specs=pl.BlockSpec((RIM, width), lambda i: (0, 0)),
        out_shape=jax.ShapeDtypeStruct((RIM, width), jnp.bfloat16),
        name="rim_rows",
    )(value, gate, segments)


def conv_body(value_ref, gate_ref, rim_ref, segments_ref, seen_ref, taps_ref, gain_ref, shift_ref, out_ref, rows_ref):
    tok = value_ref.shape[0]
    rows_ref[0, :RIM] = rim_ref[...].astype(jnp.float32)
    rows_ref[0, RIM:] = gated_rows(value_ref[...], gate_ref[...]).astype(jnp.float32)
    for r in range(1, 8):
        rows_ref[r, 8:] = rows_ref[0, 8 - r : RIM + tok - r]
    lane = lax.broadcasted_iota(jnp.int32, (1, LANES), 1)
    same = rim_ref[0:1, :LANES].astype(jnp.float32) == segments_ref[0:1, 0:1].astype(jnp.float32)
    same = jnp.where(same & (lane >= LANES - (TAPS - 1)), 1.0, 0.0)
    before = jnp.sum(same, axis=1, keepdims=True).astype(jnp.int32)

    def block(i, carry):
        at = pl.multiple_of(i * BLOCK, BLOCK)
        seen = seen_ref[pl.ds(at, BLOCK), :]
        row = at + lax.broadcasted_iota(jnp.int32, (BLOCK, LANES), 0)
        seen = jnp.where(seen == row, seen + before, seen)
        for lane in range(0, value_ref.shape[1], LANES):
            cols = slice(lane, lane + LANES)
            total = rows_ref[0, pl.ds(at + RIM, BLOCK), cols] * taps_ref[TAPS - 1 : TAPS, cols]
            for back in range(1, TAPS):
                tap = TAPS - 1 - back
                rows = rows_ref[back % 8, pl.ds(at + RIM - back // 8 * 8, BLOCK), cols]
                total = total + jnp.where(seen >= back, rows * taps_ref[tap : tap + 1, cols], 0.0)
            dev = total - jnp.mean(total, axis=1, keepdims=True)
            var = jnp.mean(dev * dev, axis=1, keepdims=True)
            v = dev * lax.rsqrt(var + 1e-05) * gain_ref[:, cols] + shift_ref[:, cols]
            out_ref[pl.ds(at, BLOCK), cols] = (v / (1.0 + jnp.exp(-v))).astype(jnp.bfloat16)
        return carry

    lax.fori_loop(0, tok // BLOCK, block, 0)


def conv_module(value, gate, rim, segments, seen, taps, gain, shift):
    tok, width = value.shape
    return kernel(
        conv_body,
        ((tok, width), jnp.bfloat16),
        (value, gate, rim, segments, seen, taps, gain[None], shift[None]),
        scratch=[pltpu.VMEM((8, RIM + tok, width), jnp.float32)],
    )


def dot(a, b):
    return jnp.dot(a, b, preferred_element_type=jnp.float32)


def places(routes, experts_n, capacity):
    rows, top_count = routes.shape
    expert = lax.broadcasted_iota(jnp.int32, (rows, experts_n), 1)
    named = [jnp.where(expert == routes[:, m : m + 1], 1.0, 0.0) for m in range(top_count)]
    earlier = lax.broadcasted_iota(jnp.int32, (rows, rows), 0) > lax.broadcasted_iota(
        jnp.int32, (rows, rows), 1
    )
    earlier = jnp.where(earlier, 1.0, 0.0).astype(jnp.bfloat16)
    taken = dot(earlier, sum(named).astype(jnp.bfloat16))
    number = lax.broadcasted_iota(jnp.int32, (rows, experts_n * capacity), 1)
    found = []
    for m in range(top_count):
        rank = jnp.sum(named[m] * taken, axis=1, keepdims=True).astype(jnp.int32)
        found.append(number == routes[:, m : m + 1] * capacity + rank)
    return found


def route_body(
    experts_n, parts_ref, residual_ref, gain_ref, routes_ref, weight_ref, stream_out, sent_out, w_ref, stream_ref, sent_ref, sems
):
    parts_n, _, width = parts_ref.shape
    spans = [slice(j * width, (j + 1) * width) for j in range(parts_n)]
    loads = fetch([(weight_ref.at[rows], w_ref.at[rows]) for rows in spans], sems)
    found = places(routes_ref[...], experts_n, sent_ref.shape[0] // experts_n)
    table = functools.reduce(jnp.logical_or, found)
    table = jnp.where(table, 1.0, 0.0).astype(jnp.bfloat16)
    for j, rows in enumerate(spans):
        loads[j].wait()
        part = dot(parts_ref[j], w_ref[rows])
        stream_ref[...] = part if j == 0 else stream_ref[...] + part
    mixed = stream_ref[...].astype(jnp.bfloat16).astype(jnp.float32)
    stream = residual_ref[...].astype(jnp.float32) + mixed
    stream_ref[...] = stream
    stores = fetch([(stream_ref, stream_out)], sems, parts_n)
    scale = lax.rsqrt(jnp.mean(stream * stream, axis=1, keepdims=True) + 1e-06)
    normed = (stream * scale * gain_ref[...]).astype(jnp.bfloat16)
    step = normed.shape[1] // 4
    for j in range(4):
        cols = slice(j * step, (j + 1) * step)
        sent_ref[:, cols] = lax.dot_general(
            table, normed[:, cols], (((0,), (0,)), ((), ())), preferred_element_type=jnp.float32
        ).astype(jnp.bfloat16)
        stores += fetch([(sent_ref.at[:, cols], sent_out.at[:, cols])], sems, parts_n + 1 + j)
    for c in stores:
        c.wait()


def combine_body(experts_n, stream_in, routes_ref, weights_ref, *refs):
    *back_refs, out, stream_ref, out_ref, sems = refs
    (load,) = fetch([(stream_in, stream_ref)], sems)
    found = places(routes_ref[...], experts_n, back_refs[0].shape[0] // experts_n)
    table = sum(jnp.where(hit, weights_ref[:, m : m + 1], 0.0) for m, hit in enumerate(found))
    high = table.astype(jnp.bfloat16)
    low = (table - high.astype(jnp.float32)).astype(jnp.bfloat16)
    load.wait()
    at, stores = 0, []
    for i, back in enumerate(back_refs):
        cols = slice(at, at + back.shape[1])
        rows = back[...]
        mixed = dot(high, rows) + dot(low, rows)
        out_ref[:, cols] = (stream_ref[:, cols] + mixed).astype(jnp.bfloat16)
        stores += fetch([(out_ref.at[:, cols], out.at[:, cols])], sems, 1 + i)
        at += back.shape[1]
    for c in stores:
        c.wait()


def experts_body(counts, cols, *refs):
    rows_in, *pieces, hidden_out, out, rows_ref, w_ref, hidden_ref, down_ref, out_ref, sems = refs
    width = pieces[0].shape[1]
    (load,) = fetch([(rows_in, rows_ref)], sems)
    loads, at = [], 1
    for q, kinds in enumerate(counts):
        copies = []
        for kind, n in enumerate(kinds):
            top = 0
            for piece in pieces[:n]:
                end = top + piece.shape[0]
                copies.append((piece, w_ref.at[q, top:end, kind * width : (kind + 1) * width]))
                top = end
            pieces = pieces[n:]
        loads.append(fetch(copies, sems, at))
        at += len(copies)
    copies, top = [], 0
    for piece in pieces:
        src = piece.at[:, cols] if top == 0 else piece
        copies.append((src, down_ref.at[top : top + piece.shape[0]]))
        top += piece.shape[0]
    downs = fetch(copies, sems, at)
    load.wait()
    for q, copies in enumerate(loads):
        for c in copies:
            c.wait()
        act = dot(rows_ref[...], w_ref[q])
        gate = act[:, :width]
        hidden = gate / (1.0 + jnp.exp(-gate)) * act[:, width:]
        hidden_ref[:, q * width : (q + 1) * width] = hidden.astype(jnp.bfloat16)
    stores = fetch([(hidden_ref, hidden_out)], sems)
    for c in downs:
        c.wait()
    out_ref[...] = dot(hidden_ref[...], down_ref[...]).astype(jnp.bfloat16)
    stores += fetch([(out_ref, out)], sems, 1)
    for c in stores:
        c.wait()


def expert_rows(rows, quarters, downs, cols):
    counts = tuple((len(gates), len(ups)) for gates, ups in quarters)
    pieces = [p for gates, ups in quarters for p in (*gates, *ups)] + downs
    (n, d), width, out_width = rows.shape, pieces[0].shape[1], cols.stop - cols.start
    units = width * len(counts)
    return kernel(
        functools.partial(experts_body, counts, cols),
        [((n, units), jnp.bfloat16), ((n, out_width), jnp.bfloat16)],
        (rows, *pieces),
        scratch=[
            pltpu.VMEM((n, d), jnp.bfloat16),
            pltpu.VMEM((len(counts), d, 2 * width), jnp.bfloat16),
            pltpu.VMEM((n, units), jnp.bfloat16),
            pltpu.VMEM((units, out_width), jnp.bfloat16),
            pltpu.VMEM((n, out_width), jnp.bfloat16),
            pltpu.SemaphoreType.DMA((len(pieces) + 1,)),
        ],
        limit=22,
        far_in=range(1 + len(pieces)),
        far_out=(0, 1),
    )


def down_body(cols, hidden_ref, own_ref, *refs):
    *pieces, out, down_ref, out_ref, sems = refs
    at = own_ref.shape[0]
    down_ref[:at] = own_ref[:, cols]
    for piece in pieces:
        down_ref[at : at + piece.shape[0]] = piece[...]
        at += piece.shape[0]
    half = out_ref.shape[1] // 2
    stores = []
    for i in range(2):
        span = slice(i * half, (i + 1) * half)
        out_ref[:, span] = dot(hidden_ref[...], down_ref[:, span]).astype(jnp.bfloat16)
        stores += fetch([(out_ref.at[:, span], out.at[:, span])], sems, i)
    for c in stores:
        c.wait()


def down_rows(hidden, own, pieces, cols):
    n, width = hidden.shape[0], cols.stop - cols.start
    return kernel(
        functools.partial(down_body, cols),
        ((n, width), jnp.bfloat16),
        (hidden, own, *pieces),
        scratch=[
            pltpu.VMEM((hidden.shape[1], width), jnp.bfloat16),
            pltpu.VMEM((n, width), jnp.bfloat16),
            pltpu.SemaphoreType.DMA((2,)),
        ],
        limit=16,
        far_out=(0,),
    )


def gathered(shard, parts):
    half = shard.shape[0] // 2
    pieces = [shard] if parts == 1 else [shard[:half], shard[half:]]
    left, right = [], []
    for piece in pieces:
        left.append(ring(piece, "tp", 1))
        right.append(ring(piece, "tp", -1))
    far = [ring(left[0][:half], "tp", 1), ring(right[-1][-half:], "tp", -1)]
    return left, right, far


def shards(
    residual,
    conv_value,
    conv_gate,
    segments,
    conv_weight,
    norm_gain,
    norm_shift,
    out_weight,
    ffn_gain,
    routes,
    route_weights,
    w_gate,
    w_up,
    w_down,
):
    tok_dev, local_channels = conv_value.shape
    reach = conv_weight.shape[0] - 1
    model_width = w_down.shape[2]
    gates = gathered(w_gate[0], 2)
    ups = gathered(w_up[0], 1)
    cut = model_width * FIRST // 8
    groups = slice(0, cut), slice(cut, model_width)
    downs = [gathered(w_down[0][:, cols], 1) for cols in groups]
    lines = segments.reshape(tok_dev // LANES, LANES)
    rim = passed_along(rim_rows(conv_value, conv_gate, lines), "sp", 1)
    padded = jnp.pad(segments, (reach, 0), constant_values=-1)
    seen = jnp.zeros((tok_dev,), jnp.int32)
    for offset in range(reach):
        seen = seen + (padded[offset : offset + tok_dev] == segments).astype(jnp.int32)
    seen = jnp.broadcast_to(seen[:, None], (tok_dev, LANES))
    conv_out = conv_module(
        conv_value, conv_gate, rim, lines, seen, conv_weight, norm_gain, norm_shift
    )
    columns = lax.axis_size("tp")
    column = lax.axis_index("tp")
    rows_own = tok_dev // columns
    regrouped = lax.all_to_all(
        conv_out.reshape(columns, rows_own, local_channels), "tp", 0, 0, tiled=True
    )
    experts_n = lax.axis_size("sp")
    top_count = routes.shape[1]
    capacity = max(2, 2 * tok_dev * top_count // (columns * experts_n))
    slot_total = experts_n * capacity
    own_routes = lax.dynamic_slice_in_dim(routes, column * rows_own, rows_own, 0)
    own_weights = lax.dynamic_slice_in_dim(route_weights, column * rows_own, rows_own, 0)
    stream, outgoing = kernel(
        functools.partial(route_body, experts_n),
        [((rows_own, model_width), jnp.float32), ((slot_total, model_width), jnp.bfloat16)],
        (regrouped, residual, ffn_gain[None], own_routes, out_weight),
        scratch=[
            pltpu.VMEM(out_weight.shape, jnp.bfloat16),
            pltpu.VMEM((rows_own, model_width), jnp.float32),
            pltpu.VMEM((slot_total, model_width), jnp.bfloat16),
            pltpu.SemaphoreType.DMA((columns + 5,)),
        ],
        limit=24,
        far_in=(4,),
        far_out=(0, 1),
    )
    arrived = lax.all_to_all(
        outgoing.reshape(experts_n, capacity, model_width), "sp", 0, 0, tiled=True
    ).reshape(slot_total, model_width)

    def returned(out):
        return lax.all_to_all(
            out.reshape(experts_n, capacity, -1), "sp", 0, 0, tiled=True
        ).reshape(slot_total, -1)

    first, second = ([w_down[0], *left, *right, *far] for left, right, far in downs)
    quarters = [([w_gate[0]], [w_up[0]])] + [(gates[side], ups[side]) for side in range(3)]
    hidden, out = expert_rows(arrived, quarters, first, groups[0])
    back = [returned(out)]
    out = down_rows(hidden, second[0], second[1:], groups[1])
    back.append(returned(out))
    return kernel(
        functools.partial(combine_body, experts_n),
        ((rows_own, model_width), jnp.bfloat16),
        (stream, own_routes, own_weights, *back),
        scratch=[
            pltpu.VMEM((rows_own, model_width), jnp.float32),
            pltpu.VMEM((rows_own, model_width), jnp.bfloat16),
            pltpu.SemaphoreType.DMA((1 + len(back),)),
        ],
        limit=24,
        far_in=(0,),
        far_out=(0,),
    )


def solution(mesh):
    return jax.shard_map(
        shards,
        mesh=mesh,
        in_specs=(
            P(("sp", "tp"), None),
            P("sp", "tp"),
            P("sp", "tp"),
            P("sp"),
            P(None, "tp"),
            P("tp"),
            P("tp"),
            P(),
            P(),
            P("sp", None),
            P("sp", None),
            P("sp", None, "tp"),
            P("sp", None, "tp"),
            P("sp", "tp", None),
        ),
        out_specs=P(("sp", "tp"), None),
        check_vma=False,
    )
```

```python
import functools

import jax
import jax.numpy as jnp
from jax import lax
from jax.experimental import pallas as pl
from jax.experimental.pallas import tpu as pltpu
from jax.sharding import PartitionSpec as P

TAPS = 31
RIM = 32
FIRST = 3
LANES = 128
BLOCK = 64


def passed_along(value, axis, steps):
    count = lax.axis_size(axis)
    initial, last = (max(0, -steps), min(count, count - steps))
    return lax.ppermute(value, axis, [(source, source + steps) for source in range(initial, last)])


def ring(value, axis, steps):
    count = lax.axis_size(axis)
    return lax.ppermute(value, axis, [(i, (i + steps) % count) for i in range(count)])


def kernel(body, out, args, scratch=(), limit=16, far_in=(), far_out=()):
    whole, far = pl.BlockSpec(memory_space=pltpu.VMEM), pl.BlockSpec(memory_space=pltpu.HBM)
    args = [
        pltpu.with_memory_space_constraint(a, pltpu.HBM if i in far_in else pltpu.VMEM)
        for i, a in enumerate(args)
    ]
    outs = out if isinstance(out, list) else [out]
    got = pl.pallas_call(
        body,
        out_shape=[
            pltpu.HBM(*o) if i in far_out else jax.ShapeDtypeStruct(*o) for i, o in enumerate(outs)
        ],
        in_specs=[far if i in far_in else whole for i in range(len(args))],
        out_specs=[far if i in far_out else whole for i in range(len(outs))],
        scratch_shapes=scratch,
        compiler_params=pltpu.CompilerParams(vmem_limit_bytes=limit << 20),
    )(*args)
    return got if isinstance(out, list) else got[0]


def fetch(copies, sems, first=0):
    started = [
        pltpu.make_async_copy(src, dst, sems.at[first + i]) for i, (src, dst) in enumerate(copies)
    ]
    for c in started:
        c.start()
    return started


def gated_rows(value, gate):
    return (value.astype(jnp.float32) * jax.nn.sigmoid(gate.astype(jnp.float32))).astype(jnp.bfloat16)


def rim_body(value_in, gate_in, segments_ref, w_gate_in, w_up_in, out_ref, head_out, tail_out, value_ref, gate_ref, sems):
    tok, width = value_in.shape
    deep, cut = w_gate_in.shape[0], head_out.shape[0]
    loads = fetch(
        [(value_in.at[tok - RIM :], value_ref), (gate_in.at[tok - RIM :], gate_ref)], sems
    )
    packs = fetch(
        [
            (w_gate_in.at[:cut], head_out),
            (w_gate_in.at[cut:], tail_out.at[: deep - cut]),
            (w_up_in, tail_out.at[deep - cut :]),
        ],
        sems,
        2,
    )
    for c in loads:
        c.wait()
    gated = gated_rows(value_ref[...], gate_ref[...]).astype(jnp.float32)
    last = segments_ref[segments_ref.shape[0] - 1 :, :].astype(jnp.float32)
    named = jnp.concatenate([last] + [jnp.zeros_like(last)] * (width // LANES - 1), axis=1)
    row = lax.broadcasted_iota(jnp.int32, gated.shape, 0)
    out_ref[...] = jnp.where(row == 0, named, gated).astype(jnp.bfloat16)
    for c in packs:
        c.wait()


def rim_and_packs(value, gate, segments, w_gate, w_up):
    width = value.shape[1]
    deep, wide = w_gate.shape
    return kernel(
        rim_body,
        [
            ((RIM, width), jnp.bfloat16),
            ((deep // 2, wide), jnp.bfloat16),
            ((deep - deep // 2 + w_up.shape[0], wide), jnp.bfloat16),
        ],
        (value, gate, segments, w_gate, w_up),
        scratch=[
            pltpu.VMEM((RIM, width), jnp.bfloat16),
            pltpu.VMEM((RIM, width), jnp.bfloat16),
            pltpu.SemaphoreType.DMA((5,)),
        ],
        limit=8,
        far_in=(0, 1, 3, 4),
        far_out=(1, 2),
    )


def conv_body(value_ref, gate_ref, rim_ref, segments_ref, seen_ref, taps_ref, gain_ref, shift_ref, out_ref, rows_ref):
    tok = value_ref.shape[0]
    rows_ref[0, :RIM] = rim_ref[...].astype(jnp.float32)
    rows_ref[0, RIM:] = gated_rows(value_ref[...], gate_ref[...]).astype(jnp.float32)
    for r in range(1, 8):
        rows_ref[r, 8:] = rows_ref[0, 8 - r : RIM + tok - r]
    lane = lax.broadcasted_iota(jnp.int32, (1, LANES), 1)
    same = rim_ref[0:1, :LANES].astype(jnp.float32) == segments_ref[0:1, 0:1].astype(jnp.float32)
    same = jnp.where(same & (lane >= LANES - (TAPS - 1)), 1.0, 0.0)
    before = jnp.sum(same, axis=1, keepdims=True).astype(jnp.int32)

    def block(i, carry):
        at = pl.multiple_of(i * BLOCK, BLOCK)
        seen = seen_ref[pl.ds(at, BLOCK), :]
        row = at + lax.broadcasted_iota(jnp.int32, (BLOCK, LANES), 0)
        seen = jnp.where(seen == row, seen + before, seen)
        for lane in range(0, value_ref.shape[1], LANES):
            cols = slice(lane, lane + LANES)
            total = rows_ref[0, pl.ds(at + RIM, BLOCK), cols] * taps_ref[TAPS - 1 : TAPS, cols]
            for back in range(1, TAPS):
                tap = TAPS - 1 - back
                rows = rows_ref[back % 8, pl.ds(at + RIM - back // 8 * 8, BLOCK), cols]
                total = total + jnp.where(seen >= back, rows * taps_ref[tap : tap + 1, cols], 0.0)
            dev = total - jnp.mean(total, axis=1, keepdims=True)
            var = jnp.mean(dev * dev, axis=1, keepdims=True)
            v = dev * lax.rsqrt(var + 1e-05) * gain_ref[:, cols] + shift_ref[:, cols]
            out_ref[pl.ds(at, BLOCK), cols] = (v / (1.0 + jnp.exp(-v))).astype(jnp.bfloat16)
        return carry

    lax.fori_loop(0, tok // BLOCK, block, 0)


def conv_module(value, gate, rim, segments, seen, taps, gain, shift):
    tok, width = value.shape
    return kernel(
        conv_body,
        ((tok, width), jnp.bfloat16),
        (value, gate, rim, segments, seen, taps, gain[None], shift[None]),
        scratch=[pltpu.VMEM((8, RIM + tok, width), jnp.float32)],
    )


def dot(a, b):
    return jnp.dot(a, b, preferred_element_type=jnp.float32)


def places(routes, experts_n, capacity):
    rows, top_count = routes.shape
    expert = lax.broadcasted_iota(jnp.int32, (rows, experts_n), 1)
    named = [jnp.where(expert == routes[:, m : m + 1], 1.0, 0.0) for m in range(top_count)]
    earlier = lax.broadcasted_iota(jnp.int32, (rows, rows), 0) > lax.broadcasted_iota(
        jnp.int32, (rows, rows), 1
    )
    earlier = jnp.where(earlier, 1.0, 0.0).astype(jnp.bfloat16)
    taken = dot(earlier, sum(named).astype(jnp.bfloat16))
    number = lax.broadcasted_iota(jnp.int32, (rows, experts_n * capacity), 1)
    found = []
    for m in range(top_count):
        rank = jnp.sum(named[m] * taken, axis=1, keepdims=True).astype(jnp.int32)
        found.append(number == routes[:, m : m + 1] * capacity + rank)
    return found


def route_body(
    experts_n, parts_ref, residual_ref, gain_ref, routes_ref, weight_ref, stream_out, sent_out, w_ref, stream_ref, sent_ref, sems
):
    parts_n, _, width = parts_ref.shape
    spans = [slice(j * width, (j + 1) * width) for j in range(parts_n)]
    loads = fetch([(weight_ref.at[rows], w_ref.at[rows]) for rows in spans], sems)
    found = places(routes_ref[...], experts_n, sent_ref.shape[0] // experts_n)
    table = functools.reduce(jnp.logical_or, found)
    table = jnp.where(table, 1.0, 0.0).astype(jnp.bfloat16)
    for j, rows in enumerate(spans):
        loads[j].wait()
        part = dot(parts_ref[j], w_ref[rows])
        stream_ref[...] = part if j == 0 else stream_ref[...] + part
    mixed = stream_ref[...].astype(jnp.bfloat16).astype(jnp.float32)
    stream = residual_ref[...].astype(jnp.float32) + mixed
    stream_ref[...] = stream
    stores = fetch([(stream_ref, stream_out)], sems, parts_n)
    scale = lax.rsqrt(jnp.mean(stream * stream, axis=1, keepdims=True) + 1e-06)
    normed = (stream * scale * gain_ref[...]).astype(jnp.bfloat16)
    step = normed.shape[1] // 4
    for j in range(4):
        cols = slice(j * step, (j + 1) * step)
        sent_ref[:, cols] = lax.dot_general(
            table, normed[:, cols], (((0,), (0,)), ((), ())), preferred_element_type=jnp.float32
        ).astype(jnp.bfloat16)
        stores += fetch([(sent_ref.at[:, cols], sent_out.at[:, cols])], sems, parts_n + 1 + j)
    for c in stores:
        c.wait()


def combine_body(experts_n, stream_in, routes_ref, weights_ref, *refs):
    *back_refs, out, stream_ref, out_ref, sems = refs
    (load,) = fetch([(stream_in, stream_ref)], sems)
    found = places(routes_ref[...], experts_n, back_refs[0].shape[0] // experts_n)
    table = sum(jnp.where(hit, weights_ref[:, m : m + 1], 0.0) for m, hit in enumerate(found))
    high = table.astype(jnp.bfloat16)
    low = (table - high.astype(jnp.float32)).astype(jnp.bfloat16)
    load.wait()
    at, stores = 0, []
    for i, back in enumerate(back_refs):
        cols = slice(at, at + back.shape[1])
        rows = back[...]
        mixed = dot(high, rows) + dot(low, rows)
        out_ref[:, cols] = (stream_ref[:, cols] + mixed).astype(jnp.bfloat16)
        stores += fetch([(out_ref.at[:, cols], out.at[:, cols])], sems, 1 + i)
        at += back.shape[1]
    for c in stores:
        c.wait()


def experts_body(layout, cols, *refs):
    rows_in, *pieces, hidden_out, out, rows_ref, w_ref, hidden_ref, down_ref, out_ref, sems = refs
    width = pieces[0].shape[1]
    (load,) = fetch([(rows_in, rows_ref)], sems)
    loads, at = [], 1
    for q, spans in enumerate(layout):
        copies = [
            (
                pieces[i].at[start:stop],
                w_ref.at[q, top : top + stop - start, kind * width : (kind + 1) * width],
            )
            for i, start, stop, kind, top in spans
        ]
        loads.append(fetch(copies, sems, at))
        at += len(copies)
    copies, top = [], 0
    for piece in pieces[1 + max(span[0] for spans in layout for span in spans) :]:
        src = piece.at[:, cols] if top == 0 else piece
        copies.append((src, down_ref.at[top : top + piece.shape[0]]))
        top += piece.shape[0]
    downs = fetch(copies, sems, at)
    load.wait()
    for q, copies in enumerate(loads):
        for c in copies:
            c.wait()
        act = dot(rows_ref[...], w_ref[q])
        gate = act[:, :width]
        hidden = gate / (1.0 + jnp.exp(-gate)) * act[:, width:]
        hidden_ref[:, q * width : (q + 1) * width] = hidden.astype(jnp.bfloat16)
    stores = fetch([(hidden_ref, hidden_out)], sems)
    for c in downs:
        c.wait()
    out_ref[...] = dot(hidden_ref[...], down_ref[...]).astype(jnp.bfloat16)
    stores += fetch([(out_ref, out)], sems, 1)
    for c in stores:
        c.wait()


def expert_rows(rows, pieces, layout, downs, cols):
    (n, d), width, out_width = rows.shape, pieces[0].shape[1], cols.stop - cols.start
    units = width * len(layout)
    n_copies = 1 + sum(len(spans) for spans in layout) + len(downs)
    return kernel(
        functools.partial(experts_body, layout, cols),
        [((n, units), jnp.bfloat16), ((n, out_width), jnp.bfloat16)],
        (rows, *pieces, *downs),
        scratch=[
            pltpu.VMEM((n, d), jnp.bfloat16),
            pltpu.VMEM((len(layout), d, 2 * width), jnp.bfloat16),
            pltpu.VMEM((n, units), jnp.bfloat16),
            pltpu.VMEM((units, out_width), jnp.bfloat16),
            pltpu.VMEM((n, out_width), jnp.bfloat16),
            pltpu.SemaphoreType.DMA((n_copies,)),
        ],
        limit=22,
        far_in=range(1 + len(pieces) + len(downs)),
        far_out=(0, 1),
    )


def down_body(cols, hidden_ref, own_ref, *refs):
    *pieces, out, down_ref, out_ref, sems = refs
    at = own_ref.shape[0]
    down_ref[:at] = own_ref[:, cols]
    for piece in pieces:
        down_ref[at : at + piece.shape[0]] = piece[...]
        at += piece.shape[0]
    half = out_ref.shape[1] // 2
    stores = []
    for i in range(2):
        span = slice(i * half, (i + 1) * half)
        out_ref[:, span] = dot(hidden_ref[...], down_ref[:, span]).astype(jnp.bfloat16)
        stores += fetch([(out_ref.at[:, span], out.at[:, span])], sems, i)
    for c in stores:
        c.wait()


def down_rows(hidden, own, pieces, cols):
    n, width = hidden.shape[0], cols.stop - cols.start
    return kernel(
        functools.partial(down_body, cols),
        ((n, width), jnp.bfloat16),
        (hidden, own, *pieces),
        scratch=[
            pltpu.VMEM((hidden.shape[1], width), jnp.bfloat16),
            pltpu.VMEM((n, width), jnp.bfloat16),
            pltpu.SemaphoreType.DMA((2,)),
        ],
        limit=16,
        far_out=(0,),
    )


def gathered_down(shard):
    half = shard.shape[0] // 2
    left, right = ring(shard, "tp", 1), ring(shard, "tp", -1)
    far = [ring(left[:half], "tp", 1), ring(right[half:], "tp", -1)]
    return [left], [right], far


def gathered_down_halves(shard):
    half = shard.shape[0] // 2
    top, low = shard[:half], shard[half:]
    left_top, right_low = ring(top, "tp", 1), ring(low, "tp", -1)
    left_low, right_top = ring(low, "tp", 1), ring(top, "tp", -1)
    far = [ring(left_top, "tp", 1), ring(right_low, "tp", -1)]
    return [left_top, left_low], [right_top, right_low], far


def shards(
    residual,
    conv_value,
    conv_gate,
    segments,
    conv_weight,
    norm_gain,
    norm_shift,
    out_weight,
    ffn_gain,
    routes,
    route_weights,
    w_gate,
    w_up,
    w_down,
):
    tok_dev, local_channels = conv_value.shape
    reach = conv_weight.shape[0] - 1
    model_width = w_down.shape[2]
    cut = model_width * FIRST // 8
    groups = slice(0, cut), slice(cut, model_width)
    lines = segments.reshape(tok_dev // LANES, LANES)
    rim, head, tail = rim_and_packs(conv_value, conv_gate, lines, w_gate[0], w_up[0])
    rim = passed_along(rim, "sp", 1)
    deep, split = w_gate.shape[1], head.shape[0]
    head_left, head_right = ring(head, "tp", 1), ring(head, "tp", -1)
    tail_left, tail_right = ring(tail, "tp", 1), ring(tail, "tp", -1)
    last = deep
    far_head = ring(head_left, "tp", 1)
    far_first = ring(tail_right[:last], "tp", -1)
    far_last = ring(tail_left[last:], "tp", 1)
    first = gathered_down(w_down[0][:, groups[0]])
    second = gathered_down_halves(w_down[0][:, groups[1]])
    padded = jnp.pad(segments, (reach, 0), constant_values=-1)
    seen = jnp.zeros((tok_dev,), jnp.int32)
    for offset in range(reach):
        seen = seen + (padded[offset : offset + tok_dev] == segments).astype(jnp.int32)
    seen = jnp.broadcast_to(seen[:, None], (tok_dev, LANES))
    conv_out = conv_module(
        conv_value, conv_gate, rim, lines, seen, conv_weight, norm_gain, norm_shift
    )
    columns = lax.axis_size("tp")
    column = lax.axis_index("tp")
    rows_own = tok_dev // columns
    regrouped = lax.all_to_all(
        conv_out.reshape(columns, rows_own, local_channels), "tp", 0, 0, tiled=True
    )
    experts_n = lax.axis_size("sp")
    top_count = routes.shape[1]
    capacity = max(2, 2 * tok_dev * top_count // (columns * experts_n))
    slot_total = experts_n * capacity
    own_routes = lax.dynamic_slice_in_dim(routes, column * rows_own, rows_own, 0)
    own_weights = lax.dynamic_slice_in_dim(route_weights, column * rows_own, rows_own, 0)
    stream, outgoing = kernel(
        functools.partial(route_body, experts_n),
        [((rows_own, model_width), jnp.float32), ((slot_total, model_width), jnp.bfloat16)],
        (regrouped, residual, ffn_gain[None], own_routes, out_weight),
        scratch=[
            pltpu.VMEM(out_weight.shape, jnp.bfloat16),
            pltpu.VMEM((rows_own, model_width), jnp.float32),
            pltpu.VMEM((slot_total, model_width), jnp.bfloat16),
            pltpu.SemaphoreType.DMA((columns + 5,)),
        ],
        limit=24,
        far_in=(4,),
        far_out=(0, 1),
    )
    arrived = lax.all_to_all(
        outgoing.reshape(experts_n, capacity, model_width), "sp", 0, 0, tiled=True
    ).reshape(slot_total, model_width)

    def returned(out):
        return lax.all_to_all(
            out.reshape(experts_n, capacity, -1), "sp", 0, 0, tiled=True
        ).reshape(slot_total, -1)

    pieces = [w_gate[0], w_up[0], head_left, tail_left, head_right, tail_right, far_head, far_first, far_last]
    own = ((0, 0, deep, 0, 0), (1, 0, deep, 1, 0))
    near = [
        ((i, 0, split, 0, 0), (i + 1, 0, deep - split, 0, split), (i + 1, deep - split, 2 * deep - split, 1, 0))
        for i in (2, 4)
    ]
    met = last - (deep - split)
    far = (
        (6, 0, split, 0, 0),
        (7, 0, deep - split, 0, split),
        (7, deep - split, last, 1, 0),
        (8, 0, deep - met, 1, met),
    )
    hidden, out = expert_rows(
        arrived, pieces, (own, *near, far), [w_down[0]] + [p for side in first for p in side], groups[0]
    )
    back = [returned(out)]
    out = down_rows(hidden, w_down[0], [p for side in second for p in side], groups[1])
    back.append(returned(out))
    return kernel(
        functools.partial(combine_body, experts_n),
        ((rows_own, model_width), jnp.bfloat16),
        (stream, own_routes, own_weights, *back),
        scratch=[
            pltpu.VMEM((rows_own, model_width), jnp.float32),
            pltpu.VMEM((rows_own, model_width), jnp.bfloat16),
            pltpu.SemaphoreType.DMA((1 + len(back),)),
        ],
        limit=24,
        far_in=(0,),
        far_out=(0,),
    )


def solution(mesh):
    return jax.shard_map(
        shards,
        mesh=mesh,
        in_specs=(
            P(("sp", "tp"), None),
            P("sp", "tp"),
            P("sp", "tp"),
            P("sp"),
            P(None, "tp"),
            P("tp"),
            P("tp"),
            P(),
            P(),
            P("sp", None),
            P("sp", None),
            P("sp", None, "tp"),
            P("sp", None, "tp"),
            P("sp", "tp", None),
        ),
        out_specs=P(("sp", "tp"), None),
        check_vma=False,
    )
```

```python
import functools

import jax
import jax.numpy as jnp
from jax import lax
from jax.experimental import pallas as pl
from jax.experimental.pallas import tpu as pltpu
from jax.sharding import PartitionSpec as P

TAPS = 31
RIM = 32
LANES = 128
BLOCK = 64


def passed_along(value, axis, steps):
    count = lax.axis_size(axis)
    initial, last = (max(0, -steps), min(count, count - steps))
    return lax.ppermute(value, axis, [(source, source + steps) for source in range(initial, last)])


def ring(value, axis, steps):
    count = lax.axis_size(axis)
    return lax.ppermute(value, axis, [(i, (i + steps) % count) for i in range(count)])


def kernel(body, out, args, scratch=(), limit=16, far_in=(), far_out=(), own_in=()):
    whole, far = pl.BlockSpec(memory_space=pltpu.VMEM), pl.BlockSpec(memory_space=pltpu.HBM)
    args = [
        a
        if i in own_in
        else pltpu.with_memory_space_constraint(a, pltpu.HBM if i in far_in else pltpu.VMEM)
        for i, a in enumerate(args)
    ]
    outs = out if isinstance(out, list) else [out]
    got = pl.pallas_call(
        body,
        out_shape=[
            pltpu.HBM(*o) if i in far_out else jax.ShapeDtypeStruct(*o) for i, o in enumerate(outs)
        ],
        in_specs=[far if i in far_in else whole for i in range(len(args))],
        out_specs=[far if i in far_out else whole for i in range(len(outs))],
        scratch_shapes=scratch,
        compiler_params=pltpu.CompilerParams(vmem_limit_bytes=limit << 20),
    )(*args)
    return got if isinstance(out, list) else got[0]


def fetch(copies, sems, first=0):
    started = [
        pltpu.make_async_copy(src, dst, sems.at[first + i]) for i, (src, dst) in enumerate(copies)
    ]
    for c in started:
        c.start()
    return started


def gated_rows(value, gate):
    return (value.astype(jnp.float32) * jax.nn.sigmoid(gate.astype(jnp.float32))).astype(jnp.bfloat16)


def rim_body(value_ref, gate_ref, segments_ref, out_ref):
    width = value_ref.shape[1]
    gated = gated_rows(value_ref[...], gate_ref[...]).astype(jnp.float32)
    last = segments_ref[segments_ref.shape[0] - 1 :, :].astype(jnp.float32)
    named = jnp.concatenate([last] + [jnp.zeros_like(last)] * (width // LANES - 1), axis=1)
    row = lax.broadcasted_iota(jnp.int32, gated.shape, 0)
    out_ref[...] = jnp.where(row == 0, named, gated).astype(jnp.bfloat16)


def rim_rows(value, gate, segments):
    tok, width = value.shape
    last = pl.BlockSpec((RIM, width), lambda i: (tok // RIM - 1, 0))
    return pl.pallas_call(
        rim_body,
        grid=(1,),
        in_specs=[last, last, pl.BlockSpec(segments.shape, lambda i: (0, 0))],
        out_specs=pl.BlockSpec((RIM, width), lambda i: (0, 0)),
        out_shape=jax.ShapeDtypeStruct((RIM, width), jnp.bfloat16),
        name="rim_rows",
    )(value, gate, segments)


def conv_body(value_ref, gate_ref, rim_ref, segments_ref, seen_ref, taps_ref, gain_ref, shift_ref, out_ref, rows_ref):
    tok = value_ref.shape[0]
    rows_ref[0, :RIM] = rim_ref[...].astype(jnp.float32)
    rows_ref[0, RIM:] = gated_rows(value_ref[...], gate_ref[...]).astype(jnp.float32)
    for r in range(1, 8):
        rows_ref[r, 8:] = rows_ref[0, 8 - r : RIM + tok - r]
    lane = lax.broadcasted_iota(jnp.int32, (1, LANES), 1)
    same = rim_ref[0:1, :LANES].astype(jnp.float32) == segments_ref[0:1, 0:1].astype(jnp.float32)
    same = jnp.where(same & (lane >= LANES - (TAPS - 1)), 1.0, 0.0)
    before = jnp.sum(same, axis=1, keepdims=True).astype(jnp.int32)

    def block(i, carry):
        at = pl.multiple_of(i * BLOCK, BLOCK)
        seen = seen_ref[pl.ds(at, BLOCK), :]
        row = at + lax.broadcasted_iota(jnp.int32, (BLOCK, LANES), 0)
        seen = jnp.where(seen == row, seen + before, seen)
        for lane in range(0, value_ref.shape[1], LANES):
            cols = slice(lane, lane + LANES)
            total = rows_ref[0, pl.ds(at + RIM, BLOCK), cols] * taps_ref[TAPS - 1 : TAPS, cols]
            for back in range(1, TAPS):
                tap = TAPS - 1 - back
                rows = rows_ref[back % 8, pl.ds(at + RIM - back // 8 * 8, BLOCK), cols]
                total = total + jnp.where(seen >= back, rows * taps_ref[tap : tap + 1, cols], 0.0)
            dev = total - jnp.mean(total, axis=1, keepdims=True)
            var = jnp.mean(dev * dev, axis=1, keepdims=True)
            v = dev * lax.rsqrt(var + 1e-05) * gain_ref[:, cols] + shift_ref[:, cols]
            out_ref[pl.ds(at, BLOCK), cols] = (v / (1.0 + jnp.exp(-v))).astype(jnp.bfloat16)
        return carry

    lax.fori_loop(0, tok // BLOCK, block, 0)


def conv_module(value, gate, rim, segments, seen, taps, gain, shift):
    tok, width = value.shape
    return kernel(
        conv_body,
        ((tok, width), jnp.bfloat16),
        (value, gate, rim, segments, seen, taps, gain[None], shift[None]),
        scratch=[pltpu.VMEM((8, RIM + tok, width), jnp.float32)],
        own_in=(0, 1, 3, 5, 6, 7),
    )


def dot(a, b):
    return jnp.dot(a, b, preferred_element_type=jnp.float32)


def places(routes, experts_n, capacity):
    rows, top_count = routes.shape
    expert = lax.broadcasted_iota(jnp.int32, (rows, experts_n), 1)
    named = [jnp.where(expert == routes[:, m : m + 1], 1.0, 0.0) for m in range(top_count)]
    earlier = lax.broadcasted_iota(jnp.int32, (rows, rows), 0) > lax.broadcasted_iota(
        jnp.int32, (rows, rows), 1
    )
    earlier = jnp.where(earlier, 1.0, 0.0).astype(jnp.bfloat16)
    taken = dot(earlier, sum(named).astype(jnp.bfloat16))
    number = lax.broadcasted_iota(jnp.int32, (rows, experts_n * capacity), 1)
    found = []
    for m in range(top_count):
        rank = jnp.sum(named[m] * taken, axis=1, keepdims=True).astype(jnp.int32)
        found.append(number == routes[:, m : m + 1] * capacity + rank)
    return found


def route_body(
    experts_n, parts_ref, residual_ref, gain_ref, routes_ref, weight_ref, stream_out, sent_out, w_ref, stream_ref, sent_ref, sems
):
    parts_n, _, width = parts_ref.shape
    spans = [slice(j * width, (j + 1) * width) for j in range(parts_n)]
    loads = fetch([(weight_ref.at[rows], w_ref.at[rows]) for rows in spans], sems)
    found = places(routes_ref[...], experts_n, sent_ref.shape[0] // experts_n)
    table = functools.reduce(jnp.logical_or, found)
    table = jnp.where(table, 1.0, 0.0).astype(jnp.bfloat16)
    for j, rows in enumerate(spans):
        loads[j].wait()
        part = dot(parts_ref[j], w_ref[rows])
        stream_ref[...] = part if j == 0 else stream_ref[...] + part
    mixed = stream_ref[...].astype(jnp.bfloat16).astype(jnp.float32)
    stream = residual_ref[...].astype(jnp.float32) + mixed
    stream_ref[...] = stream
    stores = fetch([(stream_ref, stream_out)], sems, parts_n)
    scale = lax.rsqrt(jnp.mean(stream * stream, axis=1, keepdims=True) + 1e-06)
    normed = (stream * scale * gain_ref[...]).astype(jnp.bfloat16)
    step = normed.shape[1] // 4
    for j in range(4):
        cols = slice(j * step, (j + 1) * step)
        sent_ref[:, cols] = lax.dot_general(
            table, normed[:, cols], (((0,), (0,)), ((), ())), preferred_element_type=jnp.float32
        ).astype(jnp.bfloat16)
        stores += fetch([(sent_ref.at[:, cols], sent_out.at[:, cols])], sems, parts_n + 1 + j)
    for c in stores:
        c.wait()


def combine_body(
    experts_n, stream_in, routes_ref, weights_ref, back_ref, out, stream_ref, out_ref, sems
):
    (load,) = fetch([(stream_in, stream_ref)], sems)
    found = places(routes_ref[...], experts_n, back_ref.shape[0] // experts_n)
    table = sum(jnp.where(hit, weights_ref[:, m : m + 1], 0.0) for m, hit in enumerate(found))
    high = table.astype(jnp.bfloat16)
    low = (table - high.astype(jnp.float32)).astype(jnp.bfloat16)
    load.wait()
    stores, step = [], out_ref.shape[1] // 4
    for i in range(4):
        cols = slice(i * step, (i + 1) * step)
        rows = back_ref[:, cols]
        mixed = dot(high, rows) + dot(low, rows)
        out_ref[:, cols] = (stream_ref[:, cols] + mixed).astype(jnp.bfloat16)
        stores += fetch([(out_ref.at[:, cols], out.at[:, cols])], sems, 1 + i)
    for c in stores:
        c.wait()


def hidden_body(counts, *refs):
    rows_in, *pieces, out_ref, rows_ref, w_ref, sems = refs
    width = pieces[0].shape[1]
    (load,) = fetch([(rows_in, rows_ref)], sems, len(pieces))
    loads = []
    for q, kinds in enumerate(counts):
        copies = []
        for kind, n in enumerate(kinds):
            top = 0
            for piece in pieces[:n]:
                end = top + piece.shape[0]
                copies.append((piece, w_ref.at[q, top:end, kind * width : (kind + 1) * width]))
                top = end
            pieces = pieces[n:]
        loads.append(fetch(copies, sems, sum(len(c) for c in loads)))
    load.wait()
    for q, copies in enumerate(loads):
        for c in copies:
            c.wait()
        act = dot(rows_ref[...], w_ref[q])
        gate = act[:, :width]
        hidden = gate / (1.0 + jnp.exp(-gate)) * act[:, width:]
        out_ref[:, q * width : (q + 1) * width] = hidden.astype(jnp.bfloat16)


def hidden_units(rows, quarters):
    counts = tuple((len(gates), len(ups)) for gates, ups in quarters)
    pieces = [p for gates, ups in quarters for p in (*gates, *ups)]
    (n, d), width = rows.shape, pieces[0].shape[1]
    return kernel(
        functools.partial(hidden_body, counts),
        ((n, width * len(counts)), jnp.bfloat16),
        (rows, *pieces),
        scratch=[
            pltpu.VMEM((n, d), jnp.bfloat16),
            pltpu.VMEM((len(counts), d, 2 * width), jnp.bfloat16),
            pltpu.SemaphoreType.DMA((len(pieces) + 1,)),
        ],
        limit=20,
        far_in=range(1 + len(pieces)),
    )


def down_body(hidden_ref, own_ref, *refs):
    *pieces, out, down_ref, out_ref, sems = refs
    at = own_ref.shape[0]
    (load,) = fetch([(own_ref, down_ref.at[:at])], sems)
    for piece in pieces:
        down_ref[at : at + piece.shape[0]] = piece[...]
        at += piece.shape[0]
    load.wait()
    stores, step = [], out_ref.shape[1] // 4
    for i in range(4):
        span = slice(i * step, (i + 1) * step)
        out_ref[:, span] = dot(hidden_ref[...], down_ref[:, span]).astype(jnp.bfloat16)
        stores += fetch([(out_ref.at[:, span], out.at[:, span])], sems, i)
    for c in stores:
        c.wait()


def down_rows(hidden, own, pieces):
    n, width = hidden.shape[0], own.shape[1]
    return kernel(
        down_body,
        ((n, width), jnp.bfloat16),
        (hidden, own, *pieces),
        scratch=[
            pltpu.VMEM((hidden.shape[1], width), jnp.bfloat16),
            pltpu.VMEM((n, width), jnp.bfloat16),
            pltpu.SemaphoreType.DMA((4,)),
        ],
        limit=16,
        far_in=(1,),
        far_out=(0,),
    )


def gathered(shard):
    left, right = ring(shard, "tp", 1), ring(shard, "tp", -1)
    half = shard.shape[0] // 2
    far = [ring(left[:half], "tp", 1), ring(right[half:], "tp", -1)]
    return [left], [right], far


def shards(
    residual,
    conv_value,
    conv_gate,
    segments,
    conv_weight,
    norm_gain,
    norm_shift,
    out_weight,
    ffn_gain,
    routes,
    route_weights,
    w_gate,
    w_up,
    w_down,
):
    tok_dev, local_channels = conv_value.shape
    reach = conv_weight.shape[0] - 1
    model_width = w_down.shape[2]
    gates = gathered(w_gate[0])
    ups = gathered(w_up[0])
    downs = gathered(w_down[0])
    lines = segments.reshape(tok_dev // LANES, LANES)
    rim = passed_along(rim_rows(conv_value, conv_gate, lines), "sp", 1)
    padded = jnp.pad(segments, (reach, 0), constant_values=-1)
    seen = jnp.zeros((tok_dev,), jnp.int32)
    for offset in range(reach):
        seen = seen + (padded[offset : offset + tok_dev] == segments).astype(jnp.int32)
    seen = jnp.broadcast_to(seen[:, None], (tok_dev, LANES))
    conv_out = conv_module(
        conv_value, conv_gate, rim, lines, seen, conv_weight, norm_gain, norm_shift
    )
    columns = lax.axis_size("tp")
    column = lax.axis_index("tp")
    rows_own = tok_dev // columns
    regrouped = lax.all_to_all(
        conv_out.reshape(columns, rows_own, local_channels), "tp", 0, 0, tiled=True
    )
    experts_n = lax.axis_size("sp")
    top_count = routes.shape[1]
    capacity = max(2, 2 * tok_dev * top_count // (columns * experts_n))
    slot_total = experts_n * capacity
    own_routes = lax.dynamic_slice_in_dim(routes, column * rows_own, rows_own, 0)
    own_weights = lax.dynamic_slice_in_dim(route_weights, column * rows_own, rows_own, 0)
    stream, outgoing = kernel(
        functools.partial(route_body, experts_n),
        [((rows_own, model_width), jnp.float32), ((slot_total, model_width), jnp.bfloat16)],
        (regrouped, residual, ffn_gain[None], own_routes, out_weight),
        scratch=[
            pltpu.VMEM(out_weight.shape, jnp.bfloat16),
            pltpu.VMEM((rows_own, model_width), jnp.float32),
            pltpu.VMEM((slot_total, model_width), jnp.bfloat16),
            pltpu.SemaphoreType.DMA((columns + 5,)),
        ],
        limit=24,
        far_in=(4,),
        far_out=(0, 1),
    )
    arrived = lax.all_to_all(
        outgoing.reshape(experts_n, capacity, model_width), "sp", 0, 0, tiled=True
    ).reshape(slot_total, model_width)
    hidden = hidden_units(
        arrived,
        [([w_gate[0]], [w_up[0]])] + [(gates[side], ups[side]) for side in range(3)],
    )
    out = down_rows(hidden, w_down[0], [p for side in downs for p in side])
    back = lax.all_to_all(
        out.reshape(experts_n, capacity, model_width), "sp", 0, 0, tiled=True
    ).reshape(slot_total, model_width)
    return kernel(
        functools.partial(combine_body, experts_n),
        ((rows_own, model_width), jnp.bfloat16),
        (stream, own_routes, own_weights, back),
        scratch=[
            pltpu.VMEM((rows_own, model_width), jnp.float32),
            pltpu.VMEM((rows_own, model_width), jnp.bfloat16),
            pltpu.SemaphoreType.DMA((5,)),
        ],
        limit=24,
        far_in=(0,),
        far_out=(0,),
    )


def solution(mesh):
    return jax.shard_map(
        shards,
        mesh=mesh,
        in_specs=(
            P(("sp", "tp"), None),
            P("sp", "tp"),
            P("sp", "tp"),
            P("sp"),
            P(None, "tp"),
            P("tp"),
            P("tp"),
            P(),
            P(),
            P("sp", None),
            P("sp", None),
            P("sp", None, "tp"),
            P("sp", None, "tp"),
            P("sp", "tp", None),
        ),
        out_specs=P(("sp", "tp"), None),
        check_vma=False,
    )
```

```python
import functools

import jax
import jax.numpy as jnp
from jax import lax
from jax.experimental import pallas as pl
from jax.experimental.pallas import tpu as pltpu
from jax.sharding import PartitionSpec as P

TAPS = 31
RIM = 32
LANES = 128
BLOCK = 64


def passed_along(value, axis, steps):
    count = lax.axis_size(axis)
    initial, last = (max(0, -steps), min(count, count - steps))
    return lax.ppermute(value, axis, [(source, source + steps) for source in range(initial, last)])


def ring(value, axis, steps):
    count = lax.axis_size(axis)
    return lax.ppermute(value, axis, [(i, (i + steps) % count) for i in range(count)])


def kernel(body, out, args, scratch=(), limit=16, far_in=(), far_out=()):
    whole, far = pl.BlockSpec(memory_space=pltpu.VMEM), pl.BlockSpec(memory_space=pltpu.HBM)
    args = [
        pltpu.with_memory_space_constraint(a, pltpu.HBM if i in far_in else pltpu.VMEM)
        for i, a in enumerate(args)
    ]
    outs = out if isinstance(out, list) else [out]
    got = pl.pallas_call(
        body,
        out_shape=[
            pltpu.HBM(*o) if i in far_out else jax.ShapeDtypeStruct(*o) for i, o in enumerate(outs)
        ],
        in_specs=[far if i in far_in else whole for i in range(len(args))],
        out_specs=[far if i in far_out else whole for i in range(len(outs))],
        scratch_shapes=scratch,
        compiler_params=pltpu.CompilerParams(vmem_limit_bytes=limit << 20),
    )(*args)
    return got if isinstance(out, list) else got[0]


def fetch(copies, sems, first=0):
    started = [
        pltpu.make_async_copy(src, dst, sems.at[first + i]) for i, (src, dst) in enumerate(copies)
    ]
    for c in started:
        c.start()
    return started


def gated_rows(value, gate):
    return (value.astype(jnp.float32) * jax.nn.sigmoid(gate.astype(jnp.float32))).astype(jnp.bfloat16)


def rim_body(value_ref, gate_ref, segments_ref, out_ref):
    width = value_ref.shape[1]
    gated = gated_rows(value_ref[...], gate_ref[...]).astype(jnp.float32)
    last = segments_ref[segments_ref.shape[0] - 1 :, :].astype(jnp.float32)
    named = jnp.concatenate([last] + [jnp.zeros_like(last)] * (width // LANES - 1), axis=1)
    row = lax.broadcasted_iota(jnp.int32, gated.shape, 0)
    out_ref[...] = jnp.where(row == 0, named, gated).astype(jnp.bfloat16)


def rim_rows(value, gate, segments):
    tok, width = value.shape
    last = pl.BlockSpec((RIM, width), lambda i: (tok // RIM - 1, 0))
    return pl.pallas_call(
        rim_body,
        grid=(1,),
        in_specs=[last, last, pl.BlockSpec(segments.shape, lambda i: (0, 0))],
        out_specs=pl.BlockSpec((RIM, width), lambda i: (0, 0)),
        out_shape=jax.ShapeDtypeStruct((RIM, width), jnp.bfloat16),
        name="rim_rows",
    )(value, gate, segments)


def conv_body(rim_ref, seen_ref, *refs):
    sources, (out_ref, rows_ref, *held, sems) = refs[:6], refs[6:]
    for c in fetch(list(zip(sources, held)), sems):
        c.wait()
    value_ref, gate_ref, segments_ref, taps_ref, gain_ref, shift_ref = held
    tok = value_ref.shape[0]
    rows_ref[0, :RIM] = rim_ref[...].astype(jnp.float32)
    rows_ref[0, RIM:] = gated_rows(value_ref[...], gate_ref[...]).astype(jnp.float32)
    for r in range(1, 8):
        rows_ref[r, 8:] = rows_ref[0, 8 - r : RIM + tok - r]
    lane = lax.broadcasted_iota(jnp.int32, (1, LANES), 1)
    same = rim_ref[0:1, :LANES].astype(jnp.float32) == segments_ref[0:1, 0:1].astype(jnp.float32)
    same = jnp.where(same & (lane >= LANES - (TAPS - 1)), 1.0, 0.0)
    before = jnp.sum(same, axis=1, keepdims=True).astype(jnp.int32)

    def block(i, carry):
        at = pl.multiple_of(i * BLOCK, BLOCK)
        seen = seen_ref[pl.ds(at, BLOCK), :]
        row = at + lax.broadcasted_iota(jnp.int32, (BLOCK, LANES), 0)
        seen = jnp.where(seen == row, seen + before, seen)
        for lane in range(0, value_ref.shape[1], LANES):
            cols = slice(lane, lane + LANES)
            total = rows_ref[0, pl.ds(at + RIM, BLOCK), cols] * taps_ref[TAPS - 1 : TAPS, cols]
            for back in range(1, TAPS):
                tap = TAPS - 1 - back
                rows = rows_ref[back % 8, pl.ds(at + RIM - back // 8 * 8, BLOCK), cols]
                total = total + jnp.where(seen >= back, rows * taps_ref[tap : tap + 1, cols], 0.0)
            dev = total - jnp.mean(total, axis=1, keepdims=True)
            var = jnp.mean(dev * dev, axis=1, keepdims=True)
            v = dev * lax.rsqrt(var + 1e-05) * gain_ref[:, cols] + shift_ref[:, cols]
            out_ref[pl.ds(at, BLOCK), cols] = (v / (1.0 + jnp.exp(-v))).astype(jnp.bfloat16)
        return carry

    lax.fori_loop(0, tok // BLOCK, block, 0)


def conv_module(value, gate, rim, segments, seen, taps, gain, shift):
    tok, width = value.shape
    fetched = (value, gate, segments, taps, gain[None], shift[None])
    return kernel(
        conv_body,
        ((tok, width), jnp.bfloat16),
        (rim, seen, *fetched),
        scratch=[pltpu.VMEM((8, RIM + tok, width), jnp.float32)]
        + [pltpu.VMEM(a.shape, a.dtype) for a in fetched]
        + [pltpu.SemaphoreType.DMA((len(fetched),))],
        far_in=range(2, 2 + len(fetched)),
    )


def dot(a, b):
    return jnp.dot(a, b, preferred_element_type=jnp.float32)


def places(routes, experts_n, capacity):
    rows, top_count = routes.shape
    expert = lax.broadcasted_iota(jnp.int32, (rows, experts_n), 1)
    named = [jnp.where(expert == routes[:, m : m + 1], 1.0, 0.0) for m in range(top_count)]
    earlier = lax.broadcasted_iota(jnp.int32, (rows, rows), 0) > lax.broadcasted_iota(
        jnp.int32, (rows, rows), 1
    )
    earlier = jnp.where(earlier, 1.0, 0.0).astype(jnp.bfloat16)
    taken = dot(earlier, sum(named).astype(jnp.bfloat16))
    number = lax.broadcasted_iota(jnp.int32, (rows, experts_n * capacity), 1)
    found = []
    for m in range(top_count):
        rank = jnp.sum(named[m] * taken, axis=1, keepdims=True).astype(jnp.int32)
        found.append(number == routes[:, m : m + 1] * capacity + rank)
    return found


def route_body(
    experts_n, parts_ref, residual_ref, gain_ref, routes_ref, weight_ref, stream_out, sent_out, w_ref, stream_ref, sent_ref, sems
):
    parts_n, _, width = parts_ref.shape
    spans = [slice(j * width, (j + 1) * width) for j in range(parts_n)]
    loads = fetch([(weight_ref.at[rows], w_ref.at[rows]) for rows in spans], sems)
    found = places(routes_ref[...], experts_n, sent_ref.shape[0] // experts_n)
    table = functools.reduce(jnp.logical_or, found)
    table = jnp.where(table, 1.0, 0.0).astype(jnp.bfloat16)
    for j, rows in enumerate(spans):
        loads[j].wait()
        part = dot(parts_ref[j], w_ref[rows])
        stream_ref[...] = part if j == 0 else stream_ref[...] + part
    mixed = stream_ref[...].astype(jnp.bfloat16).astype(jnp.float32)
    stream = residual_ref[...].astype(jnp.float32) + mixed
    stream_ref[...] = stream
    stores = fetch([(stream_ref, stream_out)], sems, parts_n)
    scale = lax.rsqrt(jnp.mean(stream * stream, axis=1, keepdims=True) + 1e-06)
    normed = (stream * scale * gain_ref[...]).astype(jnp.bfloat16)
    step = normed.shape[1] // 4
    for j in range(4):
        cols = slice(j * step, (j + 1) * step)
        sent_ref[:, cols] = lax.dot_general(
            table, normed[:, cols], (((0,), (0,)), ((), ())), preferred_element_type=jnp.float32
        ).astype(jnp.bfloat16)
        stores += fetch([(sent_ref.at[:, cols], sent_out.at[:, cols])], sems, parts_n + 1 + j)
    for c in stores:
        c.wait()


def table_body(experts_n, routes_ref, weights_ref, high_ref, low_ref):
    found = places(routes_ref[...], experts_n, high_ref.shape[1] // experts_n)
    table = sum(jnp.where(hit, weights_ref[:, m : m + 1], 0.0) for m, hit in enumerate(found))
    high = table.astype(jnp.bfloat16)
    high_ref[...] = high
    low_ref[...] = (table - high.astype(jnp.float32)).astype(jnp.bfloat16)


def combine_body(stream_ref, high_ref, low_ref, back_ref, out, out_ref, sems):
    stores, step = [], out_ref.shape[1] // 4
    for i in range(4):
        cols = slice(i * step, (i + 1) * step)
        rows = back_ref[:, cols]
        mixed = dot(high_ref[...], rows) + dot(low_ref[...], rows)
        out_ref[:, cols] = (stream_ref[:, cols] + mixed).astype(jnp.bfloat16)
        stores += fetch([(out_ref.at[:, cols], out.at[:, cols])], sems, i)
    for c in stores:
        c.wait()


def hidden_body(counts, *refs):
    rows_in, *pieces, far_ref, sum_ref, rows_ref, w_ref, hidden_ref, down_ref, sems = refs
    width = pieces[0].shape[1]
    (load,) = fetch([(rows_in, rows_ref)], sems)
    loads, at = [], 1
    for q, kinds in enumerate(counts):
        copies = []
        for kind, n in enumerate(kinds):
            top = 0
            for piece in pieces[:n]:
                end = top + piece.shape[0]
                copies.append((piece, w_ref.at[q, top:end, kind * width : (kind + 1) * width]))
                top = end
            pieces = pieces[n:]
        loads.append(fetch(copies, sems, at))
        at += len(copies)
    spans = [slice(q * width, (q + 1) * width) for q in range(len(pieces))]
    downs = fetch([(piece, down_ref.at[rows]) for piece, rows in zip(pieces, spans)], sems, at)
    load.wait()
    for q, copies in enumerate(loads):
        for c in copies:
            c.wait()
        act = dot(rows_ref[...], w_ref[q])
        gate = act[:, :width]
        hidden = (gate / (1.0 + jnp.exp(-gate)) * act[:, width:]).astype(jnp.bfloat16)
        if q < len(spans):
            hidden_ref[:, spans[q]] = hidden
        else:
            far_ref[...] = hidden
    for c in downs:
        c.wait()
    step = sum_ref.shape[1] // 4
    for i in range(4):
        cols = slice(i * step, (i + 1) * step)
        sum_ref[:, cols] = dot(hidden_ref[...], down_ref[:, cols])


def hidden_units(rows, quarters, downs):
    counts = tuple((len(gates), len(ups)) for gates, ups in quarters)
    pieces = [p for gates, ups in quarters for p in (*gates, *ups)] + downs
    (n, d), width, out_width = rows.shape, pieces[0].shape[1], downs[0].shape[1]
    return kernel(
        functools.partial(hidden_body, counts),
        [((n, width), jnp.bfloat16), ((n, out_width), jnp.float32)],
        (rows, *pieces),
        scratch=[
            pltpu.VMEM((n, d), jnp.bfloat16),
            pltpu.VMEM((len(counts), d, 2 * width), jnp.bfloat16),
            pltpu.VMEM((n, len(downs) * width), jnp.bfloat16),
            pltpu.VMEM((len(downs) * width, out_width), jnp.bfloat16),
            pltpu.SemaphoreType.DMA((len(pieces) + 1,)),
        ],
        limit=26,
        far_in=range(1 + len(pieces)),
    )


def down_body(hidden_ref, sum_ref, *refs):
    *pieces, out, out_ref, sems = refs
    stores, step = [], out_ref.shape[1] // 4
    for i in range(4):
        cols = slice(i * step, (i + 1) * step)
        total, at = sum_ref[:, cols], 0
        for piece in pieces:
            total = total + dot(hidden_ref[:, at : at + piece.shape[0]], piece[:, cols])
            at += piece.shape[0]
        out_ref[:, cols] = total.astype(jnp.bfloat16)
        stores += fetch([(out_ref.at[:, cols], out.at[:, cols])], sems, i)
    for c in stores:
        c.wait()


def down_rows(hidden, total, pieces):
    n, width = total.shape
    return kernel(
        down_body,
        ((n, width), jnp.bfloat16),
        (hidden, total, *pieces),
        scratch=[pltpu.VMEM((n, width), jnp.bfloat16), pltpu.SemaphoreType.DMA((4,))],
        limit=16,
        far_out=(0,),
    )


def gathered(shard):
    left, right = ring(shard, "tp", 1), ring(shard, "tp", -1)
    half = shard.shape[0] // 2
    far = [ring(left[:half], "tp", 1), ring(right[half:], "tp", -1)]
    return [left], [right], far


def shards(
    residual,
    conv_value,
    conv_gate,
    segments,
    conv_weight,
    norm_gain,
    norm_shift,
    out_weight,
    ffn_gain,
    routes,
    route_weights,
    w_gate,
    w_up,
    w_down,
):
    tok_dev, local_channels = conv_value.shape
    reach = conv_weight.shape[0] - 1
    model_width = w_down.shape[2]
    gates = gathered(w_gate[0])
    ups = gathered(w_up[0])
    downs = gathered(w_down[0])
    lines = segments.reshape(tok_dev // LANES, LANES)
    rim = passed_along(rim_rows(conv_value, conv_gate, lines), "sp", 1)
    padded = jnp.pad(segments, (reach, 0), constant_values=-1)
    seen = jnp.zeros((tok_dev,), jnp.int32)
    for offset in range(reach):
        seen = seen + (padded[offset : offset + tok_dev] == segments).astype(jnp.int32)
    seen = jnp.broadcast_to(seen[:, None], (tok_dev, LANES))
    conv_out = conv_module(
        conv_value, conv_gate, rim, lines, seen, conv_weight, norm_gain, norm_shift
    )
    columns = lax.axis_size("tp")
    column = lax.axis_index("tp")
    rows_own = tok_dev // columns
    regrouped = lax.all_to_all(
        conv_out.reshape(columns, rows_own, local_channels), "tp", 0, 0, tiled=True
    )
    experts_n = lax.axis_size("sp")
    top_count = routes.shape[1]
    capacity = max(2, 2 * tok_dev * top_count // (columns * experts_n))
    slot_total = experts_n * capacity
    own_routes = lax.dynamic_slice_in_dim(routes, column * rows_own, rows_own, 0)
    own_weights = lax.dynamic_slice_in_dim(route_weights, column * rows_own, rows_own, 0)
    stream, outgoing = kernel(
        functools.partial(route_body, experts_n),
        [((rows_own, model_width), jnp.float32), ((slot_total, model_width), jnp.bfloat16)],
        (regrouped, residual, ffn_gain[None], own_routes, out_weight),
        scratch=[
            pltpu.VMEM(out_weight.shape, jnp.bfloat16),
            pltpu.VMEM((rows_own, model_width), jnp.float32),
            pltpu.VMEM((slot_total, model_width), jnp.bfloat16),
            pltpu.SemaphoreType.DMA((columns + 5,)),
        ],
        limit=24,
        far_in=(4,),
        far_out=(0, 1),
    )
    arrived = lax.all_to_all(
        outgoing.reshape(experts_n, capacity, model_width), "sp", 0, 0, tiled=True
    ).reshape(slot_total, model_width)
    hidden, total = hidden_units(
        arrived,
        [([w_gate[0]], [w_up[0]])] + [(gates[side], ups[side]) for side in range(3)],
        [w_down[0], *downs[0], *downs[1]],
    )
    out = down_rows(hidden, total, downs[2])
    back = lax.all_to_all(
        out.reshape(experts_n, capacity, model_width), "sp", 0, 0, tiled=True
    ).reshape(slot_total, model_width)
    high, low = kernel(
        functools.partial(table_body, experts_n),
        [((rows_own, slot_total), jnp.bfloat16)] * 2,
        (own_routes, own_weights),
    )
    return kernel(
        combine_body,
        ((rows_own, model_width), jnp.bfloat16),
        (stream, high, low, back),
        scratch=[pltpu.VMEM((rows_own, model_width), jnp.bfloat16), pltpu.SemaphoreType.DMA((4,))],
        limit=24,
        far_out=(0,),
    )


def solution(mesh):
    return jax.shard_map(
        shards,
        mesh=mesh,
        in_specs=(
            P(("sp", "tp"), None),
            P("sp", "tp"),
            P("sp", "tp"),
            P("sp"),
            P(None, "tp"),
            P("tp"),
            P("tp"),
            P(),
            P(),
            P("sp", None),
            P("sp", None),
            P("sp", None, "tp"),
            P("sp", None, "tp"),
            P("sp", "tp", None),
        ),
        out_specs=P(("sp", "tp"), None),
        check_vma=False,
    )
```

```python
import functools

import jax
import jax.numpy as jnp
from jax import lax
from jax.experimental import pallas as pl
from jax.experimental.pallas import tpu as pltpu
from jax.sharding import PartitionSpec as P

TAPS = 31
RIM = 32
LANES = 128
BLOCK = 64
RING = 8


def passed_along(value, axis, steps):
    count = lax.axis_size(axis)
    initial, last = (max(0, -steps), min(count, count - steps))
    return lax.ppermute(value, axis, [(source, source + steps) for source in range(initial, last)])


def ring(value, axis, steps):
    count = lax.axis_size(axis)
    return lax.ppermute(value, axis, [(i, (i + steps) % count) for i in range(count)])


def kernel(body, out, args, scratch=(), limit=16, far_in=(), far_out=(), scalar_in=()):
    scalar = pl.BlockSpec(memory_space=pltpu.SMEM)
    whole, far = pl.BlockSpec(memory_space=pltpu.VMEM), pl.BlockSpec(memory_space=pltpu.HBM)
    args = [
        a
        if i in scalar_in
        else pltpu.with_memory_space_constraint(a, pltpu.HBM if i in far_in else pltpu.VMEM)
        for i, a in enumerate(args)
    ]
    outs = out if isinstance(out, list) else [out]
    got = pl.pallas_call(
        body,
        out_shape=[
            pltpu.HBM(*o) if i in far_out else jax.ShapeDtypeStruct(*o) for i, o in enumerate(outs)
        ],
        in_specs=[
            scalar if i in scalar_in else far if i in far_in else whole for i in range(len(args))
        ],
        out_specs=[far if i in far_out else whole for i in range(len(outs))],
        scratch_shapes=scratch,
        compiler_params=pltpu.CompilerParams(vmem_limit_bytes=limit << 20),
    )(*args)
    return got if isinstance(out, list) else got[0]


def fetch(copies, sems, first=0):
    started = [
        pltpu.make_async_copy(src, dst, sems.at[first + i]) for i, (src, dst) in enumerate(copies)
    ]
    for c in started:
        c.start()
    return started


def gated_rows(value, gate):
    return (value.astype(jnp.float32) * jax.nn.sigmoid(gate.astype(jnp.float32))).astype(jnp.bfloat16)


def rim_body(value_ref, gate_ref, segments_ref, out_ref):
    width = value_ref.shape[1]
    gated = gated_rows(value_ref[...], gate_ref[...]).astype(jnp.float32)
    last = segments_ref[segments_ref.shape[0] - 1 :, :].astype(jnp.float32)
    named = jnp.concatenate([last] + [jnp.zeros_like(last)] * (width // LANES - 1), axis=1)
    row = lax.broadcasted_iota(jnp.int32, gated.shape, 0)
    out_ref[...] = jnp.where(row == 0, named, gated).astype(jnp.bfloat16)


def rim_rows(value, gate, segments):
    tok, width = value.shape
    last = pl.BlockSpec((RIM, width), lambda i: (tok // RIM - 1, 0))
    return pl.pallas_call(
        rim_body,
        grid=(1,),
        in_specs=[last, last, pl.BlockSpec(segments.shape, lambda i: (0, 0))],
        out_specs=pl.BlockSpec((RIM, width), lambda i: (0, 0)),
        out_shape=jax.ShapeDtypeStruct((RIM, width), jnp.bfloat16),
        name="rim_rows",
    )(value, gate, segments)


def conv_body(rim_ref, seen_ref, *refs):
    sources, (out_ref, rows_ref, *held, sems) = refs[:6], refs[6:]
    for c in fetch(list(zip(sources, held)), sems):
        c.wait()
    value_ref, gate_ref, segments_ref, taps_ref, gain_ref, shift_ref = held
    tok = value_ref.shape[0]
    rows_ref[0, :RIM] = rim_ref[...].astype(jnp.float32)
    rows_ref[0, RIM:] = gated_rows(value_ref[...], gate_ref[...]).astype(jnp.float32)
    for r in range(1, 8):
        rows_ref[r, 8:] = rows_ref[0, 8 - r : RIM + tok - r]
    lane = lax.broadcasted_iota(jnp.int32, (1, LANES), 1)
    same = rim_ref[0:1, :LANES].astype(jnp.float32) == segments_ref[0:1, 0:1].astype(jnp.float32)
    same = jnp.where(same & (lane >= LANES - (TAPS - 1)), 1.0, 0.0)
    before = jnp.sum(same, axis=1, keepdims=True).astype(jnp.int32)

    def block(i, carry):
        at = pl.multiple_of(i * BLOCK, BLOCK)
        seen = seen_ref[pl.ds(at, BLOCK), :]
        row = at + lax.broadcasted_iota(jnp.int32, (BLOCK, LANES), 0)
        seen = jnp.where(seen == row, seen + before, seen)
        for lane in range(0, value_ref.shape[1], LANES):
            cols = slice(lane, lane + LANES)
            total = rows_ref[0, pl.ds(at + RIM, BLOCK), cols] * taps_ref[TAPS - 1 : TAPS, cols]
            for back in range(1, TAPS):
                tap = TAPS - 1 - back
                rows = rows_ref[back % 8, pl.ds(at + RIM - back // 8 * 8, BLOCK), cols]
                total = total + jnp.where(seen >= back, rows * taps_ref[tap : tap + 1, cols], 0.0)
            dev = total - jnp.mean(total, axis=1, keepdims=True)
            var = jnp.mean(dev * dev, axis=1, keepdims=True)
            v = dev * lax.rsqrt(var + 1e-05) * gain_ref[:, cols] + shift_ref[:, cols]
            out_ref[pl.ds(at, BLOCK), cols] = (v / (1.0 + jnp.exp(-v))).astype(jnp.bfloat16)
        return carry

    lax.fori_loop(0, tok // BLOCK, block, 0)


def conv_module(value, gate, rim, segments, seen, taps, gain, shift):
    tok, width = value.shape
    fetched = (value, gate, segments, taps, gain[None], shift[None])
    return kernel(
        conv_body,
        ((tok, width), jnp.bfloat16),
        (rim, seen, *fetched),
        scratch=[pltpu.VMEM((8, RIM + tok, width), jnp.float32)]
        + [pltpu.VMEM(a.shape, a.dtype) for a in fetched]
        + [pltpu.SemaphoreType.DMA((len(fetched),))],
        far_in=range(2, 2 + len(fetched)),
    )


def dot(a, b):
    return jnp.dot(a, b, preferred_element_type=jnp.float32)


def ranks(routes, experts_n):
    rows, top_count = routes.shape
    expert = lax.broadcasted_iota(jnp.int32, (rows, experts_n), 1)
    named = [jnp.where(expert == routes[:, m : m + 1], 1.0, 0.0) for m in range(top_count)]
    earlier = lax.broadcasted_iota(jnp.int32, (rows, rows), 0) > lax.broadcasted_iota(
        jnp.int32, (rows, rows), 1
    )
    earlier = jnp.where(earlier, 1.0, 0.0).astype(jnp.bfloat16)
    taken = dot(earlier, sum(named).astype(jnp.bfloat16))
    return [jnp.sum(n * taken, axis=1, keepdims=True).astype(jnp.int32) for n in named]


def places(routes, experts_n, capacity, seen_as=lambda expert: expert):
    number = lax.broadcasted_iota(jnp.int32, (routes.shape[0], experts_n * capacity), 1)
    return [
        number == seen_as(routes[:, m : m + 1]) * capacity + rank
        for m, rank in enumerate(ranks(routes, experts_n))
    ]


def route_body(
    experts_n, parts_ref, residual_ref, gain_ref, routes_ref, weight_ref, stream_out, sent_out, w_ref, stream_ref, sent_ref, sems
):
    parts_n, _, width = parts_ref.shape
    spans = [slice(j * width, (j + 1) * width) for j in range(parts_n)]
    loads = fetch([(weight_ref.at[rows], w_ref.at[rows]) for rows in spans], sems)
    found = places(routes_ref[...], experts_n, sent_ref.shape[0] // experts_n)
    table = functools.reduce(jnp.logical_or, found)
    table = jnp.where(table, 1.0, 0.0).astype(jnp.bfloat16)
    for j, rows in enumerate(spans):
        loads[j].wait()
        part = dot(parts_ref[j], w_ref[rows])
        stream_ref[...] = part if j == 0 else stream_ref[...] + part
    mixed = stream_ref[...].astype(jnp.bfloat16).astype(jnp.float32)
    stream = residual_ref[...].astype(jnp.float32) + mixed
    stream_ref[...] = stream
    stores = fetch([(stream_ref, stream_out)], sems, parts_n)
    scale = lax.rsqrt(jnp.mean(stream * stream, axis=1, keepdims=True) + 1e-06)
    normed = (stream * scale * gain_ref[...]).astype(jnp.bfloat16)
    step = normed.shape[1] // 4
    for j in range(4):
        cols = slice(j * step, (j + 1) * step)
        sent_ref[:, cols] = lax.dot_general(
            table, normed[:, cols], (((0,), (0,)), ((), ())), preferred_element_type=jnp.float32
        ).astype(jnp.bfloat16)
        stores += fetch([(sent_ref.at[:, cols], sent_out.at[:, cols])], sems, parts_n + 1 + j)
    for c in stores:
        c.wait()


def table_body(experts_n, me_ref, routes_ref, weights_ref, *out_refs):
    me = me_ref[0]

    def relative(expert):
        along = (me // RING - expert // RING) % RING
        across = (me // 2 % 4 - expert // 2 % 4) % 4
        return along * RING + across * 2 + (me + expert) % 2

    capacity = out_refs[0].shape[1] // experts_n
    for i, seen_as in enumerate((lambda expert: expert, relative)):
        found = places(routes_ref[...], experts_n, capacity, seen_as)
        table = sum(jnp.where(hit, weights_ref[:, m : m + 1], 0.0) for m, hit in enumerate(found))
        high = table.astype(jnp.bfloat16)
        out_refs[2 * i][...] = high
        out_refs[2 * i + 1][...] = (table - high.astype(jnp.float32)).astype(jnp.bfloat16)


def side_body(stream_ref, high_ref, low_ref, *refs):
    *parts, out_ref, back_ref, sems = refs
    for c in fetch([(part, back_ref.at[i]) for i, part in enumerate(parts)], sems):
        c.wait()
    rows = back_ref[...].reshape(high_ref.shape[1], out_ref.shape[1])
    mixed = dot(high_ref[...], rows) + dot(low_ref[...], rows)
    cols = slice(stream_ref.shape[1] - out_ref.shape[1], stream_ref.shape[1])
    out_ref[...] = (stream_ref[:, cols] + mixed).astype(jnp.bfloat16)


def combine_body(stream_ref, high_ref, low_ref, back_ref, side_ref, out, out_ref, sems):
    width = back_ref.shape[1]
    stores, step = fetch([(side_ref, out.at[:, width:])], sems), width // 3
    for i in range(3):
        cols = slice(i * step, (i + 1) * step)
        rows = back_ref[:, cols]
        mixed = dot(high_ref[...], rows) + dot(low_ref[...], rows)
        out_ref[:, cols] = (stream_ref[:, cols] + mixed).astype(jnp.bfloat16)
        stores += fetch([(out_ref.at[:, cols], out.at[:, cols])], sems, 1 + i)
    for c in stores:
        c.wait()


def across(value, step):
    count = lax.axis_size("sp")

    def to(i):
        return i // RING * RING + (i // 2 + step // 2) % 4 * 2 + (i + step) % 2

    return lax.ppermute(value, "sp", [(i, to(i)) for i in range(count)])


def along(value, step):
    count = lax.axis_size("sp")
    return lax.ppermute(value, "sp", [(i, (i + step * RING) % count) for i in range(count)])


def turn_body(me_ref, *refs):
    parts, outs, (held, sems) = refs[:RING], refs[RING : 2 * RING], refs[2 * RING :]
    z = me_ref[0] // RING
    copies = [
        (parts[j].at[(z + step) % RING], held.at[step, j]) for step in range(RING) for j in range(RING)
    ]
    for c in fetch(copies, sems):
        c.wait()
    for c in fetch([(held.at[step], outs[step]) for step in range(RING)], sems):
        c.wait()


def turned(me, parts):
    shape = parts[0].shape
    return kernel(
        turn_body,
        [(shape, jnp.bfloat16)] * RING,
        (me, *parts),
        scratch=[
            pltpu.VMEM((RING, *shape), jnp.bfloat16),
            pltpu.SemaphoreType.DMA((RING * RING,)),
        ],
        limit=8,
        scalar_in=(0,),
        far_in=range(1, 1 + RING),
        far_out=range(RING),
    )


def hidden_body(counts, *refs):
    rows_in, *pieces, far_ref, sum_ref, rows_ref, w_ref, hidden_ref, down_ref, sems = refs
    width = pieces[0].shape[1]
    (load,) = fetch([(rows_in, rows_ref)], sems)
    loads, at = [], 1
    for q, kinds in enumerate(counts):
        copies = []
        for kind, n in enumerate(kinds):
            top = 0
            for piece in pieces[:n]:
                end = top + piece.shape[0]
                copies.append((piece, w_ref.at[q, top:end, kind * width : (kind + 1) * width]))
                top = end
            pieces = pieces[n:]
        loads.append(fetch(copies, sems, at))
        at += len(copies)
    spans = [slice(q * width, (q + 1) * width) for q in range(len(pieces))]
    downs = fetch([(piece, down_ref.at[rows]) for piece, rows in zip(pieces, spans)], sems, at)
    load.wait()
    for q, copies in enumerate(loads):
        for c in copies:
            c.wait()
        act = dot(rows_ref[...], w_ref[q])
        gate = act[:, :width]
        hidden = (gate / (1.0 + jnp.exp(-gate)) * act[:, width:]).astype(jnp.bfloat16)
        if q < len(spans):
            hidden_ref[:, spans[q]] = hidden
        else:
            far_ref[...] = hidden
    for c in downs:
        c.wait()
    step = sum_ref.shape[1] // 4
    for i in range(4):
        cols = slice(i * step, (i + 1) * step)
        sum_ref[:, cols] = dot(hidden_ref[...], down_ref[:, cols])


def hidden_units(rows, quarters, downs):
    counts = tuple((len(gates), len(ups)) for gates, ups in quarters)
    pieces = [p for gates, ups in quarters for p in (*gates, *ups)] + downs
    (n, d), width, out_width = rows.shape, pieces[0].shape[1], downs[0].shape[1]
    return kernel(
        functools.partial(hidden_body, counts),
        [((n, width), jnp.bfloat16), ((n, out_width), jnp.float32)],
        (rows, *pieces),
        scratch=[
            pltpu.VMEM((n, d), jnp.bfloat16),
            pltpu.VMEM((len(counts), d, 2 * width), jnp.bfloat16),
            pltpu.VMEM((n, len(downs) * width), jnp.bfloat16),
            pltpu.VMEM((len(downs) * width, out_width), jnp.bfloat16),
            pltpu.SemaphoreType.DMA((len(pieces) + 1,)),
        ],
        limit=26,
        far_in=range(1 + len(pieces)),
    )


def down_body(me_ref, hidden_ref, sum_ref, *refs):
    *pieces, out = refs[: -RING - 3]
    side_outs, (out_ref, side_ref, sems) = refs[-RING - 3 : -3], refs[-3:]

    def columns(cols):
        total, at = sum_ref[:, cols], 0
        for piece in pieces:
            total = total + dot(hidden_ref[:, at : at + piece.shape[0]], piece[:, cols])
            at += piece.shape[0]
        return total.astype(jnp.bfloat16)

    width = out_ref.shape[1]
    side_ref[...] = columns(slice(width, sum_ref.shape[1])).reshape(side_ref.shape)
    me = me_ref[0]
    stores = []
    for step, side in enumerate(side_outs):
        k = (me // 2 + step // 2) % 4 * 2 + (me + step) % 2
        stores += fetch([(side_ref.at[:, k], side)], sems, step)
    for i in range(3):
        span = slice(i * width // 3, (i + 1) * width // 3)
        out_ref[:, span] = columns(span)
        stores += fetch([(out_ref.at[:, span], out.at[:, span])], sems, RING + i)
    for c in stores:
        c.wait()


def down_rows(me, hidden, total, pieces, width):
    n, side = total.shape[0], total.shape[1] - width
    capacity = n // RING // RING
    return kernel(
        down_body,
        [((n, width), jnp.bfloat16)] + [((RING, capacity, side), jnp.bfloat16)] * RING,
        (me, hidden, total, *pieces),
        scratch=[
            pltpu.VMEM((n, width), jnp.bfloat16),
            pltpu.VMEM((RING, RING, capacity, side), jnp.bfloat16),
            pltpu.SemaphoreType.DMA((RING + 3,)),
        ],
        limit=16,
        scalar_in=(0,),
        far_out=range(1 + RING),
    )


def gathered(shard):
    left, right = ring(shard, "tp", 1), ring(shard, "tp", -1)
    half = shard.shape[0] // 2
    far = [ring(left[:half], "tp", 1), ring(right[half:], "tp", -1)]
    return [left], [right], far


def shards(
    residual,
    conv_value,
    conv_gate,
    segments,
    conv_weight,
    norm_gain,
    norm_shift,
    out_weight,
    ffn_gain,
    routes,
    route_weights,
    w_gate,
    w_up,
    w_down,
):
    tok_dev, local_channels = conv_value.shape
    reach = conv_weight.shape[0] - 1
    model_width = w_down.shape[2]
    gates = gathered(w_gate[0])
    ups = gathered(w_up[0])
    downs = gathered(w_down[0])
    lines = segments.reshape(tok_dev // LANES, LANES)
    rim = passed_along(rim_rows(conv_value, conv_gate, lines), "sp", 1)
    padded = jnp.pad(segments, (reach, 0), constant_values=-1)
    seen = jnp.zeros((tok_dev,), jnp.int32)
    for offset in range(reach):
        seen = seen + (padded[offset : offset + tok_dev] == segments).astype(jnp.int32)
    seen = jnp.broadcast_to(seen[:, None], (tok_dev, LANES))
    conv_out = conv_module(
        conv_value, conv_gate, rim, lines, seen, conv_weight, norm_gain, norm_shift
    )
    columns = lax.axis_size("tp")
    column = lax.axis_index("tp")
    rows_own = tok_dev // columns
    regrouped = lax.all_to_all(
        conv_out.reshape(columns, rows_own, local_channels), "tp", 0, 0, tiled=True
    )
    experts_n = lax.axis_size("sp")
    top_count = routes.shape[1]
    capacity = max(2, 2 * tok_dev * top_count // (columns * experts_n))
    slot_total = experts_n * capacity
    own_routes = lax.dynamic_slice_in_dim(routes, column * rows_own, rows_own, 0)
    own_weights = lax.dynamic_slice_in_dim(route_weights, column * rows_own, rows_own, 0)
    stream, outgoing = kernel(
        functools.partial(route_body, experts_n),
        [((rows_own, model_width), jnp.float32), ((slot_total, model_width), jnp.bfloat16)],
        (regrouped, residual, ffn_gain[None], own_routes, out_weight),
        scratch=[
            pltpu.VMEM(out_weight.shape, jnp.bfloat16),
            pltpu.VMEM((rows_own, model_width), jnp.float32),
            pltpu.VMEM((slot_total, model_width), jnp.bfloat16),
            pltpu.SemaphoreType.DMA((columns + 5,)),
        ],
        limit=24,
        far_in=(4,),
        far_out=(0, 1),
    )
    arrived = lax.all_to_all(
        outgoing.reshape(experts_n, capacity, model_width), "sp", 0, 0, tiled=True
    ).reshape(slot_total, model_width)
    hidden, total = hidden_units(
        arrived,
        [([w_gate[0]], [w_up[0]])] + [(gates[side], ups[side]) for side in range(3)],
        [w_down[0], *downs[0], *downs[1]],
    )
    wide = model_width * 3 // 4
    me = lax.axis_index("sp").astype(jnp.int32)[None]
    out, *parts = down_rows(me, hidden, total, downs[2], wide)
    back = lax.all_to_all(
        out.reshape(experts_n, capacity, wide), "sp", 0, 0, tiled=True
    ).reshape(slot_total, wide)
    parts = parts[:1] + [across(parts[step], step) for step in range(1, RING)]
    parts = turned(me, parts)
    came = [parts[0]] + [None] * (RING - 1)
    for step in (4, 3, 5, 2, 6, 1, 7):
        came[step] = along(parts[step], step)
    high, low, side_high, side_low = kernel(
        functools.partial(table_body, experts_n),
        [((rows_own, slot_total), jnp.bfloat16)] * 4,
        (me, own_routes, own_weights),
        scalar_in=(0,),
    )
    side = kernel(
        side_body,
        ((rows_own, model_width - wide), jnp.bfloat16),
        (stream, side_high, side_low, *came),
        scratch=[
            pltpu.VMEM((RING, *came[0].shape), jnp.bfloat16),
            pltpu.SemaphoreType.DMA((RING,)),
        ],
        far_in=range(3, 3 + RING),
    )
    return kernel(
        combine_body,
        ((rows_own, model_width), jnp.bfloat16),
        (stream, high, low, back, side),
        scratch=[
            pltpu.VMEM((rows_own, wide), jnp.bfloat16),
            pltpu.SemaphoreType.DMA((4,)),
        ],
        limit=24,
        far_out=(0,),
    )


def solution(mesh):
    return jax.shard_map(
        shards,
        mesh=mesh,
        in_specs=(
            P(("sp", "tp"), None),
            P("sp", "tp"),
            P("sp", "tp"),
            P("sp"),
            P(None, "tp"),
            P("tp"),
            P("tp"),
            P(),
            P(),
            P("sp", None),
            P("sp", None),
            P("sp", None, "tp"),
            P("sp", None, "tp"),
            P("sp", "tp", None),
        ),
        out_specs=P(("sp", "tp"), None),
        check_vma=False,
    )
```

```python
import functools

import jax
import jax.numpy as jnp
from jax import lax
from jax.experimental import pallas as pl
from jax.experimental.pallas import tpu as pltpu
from jax.sharding import PartitionSpec as P

TAPS = 31
RIM = 32
LANES = 128
BLOCK = 64
RING = 8


def passed_along(value, axis, steps):
    count = lax.axis_size(axis)
    initial, last = (max(0, -steps), min(count, count - steps))
    return lax.ppermute(value, axis, [(source, source + steps) for source in range(initial, last)])


def ring(value, axis, steps):
    count = lax.axis_size(axis)
    return lax.ppermute(value, axis, [(i, (i + steps) % count) for i in range(count)])


def kernel(body, out, args, scratch=(), limit=16, far_in=(), far_out=(), scalar_in=()):
    scalar = pl.BlockSpec(memory_space=pltpu.SMEM)
    whole, far = pl.BlockSpec(memory_space=pltpu.VMEM), pl.BlockSpec(memory_space=pltpu.HBM)
    args = [
        a
        if i in scalar_in
        else pltpu.with_memory_space_constraint(a, pltpu.HBM if i in far_in else pltpu.VMEM)
        for i, a in enumerate(args)
    ]
    outs = out if isinstance(out, list) else [out]
    got = pl.pallas_call(
        body,
        out_shape=[
            pltpu.HBM(*o) if i in far_out else jax.ShapeDtypeStruct(*o) for i, o in enumerate(outs)
        ],
        in_specs=[
            scalar if i in scalar_in else far if i in far_in else whole for i in range(len(args))
        ],
        out_specs=[far if i in far_out else whole for i in range(len(outs))],
        scratch_shapes=scratch,
        compiler_params=pltpu.CompilerParams(vmem_limit_bytes=limit << 20),
    )(*args)
    return got if isinstance(out, list) else got[0]


def fetch(copies, sems, first=0):
    started = [
        pltpu.make_async_copy(src, dst, sems.at[first + i]) for i, (src, dst) in enumerate(copies)
    ]
    for c in started:
        c.start()
    return started


def gated_rows(value, gate):
    return (value.astype(jnp.float32) * jax.nn.sigmoid(gate.astype(jnp.float32))).astype(jnp.bfloat16)


def rim_body(value_ref, gate_ref, segments_ref, out_ref):
    width = value_ref.shape[1]
    gated = gated_rows(value_ref[...], gate_ref[...]).astype(jnp.float32)
    last = segments_ref[segments_ref.shape[0] - 1 :, :].astype(jnp.float32)
    named = jnp.concatenate([last] + [jnp.zeros_like(last)] * (width // LANES - 1), axis=1)
    row = lax.broadcasted_iota(jnp.int32, gated.shape, 0)
    out_ref[...] = jnp.where(row == 0, named, gated).astype(jnp.bfloat16)


def rim_rows(value, gate, segments):
    tok, width = value.shape
    last = pl.BlockSpec((RIM, width), lambda i: (tok // RIM - 1, 0))
    return pl.pallas_call(
        rim_body,
        grid=(1,),
        in_specs=[last, last, pl.BlockSpec(segments.shape, lambda i: (0, 0))],
        out_specs=pl.BlockSpec((RIM, width), lambda i: (0, 0)),
        out_shape=jax.ShapeDtypeStruct((RIM, width), jnp.bfloat16),
        name="rim_rows",
    )(value, gate, segments)


def conv_body(rim_ref, seen_ref, *refs):
    sources, (out_ref, rows_ref, *held, sems) = refs[:6], refs[6:]
    for c in fetch(list(zip(sources, held)), sems):
        c.wait()
    value_ref, gate_ref, segments_ref, taps_ref, gain_ref, shift_ref = held
    tok = value_ref.shape[0]
    rows_ref[0, :RIM] = rim_ref[...].astype(jnp.float32)
    rows_ref[0, RIM:] = gated_rows(value_ref[...], gate_ref[...]).astype(jnp.float32)
    for r in range(1, 8):
        rows_ref[r, 8:] = rows_ref[0, 8 - r : RIM + tok - r]
    lane = lax.broadcasted_iota(jnp.int32, (1, LANES), 1)
    same = rim_ref[0:1, :LANES].astype(jnp.float32) == segments_ref[0:1, 0:1].astype(jnp.float32)
    same = jnp.where(same & (lane >= LANES - (TAPS - 1)), 1.0, 0.0)
    before = jnp.sum(same, axis=1, keepdims=True).astype(jnp.int32)

    def block(i, carry):
        at = pl.multiple_of(i * BLOCK, BLOCK)
        seen = seen_ref[pl.ds(at, BLOCK), :]
        row = at + lax.broadcasted_iota(jnp.int32, (BLOCK, LANES), 0)
        seen = jnp.where(seen == row, seen + before, seen)
        for lane in range(0, value_ref.shape[1], LANES):
            cols = slice(lane, lane + LANES)
            total = rows_ref[0, pl.ds(at + RIM, BLOCK), cols] * taps_ref[TAPS - 1 : TAPS, cols]
            for back in range(1, TAPS):
                tap = TAPS - 1 - back
                rows = rows_ref[back % 8, pl.ds(at + RIM - back // 8 * 8, BLOCK), cols]
                total = total + jnp.where(seen >= back, rows * taps_ref[tap : tap + 1, cols], 0.0)
            dev = total - jnp.mean(total, axis=1, keepdims=True)
            var = jnp.mean(dev * dev, axis=1, keepdims=True)
            v = dev * lax.rsqrt(var + 1e-05) * gain_ref[:, cols] + shift_ref[:, cols]
            out_ref[pl.ds(at, BLOCK), cols] = (v / (1.0 + jnp.exp(-v))).astype(jnp.bfloat16)
        return carry

    lax.fori_loop(0, tok // BLOCK, block, 0)


def conv_module(value, gate, rim, segments, seen, taps, gain, shift):
    tok, width = value.shape
    fetched = (value, gate, segments, taps, gain[None], shift[None])
    return kernel(
        conv_body,
        ((tok, width), jnp.bfloat16),
        (rim, seen, *fetched),
        scratch=[pltpu.VMEM((8, RIM + tok, width), jnp.float32)]
        + [pltpu.VMEM(a.shape, a.dtype) for a in fetched]
        + [pltpu.SemaphoreType.DMA((len(fetched),))],
        far_in=range(2, 2 + len(fetched)),
    )


def dot(a, b):
    return jnp.dot(a, b, preferred_element_type=jnp.float32)


def ranks(routes, experts_n):
    rows, top_count = routes.shape
    expert = lax.broadcasted_iota(jnp.int32, (rows, experts_n), 1)
    named = [jnp.where(expert == routes[:, m : m + 1], 1.0, 0.0) for m in range(top_count)]
    earlier = lax.broadcasted_iota(jnp.int32, (rows, rows), 0) > lax.broadcasted_iota(
        jnp.int32, (rows, rows), 1
    )
    earlier = jnp.where(earlier, 1.0, 0.0).astype(jnp.bfloat16)
    taken = dot(earlier, sum(named).astype(jnp.bfloat16))
    return [jnp.sum(n * taken, axis=1, keepdims=True).astype(jnp.int32) for n in named]


def places(routes, experts_n, capacity, seen_as=lambda expert: expert):
    number = lax.broadcasted_iota(jnp.int32, (routes.shape[0], experts_n * capacity), 1)
    return [
        number == seen_as(routes[:, m : m + 1]) * capacity + rank
        for m, rank in enumerate(ranks(routes, experts_n))
    ]


def route_body(
    experts_n, parts_ref, residual_ref, gain_ref, routes_ref, weight_ref, stream_out, sent_out, w_ref, stream_ref, sent_ref, sems
):
    parts_n, _, width = parts_ref.shape
    spans = [slice(j * width, (j + 1) * width) for j in range(parts_n)]
    loads = fetch([(weight_ref.at[rows], w_ref.at[rows]) for rows in spans], sems)
    found = places(routes_ref[...], experts_n, sent_ref.shape[0] // experts_n)
    table = functools.reduce(jnp.logical_or, found)
    table = jnp.where(table, 1.0, 0.0).astype(jnp.bfloat16)
    for j, rows in enumerate(spans):
        loads[j].wait()
        part = dot(parts_ref[j], w_ref[rows])
        stream_ref[...] = part if j == 0 else stream_ref[...] + part
    mixed = stream_ref[...].astype(jnp.bfloat16).astype(jnp.float32)
    stream = residual_ref[...].astype(jnp.float32) + mixed
    stream_ref[...] = stream
    stores = fetch([(stream_ref, stream_out)], sems, parts_n)
    scale = lax.rsqrt(jnp.mean(stream * stream, axis=1, keepdims=True) + 1e-06)
    normed = (stream * scale * gain_ref[...]).astype(jnp.bfloat16)
    step = normed.shape[1] // 4
    for j in range(4):
        cols = slice(j * step, (j + 1) * step)
        sent_ref[:, cols] = lax.dot_general(
            table, normed[:, cols], (((0,), (0,)), ((), ())), preferred_element_type=jnp.float32
        ).astype(jnp.bfloat16)
        stores += fetch([(sent_ref.at[:, cols], sent_out.at[:, cols])], sems, parts_n + 1 + j)
    for c in stores:
        c.wait()


def table_body(experts_n, me_ref, routes_ref, weights_ref, *out_refs):
    me = me_ref[0]

    def relative(expert):
        along = (me // RING - expert // RING) % RING
        across = (me // 2 % 4 - expert // 2 % 4) % 4
        return along * RING + across * 2 + (me + expert) % 2

    capacity = out_refs[0].shape[1] // experts_n
    for i, seen_as in enumerate((lambda expert: expert, relative)):
        found = places(routes_ref[...], experts_n, capacity, seen_as)
        table = sum(jnp.where(hit, weights_ref[:, m : m + 1], 0.0) for m, hit in enumerate(found))
        high = table.astype(jnp.bfloat16)
        out_refs[2 * i][...] = high
        out_refs[2 * i + 1][...] = (table - high.astype(jnp.float32)).astype(jnp.bfloat16)


def side_body(stream_ref, high_ref, low_ref, *refs):
    *parts, out_ref, back_ref, sems = refs
    for c in fetch([(part, back_ref.at[i]) for i, part in enumerate(parts)], sems):
        c.wait()
    rows = back_ref[...].reshape(high_ref.shape[1], out_ref.shape[1])
    mixed = dot(high_ref[...], rows) + dot(low_ref[...], rows)
    cols = slice(stream_ref.shape[1] - out_ref.shape[1], stream_ref.shape[1])
    out_ref[...] = (stream_ref[:, cols] + mixed).astype(jnp.bfloat16)


def combine_body(stream_ref, high_ref, low_ref, back_ref, side_ref, out, out_ref, sems):
    width = back_ref.shape[1]
    stores, step = fetch([(side_ref, out.at[:, width:])], sems), width // 2
    for i in range(2):
        cols = slice(i * step, (i + 1) * step)
        rows = back_ref[:, cols]
        mixed = dot(high_ref[...], rows) + dot(low_ref[...], rows)
        out_ref[:, cols] = (stream_ref[:, cols] + mixed).astype(jnp.bfloat16)
        stores += fetch([(out_ref.at[:, cols], out.at[:, cols])], sems, 1 + i)
    for c in stores:
        c.wait()


def across(value, step):
    count = lax.axis_size("sp")

    def to(i):
        return i // RING * RING + (i // 2 + step // 2) % 4 * 2 + (i + step) % 2

    return lax.ppermute(value, "sp", [(i, to(i)) for i in range(count)])


def along(value, step):
    count = lax.axis_size("sp")
    return lax.ppermute(value, "sp", [(i, (i + step * RING) % count) for i in range(count)])


def turn_body(me_ref, *refs):
    parts, outs, (held, sems) = refs[:RING], refs[RING : 2 * RING], refs[2 * RING :]
    z = me_ref[0] // RING
    copies = [
        (parts[j].at[(z + step) % RING], held.at[step, j]) for step in range(RING) for j in range(RING)
    ]
    for c in fetch(copies, sems):
        c.wait()
    for c in fetch([(held.at[step], outs[step]) for step in range(RING)], sems):
        c.wait()


def turned(me, parts):
    shape = parts[0].shape
    return kernel(
        turn_body,
        [(shape, jnp.bfloat16)] * RING,
        (me, *parts),
        scratch=[
            pltpu.VMEM((RING, *shape), jnp.bfloat16),
            pltpu.SemaphoreType.DMA((RING * RING,)),
        ],
        limit=8,
        scalar_in=(0,),
        far_in=range(1, 1 + RING),
        far_out=range(RING),
    )


def hidden_body(counts, *refs):
    rows_in, *pieces, far_ref, sum_ref, rows_ref, w_ref, hidden_ref, down_ref, sems = refs
    width = pieces[0].shape[1]
    (load,) = fetch([(rows_in, rows_ref)], sems)
    loads, at = [], 1
    for q, kinds in enumerate(counts):
        copies = []
        for kind, n in enumerate(kinds):
            top = 0
            for piece in pieces[:n]:
                end = top + piece.shape[0]
                copies.append((piece, w_ref.at[q, top:end, kind * width : (kind + 1) * width]))
                top = end
            pieces = pieces[n:]
        loads.append(fetch(copies, sems, at))
        at += len(copies)
    spans = [slice(q * width, (q + 1) * width) for q in range(len(pieces))]
    downs = fetch([(piece, down_ref.at[rows]) for piece, rows in zip(pieces, spans)], sems, at)
    load.wait()
    for q, copies in enumerate(loads):
        for c in copies:
            c.wait()
        act = dot(rows_ref[...], w_ref[q])
        gate = act[:, :width]
        hidden = (gate / (1.0 + jnp.exp(-gate)) * act[:, width:]).astype(jnp.bfloat16)
        if q < len(spans):
            hidden_ref[:, spans[q]] = hidden
        else:
            far_ref[...] = hidden
    for c in downs:
        c.wait()
    step = sum_ref.shape[1] // 4
    for i in range(4):
        cols = slice(i * step, (i + 1) * step)
        sum_ref[:, cols] = dot(hidden_ref[...], down_ref[:, cols])


def hidden_units(rows, quarters, downs):
    counts = tuple((len(gates), len(ups)) for gates, ups in quarters)
    pieces = [p for gates, ups in quarters for p in (*gates, *ups)] + downs
    (n, d), width, out_width = rows.shape, pieces[0].shape[1], downs[0].shape[1]
    return kernel(
        functools.partial(hidden_body, counts),
        [((n, width), jnp.bfloat16), ((n, out_width), jnp.float32)],
        (rows, *pieces),
        scratch=[
            pltpu.VMEM((n, d), jnp.bfloat16),
            pltpu.VMEM((len(counts), d, 2 * width), jnp.bfloat16),
            pltpu.VMEM((n, len(downs) * width), jnp.bfloat16),
            pltpu.VMEM((len(downs) * width, out_width), jnp.bfloat16),
            pltpu.SemaphoreType.DMA((len(pieces) + 1,)),
        ],
        limit=26,
        far_in=range(1 + len(pieces)),
    )


def down_body(me_ref, hidden_ref, sum_ref, *refs):
    *pieces, out = refs[: -RING - 3]
    side_outs, (out_ref, side_ref, sems) = refs[-RING - 3 : -3], refs[-3:]

    def columns(cols):
        total, at = sum_ref[:, cols], 0
        for piece in pieces:
            total = total + dot(hidden_ref[:, at : at + piece.shape[0]], piece[:, cols])
            at += piece.shape[0]
        return total.astype(jnp.bfloat16)

    width = out_ref.shape[1]
    side_ref[...] = columns(slice(width, sum_ref.shape[1])).reshape(side_ref.shape)
    me = me_ref[0]
    stores = []
    for step, side in enumerate(side_outs):
        k = (me // 2 + step // 2) % 4 * 2 + (me + step) % 2
        stores += fetch([(side_ref.at[:, k], side)], sems, step)
    for i in range(2):
        span = slice(i * width // 2, (i + 1) * width // 2)
        out_ref[:, span] = columns(span)
        stores += fetch([(out_ref.at[:, span], out.at[:, span])], sems, RING + i)
    for c in stores:
        c.wait()


def down_rows(me, hidden, total, pieces, width):
    n, side = total.shape[0], total.shape[1] - width
    capacity = n // RING // RING
    return kernel(
        down_body,
        [((n, width), jnp.bfloat16)] + [((RING, capacity, side), jnp.bfloat16)] * RING,
        (me, hidden, total, *pieces),
        scratch=[
            pltpu.VMEM((n, width), jnp.bfloat16),
            pltpu.VMEM((RING, RING, capacity, side), jnp.bfloat16),
            pltpu.SemaphoreType.DMA((RING + 2,)),
        ],
        limit=16,
        scalar_in=(0,),
        far_out=range(1 + RING),
    )


def gathered(shard):
    left, right = ring(shard, "tp", 1), ring(shard, "tp", -1)
    half = shard.shape[0] // 2
    far = [ring(left[:half], "tp", 1), ring(right[half:], "tp", -1)]
    return [left], [right], far


def shards(
    residual,
    conv_value,
    conv_gate,
    segments,
    conv_weight,
    norm_gain,
    norm_shift,
    out_weight,
    ffn_gain,
    routes,
    route_weights,
    w_gate,
    w_up,
    w_down,
):
    tok_dev, local_channels = conv_value.shape
    reach = conv_weight.shape[0] - 1
    model_width = w_down.shape[2]
    gates = gathered(w_gate[0])
    ups = gathered(w_up[0])
    downs = gathered(w_down[0])
    lines = segments.reshape(tok_dev // LANES, LANES)
    rim = passed_along(rim_rows(conv_value, conv_gate, lines), "sp", 1)
    padded = jnp.pad(segments, (reach, 0), constant_values=-1)
    seen = jnp.zeros((tok_dev,), jnp.int32)
    for offset in range(reach):
        seen = seen + (padded[offset : offset + tok_dev] == segments).astype(jnp.int32)
    seen = jnp.broadcast_to(seen[:, None], (tok_dev, LANES))
    conv_out = conv_module(
        conv_value, conv_gate, rim, lines, seen, conv_weight, norm_gain, norm_shift
    )
    columns = lax.axis_size("tp")
    column = lax.axis_index("tp")
    rows_own = tok_dev // columns
    regrouped = lax.all_to_all(
        conv_out.reshape(columns, rows_own, local_channels), "tp", 0, 0, tiled=True
    )
    experts_n = lax.axis_size("sp")
    top_count = routes.shape[1]
    capacity = max(2, 2 * tok_dev * top_count // (columns * experts_n))
    slot_total = experts_n * capacity
    own_routes = lax.dynamic_slice_in_dim(routes, column * rows_own, rows_own, 0)
    own_weights = lax.dynamic_slice_in_dim(route_weights, column * rows_own, rows_own, 0)
    stream, outgoing = kernel(
        functools.partial(route_body, experts_n),
        [((rows_own, model_width), jnp.float32), ((slot_total, model_width), jnp.bfloat16)],
        (regrouped, residual, ffn_gain[None], own_routes, out_weight),
        scratch=[
            pltpu.VMEM(out_weight.shape, jnp.bfloat16),
            pltpu.VMEM((rows_own, model_width), jnp.float32),
            pltpu.VMEM((slot_total, model_width), jnp.bfloat16),
            pltpu.SemaphoreType.DMA((columns + 5,)),
        ],
        limit=24,
        far_in=(4,),
        far_out=(0, 1),
    )
    arrived = lax.all_to_all(
        outgoing.reshape(experts_n, capacity, model_width), "sp", 0, 0, tiled=True
    ).reshape(slot_total, model_width)
    hidden, total = hidden_units(
        arrived,
        [([w_gate[0]], [w_up[0]])] + [(gates[side], ups[side]) for side in range(3)],
        [w_down[0], *downs[0], *downs[1]],
    )
    wide = model_width * 7 // 8
    me = lax.axis_index("sp").astype(jnp.int32)[None]
    out, *parts = down_rows(me, hidden, total, downs[2], wide)
    back = lax.all_to_all(
        out.reshape(experts_n, capacity, wide), "sp", 0, 0, tiled=True
    ).reshape(slot_total, wide)
    parts = parts[:1] + [across(parts[step], step) for step in range(1, RING)]
    parts = turned(me, parts)
    came = [parts[0]] + [None] * (RING - 1)
    for step in (4, 3, 5, 2, 6, 1, 7):
        came[step] = along(parts[step], step)
    high, low, side_high, side_low = kernel(
        functools.partial(table_body, experts_n),
        [((rows_own, slot_total), jnp.bfloat16)] * 4,
        (me, own_routes, own_weights),
        scalar_in=(0,),
    )
    side = kernel(
        side_body,
        ((rows_own, model_width - wide), jnp.bfloat16),
        (stream, side_high, side_low, *came),
        scratch=[
            pltpu.VMEM((RING, *came[0].shape), jnp.bfloat16),
            pltpu.SemaphoreType.DMA((RING,)),
        ],
        far_in=range(3, 3 + RING),
    )
    return kernel(
        combine_body,
        ((rows_own, model_width), jnp.bfloat16),
        (stream, high, low, back, side),
        scratch=[
            pltpu.VMEM((rows_own, wide), jnp.bfloat16),
            pltpu.SemaphoreType.DMA((3,)),
        ],
        limit=24,
        far_out=(0,),
    )


def solution(mesh):
    return jax.shard_map(
        shards,
        mesh=mesh,
        in_specs=(
            P(("sp", "tp"), None),
            P("sp", "tp"),
            P("sp", "tp"),
            P("sp"),
            P(None, "tp"),
            P("tp"),
            P("tp"),
            P(),
            P(),
            P("sp", None),
            P("sp", None),
            P("sp", None, "tp"),
            P("sp", None, "tp"),
            P("sp", "tp", None),
        ),
        out_specs=P(("sp", "tp"), None),
        check_vma=False,
    )
```

```python
import functools

import jax
import jax.numpy as jnp
from jax import lax
from jax.experimental import pallas as pl
from jax.experimental.pallas import tpu as pltpu
from jax.sharding import PartitionSpec as P

TAPS = 31
RIM = 32
LANES = 128
BLOCK = 64


def passed_along(value, axis, steps):
    count = lax.axis_size(axis)
    initial, last = (max(0, -steps), min(count, count - steps))
    return lax.ppermute(value, axis, [(source, source + steps) for source in range(initial, last)])


def ring(value, axis, steps):
    count = lax.axis_size(axis)
    return lax.ppermute(value, axis, [(i, (i + steps) % count) for i in range(count)])


def kernel(body, out, args, scratch=(), limit=16, far_in=(), far_out=()):
    whole, far = pl.BlockSpec(memory_space=pltpu.VMEM), pl.BlockSpec(memory_space=pltpu.HBM)
    args = [
        pltpu.with_memory_space_constraint(a, pltpu.HBM if i in far_in else pltpu.VMEM)
        for i, a in enumerate(args)
    ]
    outs = out if isinstance(out, list) else [out]
    got = pl.pallas_call(
        body,
        out_shape=[
            pltpu.HBM(*o) if i in far_out else jax.ShapeDtypeStruct(*o) for i, o in enumerate(outs)
        ],
        in_specs=[far if i in far_in else whole for i in range(len(args))],
        out_specs=[far if i in far_out else whole for i in range(len(outs))],
        scratch_shapes=scratch,
        compiler_params=pltpu.CompilerParams(vmem_limit_bytes=limit << 20),
    )(*args)
    return got if isinstance(out, list) else got[0]


def fetch(copies, sems, first=0):
    started = [
        pltpu.make_async_copy(src, dst, sems.at[first + i]) for i, (src, dst) in enumerate(copies)
    ]
    for c in started:
        c.start()
    return started


def gated_rows(value, gate):
    return (value.astype(jnp.float32) * jax.nn.sigmoid(gate.astype(jnp.float32))).astype(jnp.bfloat16)


def rim_body(value_ref, gate_ref, segments_ref, out_ref):
    width = value_ref.shape[1]
    gated = gated_rows(value_ref[...], gate_ref[...]).astype(jnp.float32)
    last = segments_ref[segments_ref.shape[0] - 1 :, :].astype(jnp.float32)
    named = jnp.concatenate([last] + [jnp.zeros_like(last)] * (width // LANES - 1), axis=1)
    row = lax.broadcasted_iota(jnp.int32, gated.shape, 0)
    out_ref[...] = jnp.where(row == 0, named, gated).astype(jnp.bfloat16)


def rim_rows(value, gate, segments):
    tok, width = value.shape
    last = pl.BlockSpec((RIM, width), lambda i: (tok // RIM - 1, 0))
    return pl.pallas_call(
        rim_body,
        grid=(1,),
        in_specs=[last, last, pl.BlockSpec(segments.shape, lambda i: (0, 0))],
        out_specs=pl.BlockSpec((RIM, width), lambda i: (0, 0)),
        out_shape=jax.ShapeDtypeStruct((RIM, width), jnp.bfloat16),
        name="rim_rows",
    )(value, gate, segments)


def conv_body(rim_ref, seen_ref, *refs):
    sources, (out_ref, rows_ref, *held, sems) = refs[:6], refs[6:]
    for c in fetch(list(zip(sources, held)), sems):
        c.wait()
    value_ref, gate_ref, segments_ref, taps_ref, gain_ref, shift_ref = held
    tok = value_ref.shape[0]
    rows_ref[0, :RIM] = rim_ref[...].astype(jnp.float32)
    rows_ref[0, RIM:] = gated_rows(value_ref[...], gate_ref[...]).astype(jnp.float32)
    for r in range(1, 8):
        rows_ref[r, 8:] = rows_ref[0, 8 - r : RIM + tok - r]
    lane = lax.broadcasted_iota(jnp.int32, (1, LANES), 1)
    same = rim_ref[0:1, :LANES].astype(jnp.float32) == segments_ref[0:1, 0:1].astype(jnp.float32)
    same = jnp.where(same & (lane >= LANES - (TAPS - 1)), 1.0, 0.0)
    before = jnp.sum(same, axis=1, keepdims=True).astype(jnp.int32)

    def block(i, carry):
        at = pl.multiple_of(i * BLOCK, BLOCK)
        seen = seen_ref[pl.ds(at, BLOCK), :]
        row = at + lax.broadcasted_iota(jnp.int32, (BLOCK, LANES), 0)
        seen = jnp.where(seen == row, seen + before, seen)
        for lane in range(0, value_ref.shape[1], LANES):
            cols = slice(lane, lane + LANES)
            total = rows_ref[0, pl.ds(at + RIM, BLOCK), cols] * taps_ref[TAPS - 1 : TAPS, cols]
            for back in range(1, TAPS):
                tap = TAPS - 1 - back
                rows = rows_ref[back % 8, pl.ds(at + RIM - back // 8 * 8, BLOCK), cols]
                total = total + jnp.where(seen >= back, rows * taps_ref[tap : tap + 1, cols], 0.0)
            dev = total - jnp.mean(total, axis=1, keepdims=True)
            var = jnp.mean(dev * dev, axis=1, keepdims=True)
            v = dev * lax.rsqrt(var + 1e-05) * gain_ref[:, cols] + shift_ref[:, cols]
            out_ref[pl.ds(at, BLOCK), cols] = (v / (1.0 + jnp.exp(-v))).astype(jnp.bfloat16)
        return carry

    lax.fori_loop(0, tok // BLOCK, block, 0)


def conv_module(value, gate, rim, segments, seen, taps, gain, shift):
    tok, width = value.shape
    fetched = (value, gate, segments, taps, gain[None], shift[None])
    return kernel(
        conv_body,
        ((tok, width), jnp.bfloat16),
        (rim, seen, *fetched),
        scratch=[pltpu.VMEM((8, RIM + tok, width), jnp.float32)]
        + [pltpu.VMEM(a.shape, a.dtype) for a in fetched]
        + [pltpu.SemaphoreType.DMA((len(fetched),))],
        far_in=range(2, 2 + len(fetched)),
    )


def dot(a, b):
    return jnp.dot(a, b, preferred_element_type=jnp.float32)


def places(routes, experts_n, capacity):
    rows, top_count = routes.shape
    expert = lax.broadcasted_iota(jnp.int32, (rows, experts_n), 1)
    named = [jnp.where(expert == routes[:, m : m + 1], 1.0, 0.0) for m in range(top_count)]
    earlier = lax.broadcasted_iota(jnp.int32, (rows, rows), 0) > lax.broadcasted_iota(
        jnp.int32, (rows, rows), 1
    )
    earlier = jnp.where(earlier, 1.0, 0.0).astype(jnp.bfloat16)
    taken = dot(earlier, sum(named).astype(jnp.bfloat16))
    number = lax.broadcasted_iota(jnp.int32, (rows, experts_n * capacity), 1)
    found = []
    for m in range(top_count):
        rank = jnp.sum(named[m] * taken, axis=1, keepdims=True).astype(jnp.int32)
        found.append(number == routes[:, m : m + 1] * capacity + rank)
    return found


def route_body(
    experts_n, parts_ref, residual_ref, gain_ref, routes_ref, weight_ref, stream_out, sent_out, w_ref, stream_ref, sent_ref, sems
):
    parts_n, _, width = parts_ref.shape
    spans = [slice(j * width, (j + 1) * width) for j in range(parts_n)]
    loads = fetch([(weight_ref.at[rows], w_ref.at[rows]) for rows in spans], sems)
    found = places(routes_ref[...], experts_n, sent_ref.shape[0] // experts_n)
    table = functools.reduce(jnp.logical_or, found)
    table = jnp.where(table, 1.0, 0.0).astype(jnp.bfloat16)
    for j, rows in enumerate(spans):
        loads[j].wait()
        part = dot(parts_ref[j], w_ref[rows])
        stream_ref[...] = part if j == 0 else stream_ref[...] + part
    mixed = stream_ref[...].astype(jnp.bfloat16).astype(jnp.float32)
    stream = residual_ref[...].astype(jnp.float32) + mixed
    stream_ref[...] = stream
    stores = fetch([(stream_ref, stream_out)], sems, parts_n)
    scale = lax.rsqrt(jnp.mean(stream * stream, axis=1, keepdims=True) + 1e-06)
    normed = (stream * scale * gain_ref[...]).astype(jnp.bfloat16)
    step = normed.shape[1] // 4
    for j in range(4):
        cols = slice(j * step, (j + 1) * step)
        sent_ref[:, cols] = lax.dot_general(
            table, normed[:, cols], (((0,), (0,)), ((), ())), preferred_element_type=jnp.float32
        ).astype(jnp.bfloat16)
        stores += fetch([(sent_ref.at[:, cols], sent_out.at[:, cols])], sems, parts_n + 1 + j)
    for c in stores:
        c.wait()


def table_body(experts_n, routes_ref, weights_ref, high_ref, low_ref):
    found = places(routes_ref[...], experts_n, high_ref.shape[1] // experts_n)
    table = sum(jnp.where(hit, weights_ref[:, m : m + 1], 0.0) for m, hit in enumerate(found))
    high = table.astype(jnp.bfloat16)
    high_ref[...] = high
    low_ref[...] = (table - high.astype(jnp.float32)).astype(jnp.bfloat16)


def combine_body(stream_ref, high_ref, low_ref, back_ref, out, out_ref, sems):
    stores, step = [], out_ref.shape[1] // 4
    for i in range(4):
        cols = slice(i * step, (i + 1) * step)
        rows = back_ref[:, cols]
        mixed = dot(high_ref[...], rows) + dot(low_ref[...], rows)
        out_ref[:, cols] = (stream_ref[:, cols] + mixed).astype(jnp.bfloat16)
        stores += fetch([(out_ref.at[:, cols], out.at[:, cols])], sems, i)
    for c in stores:
        c.wait()


def hidden_body(counts, *refs):
    rows_in, *pieces, far_ref, sum_ref, rows_ref, w_ref, hidden_ref, down_ref, sems = refs
    width = pieces[0].shape[1]
    (load,) = fetch([(rows_in, rows_ref)], sems)
    loads, at = [], 1
    for q, kinds in enumerate(counts):
        copies = []
        for kind, n in enumerate(kinds):
            top = 0
            for piece in pieces[:n]:
                end = top + piece.shape[0]
                copies.append((piece, w_ref.at[q, top:end, kind * width : (kind + 1) * width]))
                top = end
            pieces = pieces[n:]
        loads.append(fetch(copies, sems, at))
        at += len(copies)
    copies, top = [], 0
    for piece in pieces:
        copies.append((piece, down_ref.at[top : top + piece.shape[0]]))
        top += piece.shape[0]
    downs = fetch(copies, sems, at)
    load.wait()
    for q, copies in enumerate(loads):
        for c in copies:
            c.wait()
        act = dot(rows_ref[...], w_ref[q])
        gate = act[:, :width]
        hidden = (gate / (1.0 + jnp.exp(-gate)) * act[:, width:]).astype(jnp.bfloat16)
        if q < len(counts) - 1:
            hidden_ref[:, q * width : (q + 1) * width] = hidden
        else:
            far_ref[...] = hidden
    for c in downs:
        c.wait()
    step = sum_ref.shape[1] // 4
    for i in range(4):
        cols = slice(i * step, (i + 1) * step)
        sum_ref[:, cols] = dot(hidden_ref[...], down_ref[:, cols])


def hidden_units(rows, quarters, downs):
    counts = tuple((len(gates), len(ups)) for gates, ups in quarters)
    pieces = [p for gates, ups in quarters for p in (*gates, *ups)] + downs
    (n, d), width, out_width = rows.shape, pieces[0].shape[1], downs[0].shape[1]
    return kernel(
        functools.partial(hidden_body, counts),
        [((n, width), jnp.bfloat16), ((n, out_width), jnp.float32)],
        (rows, *pieces),
        scratch=[
            pltpu.VMEM((n, d), jnp.bfloat16),
            pltpu.VMEM((len(counts), d, 2 * width), jnp.bfloat16),
            pltpu.VMEM((n, (len(counts) - 1) * width), jnp.bfloat16),
            pltpu.VMEM(((len(counts) - 1) * width, out_width), jnp.bfloat16),
            pltpu.SemaphoreType.DMA((len(pieces) + 1,)),
        ],
        limit=26,
        far_in=range(1 + len(pieces)),
    )


def down_body(hidden_ref, sum_ref, *refs):
    *pieces, out, out_ref, sems = refs
    stores, step = [], out_ref.shape[1] // 4
    for i in range(4):
        cols = slice(i * step, (i + 1) * step)
        total, at = sum_ref[:, cols], 0
        for piece in pieces:
            total = total + dot(hidden_ref[:, at : at + piece.shape[0]], piece[:, cols])
            at += piece.shape[0]
        out_ref[:, cols] = total.astype(jnp.bfloat16)
        stores += fetch([(out_ref.at[:, cols], out.at[:, cols])], sems, i)
    for c in stores:
        c.wait()


def down_rows(hidden, total, pieces):
    n, width = total.shape
    return kernel(
        down_body,
        ((n, width), jnp.bfloat16),
        (hidden, total, *pieces),
        scratch=[pltpu.VMEM((n, width), jnp.bfloat16), pltpu.SemaphoreType.DMA((4,))],
        limit=16,
        far_out=(0,),
    )


def gathered(shard):
    left, right = ring(shard, "tp", 1), ring(shard, "tp", -1)
    half = shard.shape[0] // 2
    far = [ring(left[:half], "tp", 1), ring(right[half:], "tp", -1)]
    return [left], [right], far


def gathered_halves(shard):
    half = shard.shape[0] // 2
    top, low = shard[:half], shard[half:]
    left_top, right_low = ring(top, "tp", 1), ring(low, "tp", -1)
    left_low, right_top = ring(low, "tp", 1), ring(top, "tp", -1)
    far = [ring(left_top, "tp", 1), ring(right_low, "tp", -1)]
    return [left_top, left_low], [right_top, right_low], far


def shards(
    residual,
    conv_value,
    conv_gate,
    segments,
    conv_weight,
    norm_gain,
    norm_shift,
    out_weight,
    ffn_gain,
    routes,
    route_weights,
    w_gate,
    w_up,
    w_down,
):
    tok_dev, local_channels = conv_value.shape
    reach = conv_weight.shape[0] - 1
    model_width = w_down.shape[2]
    gates = gathered(w_gate[0])
    ups = gathered(w_up[0])
    downs = gathered_halves(w_down[0])
    lines = segments.reshape(tok_dev // LANES, LANES)
    rim = passed_along(rim_rows(conv_value, conv_gate, lines), "sp", 1)
    padded = jnp.pad(segments, (reach, 0), constant_values=-1)
    seen = jnp.zeros((tok_dev,), jnp.int32)
    for offset in range(reach):
        seen = seen + (padded[offset : offset + tok_dev] == segments).astype(jnp.int32)
    seen = jnp.broadcast_to(seen[:, None], (tok_dev, LANES))
    conv_out = conv_module(
        conv_value, conv_gate, rim, lines, seen, conv_weight, norm_gain, norm_shift
    )
    columns = lax.axis_size("tp")
    column = lax.axis_index("tp")
    rows_own = tok_dev // columns
    regrouped = lax.all_to_all(
        conv_out.reshape(columns, rows_own, local_channels), "tp", 0, 0, tiled=True
    )
    experts_n = lax.axis_size("sp")
    top_count = routes.shape[1]
    capacity = max(2, 2 * tok_dev * top_count // (columns * experts_n))
    slot_total = experts_n * capacity
    own_routes = lax.dynamic_slice_in_dim(routes, column * rows_own, rows_own, 0)
    own_weights = lax.dynamic_slice_in_dim(route_weights, column * rows_own, rows_own, 0)
    stream, outgoing = kernel(
        functools.partial(route_body, experts_n),
        [((rows_own, model_width), jnp.float32), ((slot_total, model_width), jnp.bfloat16)],
        (regrouped, residual, ffn_gain[None], own_routes, out_weight),
        scratch=[
            pltpu.VMEM(out_weight.shape, jnp.bfloat16),
            pltpu.VMEM((rows_own, model_width), jnp.float32),
            pltpu.VMEM((slot_total, model_width), jnp.bfloat16),
            pltpu.SemaphoreType.DMA((columns + 5,)),
        ],
        limit=24,
        far_in=(4,),
        far_out=(0, 1),
    )
    arrived = lax.all_to_all(
        outgoing.reshape(experts_n, capacity, model_width), "sp", 0, 0, tiled=True
    ).reshape(slot_total, model_width)
    hidden, total = hidden_units(
        arrived,
        [([w_gate[0]], [w_up[0]])] + [(gates[side], ups[side]) for side in range(3)],
        [w_down[0], *downs[0], *downs[1]],
    )
    out = down_rows(hidden, total, downs[2])
    back = lax.all_to_all(
        out.reshape(experts_n, capacity, model_width), "sp", 0, 0, tiled=True
    ).reshape(slot_total, model_width)
    high, low = kernel(
        functools.partial(table_body, experts_n),
        [((rows_own, slot_total), jnp.bfloat16)] * 2,
        (own_routes, own_weights),
    )
    return kernel(
        combine_body,
        ((rows_own, model_width), jnp.bfloat16),
        (stream, high, low, back),
        scratch=[pltpu.VMEM((rows_own, model_width), jnp.bfloat16), pltpu.SemaphoreType.DMA((4,))],
        limit=24,
        far_out=(0,),
    )


def solution(mesh):
    return jax.shard_map(
        shards,
        mesh=mesh,
        in_specs=(
            P(("sp", "tp"), None),
            P("sp", "tp"),
            P("sp", "tp"),
            P("sp"),
            P(None, "tp"),
            P("tp"),
            P("tp"),
            P(),
            P(),
            P("sp", None),
            P("sp", None),
            P("sp", None, "tp"),
            P("sp", None, "tp"),
            P("sp", "tp", None),
        ),
        out_specs=P(("sp", "tp"), None),
        check_vma=False,
    )
```

```python
import functools

import jax
import jax.numpy as jnp
from jax import lax
from jax.experimental import pallas as pl
from jax.experimental.pallas import tpu as pltpu
from jax.sharding import PartitionSpec as P

TAPS = 31
RIM = 32
LANES = 128
BLOCK = 64


def passed_along(value, axis, steps):
    count = lax.axis_size(axis)
    initial, last = (max(0, -steps), min(count, count - steps))
    return lax.ppermute(value, axis, [(source, source + steps) for source in range(initial, last)])


def ring(value, axis, steps):
    count = lax.axis_size(axis)
    return lax.ppermute(value, axis, [(i, (i + steps) % count) for i in range(count)])


def kernel(body, out, args, scratch=(), limit=16, far_in=(), far_out=()):
    whole, far = pl.BlockSpec(memory_space=pltpu.VMEM), pl.BlockSpec(memory_space=pltpu.HBM)
    args = [
        pltpu.with_memory_space_constraint(a, pltpu.HBM if i in far_in else pltpu.VMEM)
        for i, a in enumerate(args)
    ]
    outs = out if isinstance(out, list) else [out]
    got = pl.pallas_call(
        body,
        out_shape=[
            pltpu.HBM(*o) if i in far_out else jax.ShapeDtypeStruct(*o) for i, o in enumerate(outs)
        ],
        in_specs=[far if i in far_in else whole for i in range(len(args))],
        out_specs=[far if i in far_out else whole for i in range(len(outs))],
        scratch_shapes=scratch,
        compiler_params=pltpu.CompilerParams(vmem_limit_bytes=limit << 20),
    )(*args)
    return got if isinstance(out, list) else got[0]


def fetch(copies, sems, first=0):
    started = [
        pltpu.make_async_copy(src, dst, sems.at[first + i]) for i, (src, dst) in enumerate(copies)
    ]
    for c in started:
        c.start()
    return started


def gated_rows(value, gate):
    return (value.astype(jnp.float32) * jax.nn.sigmoid(gate.astype(jnp.float32))).astype(jnp.bfloat16)


def rim_body(value_ref, gate_ref, segments_ref, out_ref):
    width = value_ref.shape[1]
    gated = gated_rows(value_ref[...], gate_ref[...]).astype(jnp.float32)
    last = segments_ref[segments_ref.shape[0] - 1 :, :].astype(jnp.float32)
    named = jnp.concatenate([last] + [jnp.zeros_like(last)] * (width // LANES - 1), axis=1)
    row = lax.broadcasted_iota(jnp.int32, gated.shape, 0)
    out_ref[...] = jnp.where(row == 0, named, gated).astype(jnp.bfloat16)


def rim_rows(value, gate, segments):
    tok, width = value.shape
    last = pl.BlockSpec((RIM, width), lambda i: (tok // RIM - 1, 0))
    return pl.pallas_call(
        rim_body,
        grid=(1,),
        in_specs=[last, last, pl.BlockSpec(segments.shape, lambda i: (0, 0))],
        out_specs=pl.BlockSpec((RIM, width), lambda i: (0, 0)),
        out_shape=jax.ShapeDtypeStruct((RIM, width), jnp.bfloat16),
        name="rim_rows",
    )(value, gate, segments)


def conv_body(rim_ref, seen_ref, *refs):
    sources, (out_ref, rows_ref, *held, sems) = refs[:6], refs[6:]
    for c in fetch(list(zip(sources, held)), sems):
        c.wait()
    value_ref, gate_ref, segments_ref, taps_ref, gain_ref, shift_ref = held
    tok = value_ref.shape[0]
    rows_ref[0, :RIM] = rim_ref[...].astype(jnp.float32)
    rows_ref[0, RIM:] = gated_rows(value_ref[...], gate_ref[...]).astype(jnp.float32)
    for r in range(1, 8):
        rows_ref[r, 8:] = rows_ref[0, 8 - r : RIM + tok - r]
    lane = lax.broadcasted_iota(jnp.int32, (1, LANES), 1)
    same = rim_ref[0:1, :LANES].astype(jnp.float32) == segments_ref[0:1, 0:1].astype(jnp.float32)
    same = jnp.where(same & (lane >= LANES - (TAPS - 1)), 1.0, 0.0)
    before = jnp.sum(same, axis=1, keepdims=True).astype(jnp.int32)

    def block(i, carry):
        at = pl.multiple_of(i * BLOCK, BLOCK)
        seen = seen_ref[pl.ds(at, BLOCK), :]
        row = at + lax.broadcasted_iota(jnp.int32, (BLOCK, LANES), 0)
        seen = jnp.where(seen == row, seen + before, seen)
        for lane in range(0, value_ref.shape[1], LANES):
            cols = slice(lane, lane + LANES)
            total = rows_ref[0, pl.ds(at + RIM, BLOCK), cols] * taps_ref[TAPS - 1 : TAPS, cols]
            for back in range(1, TAPS):
                tap = TAPS - 1 - back
                rows = rows_ref[back % 8, pl.ds(at + RIM - back // 8 * 8, BLOCK), cols]
                total = total + jnp.where(seen >= back, rows * taps_ref[tap : tap + 1, cols], 0.0)
            dev = total - jnp.mean(total, axis=1, keepdims=True)
            var = jnp.mean(dev * dev, axis=1, keepdims=True)
            v = dev * lax.rsqrt(var + 1e-05) * gain_ref[:, cols] + shift_ref[:, cols]
            out_ref[pl.ds(at, BLOCK), cols] = (v / (1.0 + jnp.exp(-v))).astype(jnp.bfloat16)
        return carry

    lax.fori_loop(0, tok // BLOCK, block, 0)


def conv_module(value, gate, rim, segments, seen, taps, gain, shift):
    tok, width = value.shape
    fetched = (value, gate, segments, taps, gain[None], shift[None])
    return kernel(
        conv_body,
        ((tok, width), jnp.bfloat16),
        (rim, seen, *fetched),
        scratch=[pltpu.VMEM((8, RIM + tok, width), jnp.float32)]
        + [pltpu.VMEM(a.shape, a.dtype) for a in fetched]
        + [pltpu.SemaphoreType.DMA((len(fetched),))],
        far_in=range(2, 2 + len(fetched)),
    )


def dot(a, b):
    return jnp.dot(a, b, preferred_element_type=jnp.float32)


def places(routes, experts_n, capacity):
    rows, top_count = routes.shape
    expert = lax.broadcasted_iota(jnp.int32, (rows, experts_n), 1)
    named = [jnp.where(expert == routes[:, m : m + 1], 1.0, 0.0) for m in range(top_count)]
    earlier = lax.broadcasted_iota(jnp.int32, (rows, rows), 0) > lax.broadcasted_iota(
        jnp.int32, (rows, rows), 1
    )
    earlier = jnp.where(earlier, 1.0, 0.0).astype(jnp.bfloat16)
    taken = dot(earlier, sum(named).astype(jnp.bfloat16))
    number = lax.broadcasted_iota(jnp.int32, (rows, experts_n * capacity), 1)
    found = []
    for m in range(top_count):
        rank = jnp.sum(named[m] * taken, axis=1, keepdims=True).astype(jnp.int32)
        found.append(number == routes[:, m : m + 1] * capacity + rank)
    return found


def route_body(
    experts_n, parts_ref, residual_ref, gain_ref, routes_ref, weight_ref, stream_out, sent_out, w_ref, stream_ref, sent_ref, sems
):
    parts_n, _, width = parts_ref.shape
    spans = [slice(j * width, (j + 1) * width) for j in range(parts_n)]
    loads = fetch([(weight_ref.at[rows], w_ref.at[rows]) for rows in spans], sems)
    found = places(routes_ref[...], experts_n, sent_ref.shape[0] // experts_n)
    table = functools.reduce(jnp.logical_or, found)
    table = jnp.where(table, 1.0, 0.0).astype(jnp.bfloat16)
    for j, rows in enumerate(spans):
        loads[j].wait()
        part = dot(parts_ref[j], w_ref[rows])
        stream_ref[...] = part if j == 0 else stream_ref[...] + part
    mixed = stream_ref[...].astype(jnp.bfloat16).astype(jnp.float32)
    stream = residual_ref[...].astype(jnp.float32) + mixed
    stream_ref[...] = stream
    stores = fetch([(stream_ref, stream_out)], sems, parts_n)
    scale = lax.rsqrt(jnp.mean(stream * stream, axis=1, keepdims=True) + 1e-06)
    normed = (stream * scale * gain_ref[...]).astype(jnp.bfloat16)
    step = normed.shape[1] // 4
    for j in range(4):
        cols = slice(j * step, (j + 1) * step)
        sent_ref[:, cols] = lax.dot_general(
            table, normed[:, cols], (((0,), (0,)), ((), ())), preferred_element_type=jnp.float32
        ).astype(jnp.bfloat16)
        stores += fetch([(sent_ref.at[:, cols], sent_out.at[:, cols])], sems, parts_n + 1 + j)
    for c in stores:
        c.wait()


def table_body(experts_n, routes_ref, weights_ref, high_ref, low_ref):
    found = places(routes_ref[...], experts_n, high_ref.shape[1] // experts_n)
    table = sum(jnp.where(hit, weights_ref[:, m : m + 1], 0.0) for m, hit in enumerate(found))
    high = table.astype(jnp.bfloat16)
    high_ref[...] = high
    low_ref[...] = (table - high.astype(jnp.float32)).astype(jnp.bfloat16)


def combine_body(stream_ref, high_ref, low_ref, back_ref, out, out_ref, sems):
    stores, step = [], out_ref.shape[1] // 4
    for i in range(4):
        cols = slice(i * step, (i + 1) * step)
        rows = back_ref[:, cols]
        mixed = dot(high_ref[...], rows) + dot(low_ref[...], rows)
        out_ref[:, cols] = (stream_ref[:, cols] + mixed).astype(jnp.bfloat16)
        stores += fetch([(out_ref.at[:, cols], out.at[:, cols])], sems, i)
    for c in stores:
        c.wait()


def hidden_body(counts, *refs):
    rows_ref, *pieces, far_ref, sum_ref, w_ref, hidden_ref, down_ref, sems = refs
    width = pieces[0].shape[1]
    loads, at = [], 0
    for q, kinds in enumerate(counts):
        copies = []
        for kind, n in enumerate(kinds):
            top = 0
            for piece in pieces[:n]:
                end = top + piece.shape[0]
                copies.append((piece, w_ref.at[q, top:end, kind * width : (kind + 1) * width]))
                top = end
            pieces = pieces[n:]
        loads.append(fetch(copies, sems, at))
        at += len(copies)
    spans = [slice(q * width, (q + 1) * width) for q in range(len(pieces))]
    downs = fetch([(piece, down_ref.at[rows]) for piece, rows in zip(pieces, spans)], sems, at)
    for q, copies in enumerate(loads):
        for c in copies:
            c.wait()
        act = dot(rows_ref[...], w_ref[q])
        gate = act[:, :width]
        hidden = (gate / (1.0 + jnp.exp(-gate)) * act[:, width:]).astype(jnp.bfloat16)
        if q < len(spans):
            hidden_ref[:, spans[q]] = hidden
        else:
            far_ref[...] = hidden
    for c in downs:
        c.wait()
    step = sum_ref.shape[1] // 4
    for i in range(4):
        cols = slice(i * step, (i + 1) * step)
        sum_ref[:, cols] = dot(hidden_ref[...], down_ref[:, cols])


def hidden_units(rows, quarters, downs):
    counts = tuple((len(gates), len(ups)) for gates, ups in quarters)
    pieces = [p for gates, ups in quarters for p in (*gates, *ups)] + downs
    (n, d), width, out_width = rows.shape, pieces[0].shape[1], downs[0].shape[1]
    return kernel(
        functools.partial(hidden_body, counts),
        [((n, width), jnp.bfloat16), ((n, out_width), jnp.float32)],
        (rows, *pieces),
        scratch=[
            pltpu.VMEM((len(counts), d, 2 * width), jnp.bfloat16),
            pltpu.VMEM((n, len(downs) * width), jnp.bfloat16),
            pltpu.VMEM((len(downs) * width, out_width), jnp.bfloat16),
            pltpu.SemaphoreType.DMA((len(pieces),)),
        ],
        limit=24,
        far_in=range(1, 1 + len(pieces)),
    )


def down_body(hidden_ref, sum_ref, *refs):
    *pieces, out, out_ref, sems = refs
    stores, step = [], out_ref.shape[1] // 4
    for i in range(4):
        cols = slice(i * step, (i + 1) * step)
        total, at = sum_ref[:, cols], 0
        for piece in pieces:
            total = total + dot(hidden_ref[:, at : at + piece.shape[0]], piece[:, cols])
            at += piece.shape[0]
        out_ref[:, cols] = total.astype(jnp.bfloat16)
        stores += fetch([(out_ref.at[:, cols], out.at[:, cols])], sems, i)
    for c in stores:
        c.wait()


def down_rows(hidden, total, pieces):
    n, width = total.shape
    return kernel(
        down_body,
        ((n, width), jnp.bfloat16),
        (hidden, total, *pieces),
        scratch=[pltpu.VMEM((n, width), jnp.bfloat16), pltpu.SemaphoreType.DMA((4,))],
        limit=16,
        far_out=(0,),
    )


def gathered(shard):
    left, right = ring(shard, "tp", 1), ring(shard, "tp", -1)
    half = shard.shape[0] // 2
    far = [ring(left[:half], "tp", 1), ring(right[half:], "tp", -1)]
    return [left], [right], far


def shards(
    residual,
    conv_value,
    conv_gate,
    segments,
    conv_weight,
    norm_gain,
    norm_shift,
    out_weight,
    ffn_gain,
    routes,
    route_weights,
    w_gate,
    w_up,
    w_down,
):
    tok_dev, local_channels = conv_value.shape
    reach = conv_weight.shape[0] - 1
    model_width = w_down.shape[2]
    gates = gathered(w_gate[0])
    ups = gathered(w_up[0])
    downs = gathered(w_down[0])
    lines = segments.reshape(tok_dev // LANES, LANES)
    rim = passed_along(rim_rows(conv_value, conv_gate, lines), "sp", 1)
    padded = jnp.pad(segments, (reach, 0), constant_values=-1)
    seen = jnp.zeros((tok_dev,), jnp.int32)
    for offset in range(reach):
        seen = seen + (padded[offset : offset + tok_dev] == segments).astype(jnp.int32)
    seen = jnp.broadcast_to(seen[:, None], (tok_dev, LANES))
    conv_out = conv_module(
        conv_value, conv_gate, rim, lines, seen, conv_weight, norm_gain, norm_shift
    )
    columns = lax.axis_size("tp")
    column = lax.axis_index("tp")
    rows_own = tok_dev // columns
    regrouped = lax.all_to_all(
        conv_out.reshape(columns, rows_own, local_channels), "tp", 0, 0, tiled=True
    )
    experts_n = lax.axis_size("sp")
    top_count = routes.shape[1]
    capacity = max(2, 2 * tok_dev * top_count // (columns * experts_n))
    slot_total = experts_n * capacity
    own_routes = lax.dynamic_slice_in_dim(routes, column * rows_own, rows_own, 0)
    own_weights = lax.dynamic_slice_in_dim(route_weights, column * rows_own, rows_own, 0)
    stream, outgoing = kernel(
        functools.partial(route_body, experts_n),
        [((rows_own, model_width), jnp.float32), ((slot_total, model_width), jnp.bfloat16)],
        (regrouped, residual, ffn_gain[None], own_routes, out_weight),
        scratch=[
            pltpu.VMEM(out_weight.shape, jnp.bfloat16),
            pltpu.VMEM((rows_own, model_width), jnp.float32),
            pltpu.VMEM((slot_total, model_width), jnp.bfloat16),
            pltpu.SemaphoreType.DMA((columns + 5,)),
        ],
        limit=24,
        far_in=(4,),
        far_out=(0, 1),
    )
    arrived = lax.all_to_all(
        outgoing.reshape(experts_n, capacity, model_width), "sp", 0, 0, tiled=True
    ).reshape(slot_total, model_width)
    hidden, total = hidden_units(
        arrived,
        [([w_gate[0]], [w_up[0]])] + [(gates[side], ups[side]) for side in range(3)],
        [w_down[0], *downs[0], *downs[1]],
    )
    out = down_rows(hidden, total, downs[2])
    back = lax.all_to_all(
        out.reshape(experts_n, capacity, model_width), "sp", 0, 0, tiled=True
    ).reshape(slot_total, model_width)
    high, low = kernel(
        functools.partial(table_body, experts_n),
        [((rows_own, slot_total), jnp.bfloat16)] * 2,
        (own_routes, own_weights),
    )
    return kernel(
        combine_body,
        ((rows_own, model_width), jnp.bfloat16),
        (stream, high, low, back),
        scratch=[pltpu.VMEM((rows_own, model_width), jnp.bfloat16), pltpu.SemaphoreType.DMA((4,))],
        limit=24,
        far_out=(0,),
    )


def solution(mesh):
    return jax.shard_map(
        shards,
        mesh=mesh,
        in_specs=(
            P(("sp", "tp"), None),
            P("sp", "tp"),
            P("sp", "tp"),
            P("sp"),
            P(None, "tp"),
            P("tp"),
            P("tp"),
            P(),
            P(),
            P("sp", None),
            P("sp", None),
            P("sp", None, "tp"),
            P("sp", None, "tp"),
            P("sp", "tp", None),
        ),
        out_specs=P(("sp", "tp"), None),
        check_vma=False,
    )
```

```python
import functools

import jax
import jax.numpy as jnp
from jax import lax
from jax.experimental import pallas as pl
from jax.experimental.pallas import tpu as pltpu
from jax.sharding import PartitionSpec as P

TAPS = 31
RIM = 32
LANES = 128
BLOCK = 64


def passed_along(value, axis, steps):
    count = lax.axis_size(axis)
    initial, last = (max(0, -steps), min(count, count - steps))
    return lax.ppermute(value, axis, [(source, source + steps) for source in range(initial, last)])


def ring(value, axis, steps):
    count = lax.axis_size(axis)
    return lax.ppermute(value, axis, [(i, (i + steps) % count) for i in range(count)])


def kernel(body, out, args, scratch=(), limit=16, far_in=(), far_out=()):
    whole, far = pl.BlockSpec(memory_space=pltpu.VMEM), pl.BlockSpec(memory_space=pltpu.HBM)
    args = [
        pltpu.with_memory_space_constraint(a, pltpu.HBM if i in far_in else pltpu.VMEM)
        for i, a in enumerate(args)
    ]
    outs = out if isinstance(out, list) else [out]
    got = pl.pallas_call(
        body,
        out_shape=[
            pltpu.HBM(*o) if i in far_out else jax.ShapeDtypeStruct(*o) for i, o in enumerate(outs)
        ],
        in_specs=[far if i in far_in else whole for i in range(len(args))],
        out_specs=[far if i in far_out else whole for i in range(len(outs))],
        scratch_shapes=scratch,
        compiler_params=pltpu.CompilerParams(vmem_limit_bytes=limit << 20),
    )(*args)
    return got if isinstance(out, list) else got[0]


def fetch(copies, sems, first=0):
    started = [
        pltpu.make_async_copy(src, dst, sems.at[first + i]) for i, (src, dst) in enumerate(copies)
    ]
    for c in started:
        c.start()
    return started


def gated_rows(value, gate):
    return (value.astype(jnp.float32) * jax.nn.sigmoid(gate.astype(jnp.float32))).astype(jnp.bfloat16)


def rim_body(value_ref, gate_ref, segments_ref, out_ref):
    width = value_ref.shape[1]
    gated = gated_rows(value_ref[...], gate_ref[...]).astype(jnp.float32)
    last = segments_ref[segments_ref.shape[0] - 1 :, :].astype(jnp.float32)
    named = jnp.concatenate([last] + [jnp.zeros_like(last)] * (width // LANES - 1), axis=1)
    row = lax.broadcasted_iota(jnp.int32, gated.shape, 0)
    out_ref[...] = jnp.where(row == 0, named, gated).astype(jnp.bfloat16)


def rim_rows(value, gate, segments):
    tok, width = value.shape
    last = pl.BlockSpec((RIM, width), lambda i: (tok // RIM - 1, 0))
    return pl.pallas_call(
        rim_body,
        grid=(1,),
        in_specs=[last, last, pl.BlockSpec(segments.shape, lambda i: (0, 0))],
        out_specs=pl.BlockSpec((RIM, width), lambda i: (0, 0)),
        out_shape=jax.ShapeDtypeStruct((RIM, width), jnp.bfloat16),
        name="rim_rows",
    )(value, gate, segments)


def conv_body(rim_ref, seen_ref, *refs):
    sources, (out_ref, rows_ref, *held, sems) = refs[:6], refs[6:]
    for c in fetch(list(zip(sources, held)), sems):
        c.wait()
    value_ref, gate_ref, segments_ref, taps_ref, gain_ref, shift_ref = held
    tok = value_ref.shape[0]
    rows_ref[0, :RIM] = rim_ref[...].astype(jnp.float32)
    rows_ref[0, RIM:] = gated_rows(value_ref[...], gate_ref[...]).astype(jnp.float32)
    for r in range(1, 8):
        rows_ref[r, 8:] = rows_ref[0, 8 - r : RIM + tok - r]
    lane = lax.broadcasted_iota(jnp.int32, (1, LANES), 1)
    same = rim_ref[0:1, :LANES].astype(jnp.float32) == segments_ref[0:1, 0:1].astype(jnp.float32)
    same = jnp.where(same & (lane >= LANES - (TAPS - 1)), 1.0, 0.0)
    before = jnp.sum(same, axis=1, keepdims=True).astype(jnp.int32)

    def block(i, carry):
        at = pl.multiple_of(i * BLOCK, BLOCK)
        seen = seen_ref[pl.ds(at, BLOCK), :]
        row = at + lax.broadcasted_iota(jnp.int32, (BLOCK, LANES), 0)
        seen = jnp.where(seen == row, seen + before, seen)
        for lane in range(0, value_ref.shape[1], LANES):
            cols = slice(lane, lane + LANES)
            total = rows_ref[0, pl.ds(at + RIM, BLOCK), cols] * taps_ref[TAPS - 1 : TAPS, cols]
            for back in range(1, TAPS):
                tap = TAPS - 1 - back
                rows = rows_ref[back % 8, pl.ds(at + RIM - back // 8 * 8, BLOCK), cols]
                total = total + jnp.where(seen >= back, rows * taps_ref[tap : tap + 1, cols], 0.0)
            dev = total - jnp.mean(total, axis=1, keepdims=True)
            var = jnp.mean(dev * dev, axis=1, keepdims=True)
            v = dev * lax.rsqrt(var + 1e-05) * gain_ref[:, cols] + shift_ref[:, cols]
            out_ref[pl.ds(at, BLOCK), cols] = (v / (1.0 + jnp.exp(-v))).astype(jnp.bfloat16)
        return carry

    lax.fori_loop(0, tok // BLOCK, block, 0)


def conv_module(value, gate, rim, segments, seen, taps, gain, shift):
    tok, width = value.shape
    fetched = (value, gate, segments, taps, gain[None], shift[None])
    return kernel(
        conv_body,
        ((tok, width), jnp.bfloat16),
        (rim, seen, *fetched),
        scratch=[pltpu.VMEM((8, RIM + tok, width), jnp.float32)]
        + [pltpu.VMEM(a.shape, a.dtype) for a in fetched]
        + [pltpu.SemaphoreType.DMA((len(fetched),))],
        far_in=range(2, 2 + len(fetched)),
    )


def dot(a, b):
    return jnp.dot(a, b, preferred_element_type=jnp.float32)


def places(routes, experts_n, capacity):
    rows, top_count = routes.shape
    expert = lax.broadcasted_iota(jnp.int32, (rows, experts_n), 1)
    named = [jnp.where(expert == routes[:, m : m + 1], 1.0, 0.0) for m in range(top_count)]
    earlier = lax.broadcasted_iota(jnp.int32, (rows, rows), 0) > lax.broadcasted_iota(
        jnp.int32, (rows, rows), 1
    )
    earlier = jnp.where(earlier, 1.0, 0.0).astype(jnp.bfloat16)
    taken = dot(earlier, sum(named).astype(jnp.bfloat16))
    number = lax.broadcasted_iota(jnp.int32, (rows, experts_n * capacity), 1)
    found = []
    for m in range(top_count):
        rank = jnp.sum(named[m] * taken, axis=1, keepdims=True).astype(jnp.int32)
        found.append(number == routes[:, m : m + 1] * capacity + rank)
    return found


def route_body(
    experts_n, parts_ref, residual_ref, gain_ref, routes_ref, weight_ref, stream_out, sent_out, w_ref, stream_ref, sent_ref, sems
):
    parts_n, _, width = parts_ref.shape
    spans = [slice(j * width, (j + 1) * width) for j in range(parts_n)]
    loads = fetch([(weight_ref.at[rows], w_ref.at[rows]) for rows in spans], sems)
    found = places(routes_ref[...], experts_n, sent_ref.shape[0] // experts_n)
    table = functools.reduce(jnp.logical_or, found)
    table = jnp.where(table, 1.0, 0.0).astype(jnp.bfloat16)
    for j, rows in enumerate(spans):
        loads[j].wait()
        part = dot(parts_ref[j], w_ref[rows])
        stream_ref[...] = part if j == 0 else stream_ref[...] + part
    mixed = stream_ref[...].astype(jnp.bfloat16).astype(jnp.float32)
    stream = residual_ref[...].astype(jnp.float32) + mixed
    stream_ref[...] = stream
    stores = fetch([(stream_ref, stream_out)], sems, parts_n)
    scale = lax.rsqrt(jnp.mean(stream * stream, axis=1, keepdims=True) + 1e-06)
    normed = (stream * scale * gain_ref[...]).astype(jnp.bfloat16)
    step = normed.shape[1] // 4
    for j in range(4):
        cols = slice(j * step, (j + 1) * step)
        sent_ref[:, cols] = lax.dot_general(
            table, normed[:, cols], (((0,), (0,)), ((), ())), preferred_element_type=jnp.float32
        ).astype(jnp.bfloat16)
        stores += fetch([(sent_ref.at[:, cols], sent_out.at[:, cols])], sems, parts_n + 1 + j)
    for c in stores:
        c.wait()


def table_body(experts_n, routes_ref, weights_ref, high_ref, low_ref):
    found = places(routes_ref[...], experts_n, high_ref.shape[1] // experts_n)
    table = sum(jnp.where(hit, weights_ref[:, m : m + 1], 0.0) for m, hit in enumerate(found))
    high = table.astype(jnp.bfloat16)
    high_ref[...] = high
    low_ref[...] = (table - high.astype(jnp.float32)).astype(jnp.bfloat16)


def combine_body(stream_ref, high_ref, low_ref, back_ref, out, out_ref, sems):
    stores, step = [], out_ref.shape[1] // 4
    for i in range(4):
        cols = slice(i * step, (i + 1) * step)
        rows = back_ref[:, cols]
        mixed = dot(high_ref[...], rows) + dot(low_ref[...], rows)
        out_ref[:, cols] = (stream_ref[:, cols] + mixed).astype(jnp.bfloat16)
        stores += fetch([(out_ref.at[:, cols], out.at[:, cols])], sems, i)
    for c in stores:
        c.wait()


def hidden_body(counts, *refs):
    rows_ref, *pieces, far_ref, sum_ref, w_ref, hidden_ref, down_ref, sems = refs
    deep, width = pieces[0].shape
    loads, at = [], 0
    for q, kinds in enumerate(counts):
        copies = []
        for kind, n in enumerate(kinds):
            top = 0
            for piece in pieces[:n]:
                end = top + piece.shape[0]
                copies.append((piece, w_ref.at[q, top:end, kind * width : (kind + 1) * width]))
                top = end
            pieces = pieces[n:]
        if q == 0:
            copies = [
                (src.at[rows], dst.at[rows])
                for rows in (slice(0, deep // 2), slice(deep // 2, deep))
                for src, dst in copies
            ]
        loads.append(fetch(copies, sems, at))
        at += len(copies)
    spans = [slice(q * width, (q + 1) * width) for q in range(len(pieces))]
    downs = fetch([(piece, down_ref.at[rows]) for piece, rows in zip(pieces, spans)], sems, at)
    for q, copies in enumerate(loads):
        act, parts = None, 2 if q == 0 else 1
        for part in range(parts):
            for c in copies[part * len(copies) // parts : (part + 1) * len(copies) // parts]:
                c.wait()
            rows = slice(part * deep // parts, (part + 1) * deep // parts)
            found = dot(rows_ref[:, rows], w_ref[q, rows])
            act = found if act is None else act + found
        gate = act[:, :width]
        hidden = (gate / (1.0 + jnp.exp(-gate)) * act[:, width:]).astype(jnp.bfloat16)
        if q < len(spans):
            hidden_ref[:, spans[q]] = hidden
        else:
            far_ref[...] = hidden
    for c in downs:
        c.wait()
    step = sum_ref.shape[1] // 4
    for i in range(4):
        cols = slice(i * step, (i + 1) * step)
        sum_ref[:, cols] = dot(hidden_ref[...], down_ref[:, cols])


def hidden_units(rows, quarters, downs):
    counts = tuple((len(gates), len(ups)) for gates, ups in quarters)
    pieces = [p for gates, ups in quarters for p in (*gates, *ups)] + downs
    (n, d), width, out_width = rows.shape, pieces[0].shape[1], downs[0].shape[1]
    return kernel(
        functools.partial(hidden_body, counts),
        [((n, width), jnp.bfloat16), ((n, out_width), jnp.float32)],
        (rows, *pieces),
        scratch=[
            pltpu.VMEM((len(counts), d, 2 * width), jnp.bfloat16),
            pltpu.VMEM((n, len(downs) * width), jnp.bfloat16),
            pltpu.VMEM((len(downs) * width, out_width), jnp.bfloat16),
            pltpu.SemaphoreType.DMA((len(pieces) + 2,)),
        ],
        limit=24,
        far_in=range(1, 1 + len(pieces)),
    )


def down_body(hidden_ref, sum_ref, *refs):
    *pieces, out, out_ref, sems = refs
    stores, step = [], out_ref.shape[1] // 4
    for i in range(4):
        cols = slice(i * step, (i + 1) * step)
        total, at = sum_ref[:, cols], 0
        for piece in pieces:
            total = total + dot(hidden_ref[:, at : at + piece.shape[0]], piece[:, cols])
            at += piece.shape[0]
        out_ref[:, cols] = total.astype(jnp.bfloat16)
        stores += fetch([(out_ref.at[:, cols], out.at[:, cols])], sems, i)
    for c in stores:
        c.wait()


def down_rows(hidden, total, pieces):
    n, width = total.shape
    return kernel(
        down_body,
        ((n, width), jnp.bfloat16),
        (hidden, total, *pieces),
        scratch=[pltpu.VMEM((n, width), jnp.bfloat16), pltpu.SemaphoreType.DMA((4,))],
        limit=16,
        far_out=(0,),
    )


def gathered(shard):
    left, right = ring(shard, "tp", 1), ring(shard, "tp", -1)
    half = shard.shape[0] // 2
    far = [ring(left[:half], "tp", 1), ring(right[half:], "tp", -1)]
    return [left], [right], far


def shards(
    residual,
    conv_value,
    conv_gate,
    segments,
    conv_weight,
    norm_gain,
    norm_shift,
    out_weight,
    ffn_gain,
    routes,
    route_weights,
    w_gate,
    w_up,
    w_down,
):
    tok_dev, local_channels = conv_value.shape
    reach = conv_weight.shape[0] - 1
    model_width = w_down.shape[2]
    gates = gathered(w_gate[0])
    ups = gathered(w_up[0])
    downs = gathered(w_down[0])
    lines = segments.reshape(tok_dev // LANES, LANES)
    rim = passed_along(rim_rows(conv_value, conv_gate, lines), "sp", 1)
    padded = jnp.pad(segments, (reach, 0), constant_values=-1)
    seen = jnp.zeros((tok_dev,), jnp.int32)
    for offset in range(reach):
        seen = seen + (padded[offset : offset + tok_dev] == segments).astype(jnp.int32)
    seen = jnp.broadcast_to(seen[:, None], (tok_dev, LANES))
    conv_out = conv_module(
        conv_value, conv_gate, rim, lines, seen, conv_weight, norm_gain, norm_shift
    )
    columns = lax.axis_size("tp")
    column = lax.axis_index("tp")
    rows_own = tok_dev // columns
    regrouped = lax.all_to_all(
        conv_out.reshape(columns, rows_own, local_channels), "tp", 0, 0, tiled=True
    )
    experts_n = lax.axis_size("sp")
    top_count = routes.shape[1]
    capacity = max(2, 2 * tok_dev * top_count // (columns * experts_n))
    slot_total = experts_n * capacity
    own_routes = lax.dynamic_slice_in_dim(routes, column * rows_own, rows_own, 0)
    own_weights = lax.dynamic_slice_in_dim(route_weights, column * rows_own, rows_own, 0)
    stream, outgoing = kernel(
        functools.partial(route_body, experts_n),
        [((rows_own, model_width), jnp.float32), ((slot_total, model_width), jnp.bfloat16)],
        (regrouped, residual, ffn_gain[None], own_routes, out_weight),
        scratch=[
            pltpu.VMEM(out_weight.shape, jnp.bfloat16),
            pltpu.VMEM((rows_own, model_width), jnp.float32),
            pltpu.VMEM((slot_total, model_width), jnp.bfloat16),
            pltpu.SemaphoreType.DMA((columns + 5,)),
        ],
        limit=24,
        far_in=(4,),
        far_out=(0, 1),
    )
    arrived = lax.all_to_all(
        outgoing.reshape(experts_n, capacity, model_width), "sp", 0, 0, tiled=True
    ).reshape(slot_total, model_width)
    hidden, total = hidden_units(
        arrived,
        [([w_gate[0]], [w_up[0]])] + [(gates[side], ups[side]) for side in range(3)],
        [w_down[0], *downs[0], *downs[1]],
    )
    out = down_rows(hidden, total, downs[2])
    back = lax.all_to_all(
        out.reshape(experts_n, capacity, model_width), "sp", 0, 0, tiled=True
    ).reshape(slot_total, model_width)
    high, low = kernel(
        functools.partial(table_body, experts_n),
        [((rows_own, slot_total), jnp.bfloat16)] * 2,
        (own_routes, own_weights),
    )
    return kernel(
        combine_body,
        ((rows_own, model_width), jnp.bfloat16),
        (stream, high, low, back),
        scratch=[pltpu.VMEM((rows_own, model_width), jnp.bfloat16), pltpu.SemaphoreType.DMA((4,))],
        limit=24,
        far_out=(0,),
    )


def solution(mesh):
    return jax.shard_map(
        shards,
        mesh=mesh,
        in_specs=(
            P(("sp", "tp"), None),
            P("sp", "tp"),
            P("sp", "tp"),
            P("sp"),
            P(None, "tp"),
            P("tp"),
            P("tp"),
            P(),
            P(),
            P("sp", None),
            P("sp", None),
            P("sp", None, "tp"),
            P("sp", None, "tp"),
            P("sp", "tp", None),
        ),
        out_specs=P(("sp", "tp"), None),
        check_vma=False,
    )
```
